512 devices in a mesh: sp: 128 (over z, y, core), tp: 4 (over x).
Axes of the slice: x: 4, y: 8, z: 8, core: 2. Of those that a mesh axis runs over, the one named last changes fastest.
Arguments:
- tokens: bfloat16 [24576, 2048], P('sp', 'tp'), may hold values from -6 to 6
- norm_gain: float32 [2048], replicated, may hold values from 0.1 to 1.9
- query_weight: bfloat16 [2048, 512], P('sp', 'tp'), may hold values from -0.125 to 0.125
- key_weight: bfloat16 [2048, 512], P('sp', 'tp'), may hold values from -0.125 to 0.125
- value_weight: bfloat16 [2048, 512], P('sp', 'tp'), may hold values from -0.125 to 0.125
- decay_weight: bfloat16 [2048, 512], P('sp', 'tp'), may hold values from -0.09375 to 0.09375
- removal_weight: bfloat16 [2048, 512], P('sp', 'tp'), may hold values from -0.125 to 0.125
- gate_weight: bfloat16 [2048, 512], P('sp', 'tp'), may hold values from -0.125 to 0.125
- key_gain: float32 [512], P('tp'), may hold values from 0.1 to 1.9
- removal_gain: float32 [512], P('tp'), may hold values from 0.1 to 1.9
- removal_bias: float32 [512], P('tp'), may hold values from -9 to 1
- decay_bias: float32 [512], P('tp'), may hold values from -12.7 to -1.8
- decay_extra: float32 [24576, 512], P('sp', 'tp'), may hold values from 0 to 0.7
- scan_norm_gain: float32 [512], P('tp'), may hold values from 0.1 to 1.9
- conv_value_weight: bfloat16 [2048, 512], P('sp', 'tp'), may hold values from -0.125 to 0.125
- conv_gate_weight: bfloat16 [2048, 512], P('sp', 'tp'), may hold values from -0.125 to 0.125
- conv_kernel: float32 [31, 512], P(None, 'tp'), may hold values from -2 to 2
- conv_bias: float32 [512], P('tp'), may hold values from -2 to 3
- conv_norm_gain: float32 [512], P('tp'), may hold values from 0.1 to 1.9
- out_scan_weight: bfloat16 [512, 2048], P('tp', 'sp'), may hold values from -0.1875 to 0.1875
- out_conv_weight: bfloat16 [512, 2048], P('tp', 'sp'), may hold values from -0.1875 to 0.1875
Outputs:
- mixed: bfloat16 [24576, 2048], P('sp', 'tp')
The draws below stay inside these ranges and needn't reach their ends.
All inputs are finite; a program needn't handle non-finite values.
Results may differ from the reference program's by a relative error of at most 0.0073.
Values may be sent and summed in bfloat16 or wider, within the bound.
A program may use at most 64 MiB of HBM per device.

```python
import math
import jax
import jax.numpy as jnp
from jax import lax

MODEL = 2048
HEADS = 8
HEAD_SIZE = 64
CONV_K = 31
TOK_DEV = 192
WIDTH = 512
TOKENS = 24576


def head_ranks(key):
    return jax.random.permutation(jax.random.fold_in(key, 5), HEADS)


def slow_count():
    return HEADS // 2


def draw_decay_bias(key, part):
    ranks = head_ranks(key)
    jitter_key = jax.random.fold_in(key, 11)
    slow_heads = ranks < slow_count()
    jitter = jax.random.uniform(jitter_key, (WIDTH,), jnp.float32, -0.7, 0.7)
    centers = jnp.repeat(jnp.where(slow_heads, -12.0, -2.5), HEAD_SIZE)
    return (centers + jitter).astype(jnp.float32)


def draw_removal_bias(key, part):
    ranks = head_ranks(key)
    jitter_key = jax.random.fold_in(key, 13)
    lasting = max(1, HEADS // 4)
    keeping = ranks < lasting
    jitter = jax.random.uniform(jitter_key, (WIDTH,), jnp.float32, -1.0, 1.0)
    centers = jnp.repeat(jnp.where(keeping, -8.0, 0.0), HEAD_SIZE)
    return (centers + jitter).astype(jnp.float32)


def draw_decay_extra(key, part):
    keys = jax.random.split(jax.random.fold_in(key, 23), 3)
    spans = TOKENS // TOK_DEV
    levels = jnp.exp(jax.random.uniform(keys[0], (spans, HEADS), jnp.float32, math.log(3e-06), math.log(2.4e-05)))
    baseline = jnp.repeat(jnp.repeat(levels, TOK_DEV, axis=0), HEAD_SIZE, axis=1)
    places = jax.random.randint(keys[1], (3,), 0, TOKENS)
    hits = jnp.any(jnp.arange(TOKENS)[:, None] == places[None, :], axis=1)
    lowest = 0.22
    sizes = jnp.repeat(jax.random.uniform(keys[2], (TOKENS, HEADS), jnp.float32, lowest, 0.69), HEAD_SIZE, axis=1)
    return (baseline + jnp.where(hits[:, None], sizes, 0.0)).astype(jnp.float32)


def draw_conv_kernel(key, part):
    keys = jax.random.split(jax.random.fold_in(key, 37), 2)
    reach = 0.8
    rising = jnp.exp(jnp.linspace(-reach, reach, WIDTH))
    jitter = jnp.exp(jax.random.uniform(keys[0], (WIDTH,), jnp.float32, -0.3, 0.3))
    taps = jax.random.normal(keys[1], (CONV_K, WIDTH), jnp.float32) * CONV_K ** (-0.5)
    return jnp.clip(taps * rising * jitter, -2.0, 2.0).astype(jnp.float32)


def draw_conv_bias(key, part):
    jitter = jax.random.uniform(jax.random.fold_in(key, 41), (WIDTH,), jnp.float32, -0.4, 0.4)
    rising = jnp.linspace(-1.5, 1.5, WIDTH)
    return jnp.clip(rising + jitter, -2.0, 3.0).astype(jnp.float32)


def steps_of(rng, dims, cuts, low, high):
    loudness = 1.0
    for position, blocks in cuts:
        steps = jax.random.uniform(jax.random.fold_in(jax.random.fold_in(rng, 6), position), (blocks,), jnp.float32, low / len(cuts), high / len(cuts))
        loudness = loudness * jnp.repeat(jnp.exp(steps), dims[position] // blocks).reshape((-1,) + (1,) * (len(dims) - 1 - position))
    return loudness


def noise(key, shape, width, most, cuts=(), kind=jnp.bfloat16):
    result = jax.random.normal(key, shape, jnp.float32) * width
    if len(cuts) > 0:
        result = steps_of(key, shape, cuts, -0.22, 0.18) * result
    return jnp.clip(result, min=-most, max=most).astype(kind)


def setup_inputs(seed: int = 0) -> dict:
    key_of = jax.random.split(jax.random.key(seed), 22)
    return {
        "tokens": noise(key_of[0], (TOKENS, MODEL), 1.0, 6.0, ((0, 128), (1, 4))),
        "norm_gain": jnp.clip(1.0 + 0.18 * jax.random.normal(key_of[1], (MODEL,), jnp.float32), 0.1, 1.9),
        "query_weight": noise(key_of[2], (MODEL, WIDTH), MODEL ** -0.5, 0.125, ((0, 128), (1, 4))),
        "key_weight": noise(key_of[3], (MODEL, WIDTH), MODEL ** -0.5, 0.125, ((0, 128), (1, 4))),
        "value_weight": noise(key_of[4], (MODEL, WIDTH), MODEL ** -0.5, 0.125, ((0, 128), (1, 4))),
        "decay_weight": noise(key_of[5], (MODEL, WIDTH), (2 * MODEL) ** -0.5, 0.09375, ((0, 128), (1, 4))),
        "removal_weight": noise(key_of[6], (MODEL, WIDTH), MODEL ** -0.5, 0.125, ((0, 128), (1, 4))),
        "gate_weight": noise(key_of[7], (MODEL, WIDTH), MODEL ** -0.5, 0.125, ((0, 128), (1, 4))),
        "key_gain": jnp.clip(1.0 + 0.18 * jax.random.normal(key_of[8], (WIDTH,), jnp.float32), 0.1, 1.9),
        "removal_gain": jnp.clip(1.0 + 0.18 * jax.random.normal(key_of[9], (WIDTH,), jnp.float32), 0.1, 1.9),
        "removal_bias": draw_removal_bias(jax.random.fold_in(key_of[21], 71), 0),
        "decay_bias": draw_decay_bias(jax.random.fold_in(key_of[21], 71), 0),
        "decay_extra": draw_decay_extra(jax.random.fold_in(key_of[21], 71), 0),
        "scan_norm_gain": jnp.clip(1.0 + 0.18 * jax.random.normal(key_of[13], (WIDTH,), jnp.float32), 0.1, 1.9),
        "conv_value_weight": noise(key_of[14], (MODEL, WIDTH), MODEL ** -0.5, 0.125, ((0, 128), (1, 4))),
        "conv_gate_weight": noise(key_of[15], (MODEL, WIDTH), MODEL ** -0.5, 0.125, ((0, 128), (1, 4))),
        "conv_kernel": draw_conv_kernel(jax.random.fold_in(key_of[21], 71), 0),
        "conv_bias": draw_conv_bias(jax.random.fold_in(key_of[21], 71), 0),
        "conv_norm_gain": jnp.clip(1.0 + 0.18 * jax.random.normal(key_of[18], (WIDTH,), jnp.float32), 0.1, 1.9),
        "out_scan_weight": noise(key_of[19], (WIDTH, MODEL), (2 * WIDTH) ** -0.5, 0.1875, ((0, 4), (1, 128))),
        "out_conv_weight": noise(key_of[20], (WIDTH, MODEL), (2 * WIDTH) ** -0.5, 0.1875, ((0, 4), (1, 128))),
    }


def reference(tokens, norm_gain, query_weight, key_weight, value_weight, decay_weight, removal_weight, gate_weight, key_gain, removal_gain, removal_bias, decay_bias, decay_extra, scan_norm_gain, conv_value_weight, conv_gate_weight, conv_kernel, conv_bias, conv_norm_gain, out_scan_weight, out_conv_weight):
    exact_setting = lax.Precision.HIGHEST
    floats = tokens.astype(jnp.float32)
    normed = (floats * lax.rsqrt(lax.optimization_barrier(jnp.mean(floats * floats, axis=-1, keepdims=True)) + 1e-06) * norm_gain).astype(jnp.bfloat16)
    matrices = (query_weight, key_weight, value_weight, decay_weight, removal_weight, gate_weight, conv_value_weight, conv_gate_weight)
    stored = tuple((jnp.dot(normed, matrix, preferred_element_type=jnp.float32).astype(jnp.bfloat16) for matrix in matrices))
    stored = lax.optimization_barrier(stored)
    recept, key_rows, value_rows, decay_pre, removal_pre, gate_pre, conv_value, conv_gate = [item.astype(jnp.float32) for item in stored]
    decay_rate = jnp.exp(-jax.nn.softplus(-(decay_bias + decay_pre)) - 0.5) + decay_extra
    decay_factor = jnp.exp(-decay_rate)
    removal = jax.nn.sigmoid(removal_bias + removal_pre)

    def split_heads(table):
        return table.reshape(TOKENS, HEADS, HEAD_SIZE)
    scaled = split_heads(key_rows * key_gain)
    unit_keys = scaled * lax.rsqrt(lax.optimization_barrier(jnp.sum(scaled * scaled, axis=-1, keepdims=True)) + 1e-06)
    written = key_rows * (1.0 + (removal - 1.0) * removal_gain)

    def advance(memory, inputs):
        recept_t, decay_t, written_t, value_t, unit_t, removal_t = inputs
        removed_value = jnp.einsum('hvk,hk->hv', memory, -unit_t, precision=exact_setting)
        memory = memory * decay_t[:, None, :] + removed_value[:, :, None] * (unit_t * removal_t)[:, None, :] + value_t[:, :, None] * written_t[:, None, :]
        return (memory, jnp.einsum('hvk,hk->hv', memory, recept_t, precision=exact_setting))
    initial = jnp.zeros((HEADS, HEAD_SIZE, HEAD_SIZE), jnp.float32)
    _, reads = lax.scan(advance, initial, (split_heads(recept), split_heads(decay_factor), split_heads(written), split_heads(value_rows), unit_keys, split_heads(removal)))
    center = lax.optimization_barrier(jnp.mean(reads, axis=-1, keepdims=True))
    spread = lax.optimization_barrier(jnp.mean((reads - center) ** 2, axis=-1, keepdims=True))
    normalized = ((reads - center) * lax.rsqrt(spread + 0.00064)).reshape(TOKENS, WIDTH)
    scan_out = (normalized * scan_norm_gain * jax.nn.sigmoid(gate_pre)).astype(jnp.bfloat16)
    conv_input = (conv_value * jax.nn.sigmoid(conv_gate)).astype(jnp.bfloat16)
    padded = jnp.concatenate([jnp.zeros((CONV_K - 1, WIDTH), jnp.float32), conv_input.astype(jnp.float32)], axis=0)
    filtered = conv_bias + conv_kernel[0] * padded[0:TOKENS]
    for index in range(1, CONV_K):
        filtered = filtered + conv_kernel[index] * padded[index:index + TOKENS]
    channel_mean = lax.optimization_barrier(jnp.mean(filtered, axis=-1, keepdims=True))
    channel_var = lax.optimization_barrier(jnp.mean((filtered - channel_mean) ** 2, axis=-1, keepdims=True))
    conv_out = jax.nn.silu((filtered - channel_mean) * lax.rsqrt(channel_var + 1e-05) * conv_norm_gain).astype(jnp.bfloat16)
    total = jnp.dot(scan_out, out_scan_weight, preferred_element_type=jnp.float32) + jnp.dot(conv_out, out_conv_weight, preferred_element_type=jnp.float32)
    return total.astype(jnp.bfloat16)
```

```python
import functools
import math

import jax
import jax.numpy as jnp
from jax import lax
from jax.experimental import pallas as pl
from jax.experimental.pallas import tpu as pltpu
from jax.sharding import Mesh
from jax.sharding import PartitionSpec as P

F32 = jnp.float32
BF16 = jnp.bfloat16
SP = ("sp_0", "sp_1", "sp_2")
MESH = pl.DeviceIdType.MESH
CONV_K = 31
ROWS = 192
BLOCK = 64
BLOCKS = ROWS // BLOCK
MODEL = 2048
NX = 4
PROJ = 1024
CHUNK = 1280
N = 8


def split2(a):
    high = a.astype(BF16)
    return high, (a - high.astype(F32)).astype(BF16)


def one(a, b):
    return jnp.dot(a.astype(BF16), b.astype(BF16), preferred_element_type=F32)


def one_nt(a, b):
    return lax.dot_general(
        a.astype(BF16), b.astype(BF16), (((1,), (1,)), ((), ())), preferred_element_type=F32
    )


def three(a, b):
    ah, al = split2(a)
    bh, bl = split2(b)
    return one(ah, bh) + one(al, bh) + one(ah, bl)


def three_nt(a, b):
    ah, al = split2(a)
    bh, bl = split2(b)
    return one_nt(ah, bh) + one_nt(al, bh) + one_nt(ah, bl)


def left_exact(a, b):
    bh, bm = split2(b)
    bl = (b - bh.astype(F32) - bm.astype(F32)).astype(BF16)
    return one(a, bh) + one(a, bm) + one(a, bl)


def right_exact(a, b):
    ah, al = split2(a)
    return one(ah, b) + one(al, b)


def iotas(rows, columns):
    return (
        lax.broadcasted_iota(jnp.int32, (rows, columns), 0),
        lax.broadcasted_iota(jnp.int32, (rows, columns), 1),
    )


def sigmoid(x):
    return 1.0 / (1.0 + jnp.exp(-x))


def head_ones():
    i, j = iotas(128, 128)
    return ((i >> 6) == (j >> 6)).astype(BF16)


def local_scan(
    recept, keys, values, decay_pre, removal_pre, key_gain, removal_gain, removal_bias, decay_bias, extra
):
    ones = head_ones()
    rate = sigmoid(decay_bias + decay_pre) * math.exp(-0.5) + extra
    removal = sigmoid(removal_bias + removal_pre)
    scaled = keys * key_gain
    unit = scaled * lax.rsqrt(right_exact(scaled * scaled, ones) + 1e-06)
    written = keys * (1.0 + (removal - 1.0) * removal_gain)
    beta = unit * removal
    i, j = iotas(BLOCK, BLOCK)
    lower = (i >= j).astype(BF16)

    lane = lax.broadcasted_iota(jnp.int32, (BLOCK, 128), 1)
    first = lane < 64

    def spread(a):
        return jnp.concatenate([jnp.where(first, a, 0.0), jnp.where(first, 0.0, a)], axis=0)

    i, j = iotas(128, 128)
    same_head = (i >> 6) == (j >> 6)
    inclusive = same_head & (i >= j)
    strict = same_head & (i > j)
    eye = (i == j).astype(F32)
    sames = [(i >> s) == (j >> s) for s in (3, 4, 5)] + [same_head]

    parts = []
    for b in range(BLOCKS):
        rows = slice(b * BLOCK, (b + 1) * BLOCK)
        rate_b = rate[rows]
        falling = -left_exact(lower, rate_b)
        before = falling + rate_b
        middle = falling[BLOCK // 2 : BLOCK // 2 + 1]
        ending = falling[BLOCK - 1 :]
        up = jnp.exp(middle - falling)
        alpha_mid = -unit[rows] * jnp.exp(before - middle)
        recept_mid = recept[rows] * jnp.exp(falling - middle)
        beta_mid = beta[rows] * up
        keys_mid = written[rows] * up
        to_end = jnp.exp(ending - falling)
        end_decay = jnp.exp(ending)
        start_alpha = spread(-unit[rows] * jnp.exp(before))
        start_recept = spread(recept[rows] * jnp.exp(falling))
        end_beta = spread(beta[rows] * to_end)
        end_keys = spread(written[rows] * to_end)
        values_b = spread(values[rows])
        left = jnp.concatenate([spread(alpha_mid), spread(recept_mid)], axis=0)
        right = jnp.concatenate([beta_mid, beta_mid, keys_mid, keys_mid], axis=0)
        pairs = three_nt(left, right)
        alpha_beta = jnp.where(strict, pairs[:128, :128], 0.0)
        alpha_keys = jnp.where(strict, pairs[:128, 128:], 0.0)
        recept_beta = jnp.where(inclusive, pairs[128:, :128], 0.0)
        recept_keys = jnp.where(inclusive, pairs[128:, 128:], 0.0)
        local = three(jnp.concatenate([alpha_keys, recept_keys], axis=0), values_b)
        base = jnp.where(sames[0], alpha_beta, 0.0)
        inverse = eye + base
        power = three(base, base)
        inverse = inverse + three(inverse, power)
        power = three(power, power)
        inverse = inverse + three(inverse, power)
        for s in range(3):
            off = jnp.where(sames[s + 1] & ~sames[s], alpha_beta, 0.0)
            inverse = inverse + three(inverse, three(off, inverse))
        gathered = three(inverse, jnp.concatenate([start_alpha, local[:128]], axis=1))
        step = three(end_beta.T, gathered)
        step_a = step[:, :128] + jnp.where(i == j, end_decay, 0.0)
        step_b = step[:, 128:] + three(end_keys.T, values_b)
        reads = three(recept_beta, gathered)
        read_a = reads[:, :128] + start_recept
        read_b = reads[:, 128:] + local[128:]
        parts.append(
            (step_a, step_b, read_a[:64] + read_a[64:], read_b[:64] + read_b[64:])
        )
    trans_a, trans_b = parts[0][0], parts[0][1]
    reads_a, reads_b = [parts[0][2]], [parts[0][3]]
    for b in range(1, BLOCKS):
        step_a, step_b, read_a, read_b = parts[b]
        both = jnp.concatenate([trans_a, trans_b], axis=1)
        seen = three(read_a, both)
        reads_a.append(seen[:, :128])
        reads_b.append(seen[:, 128:] + read_b)
        moved = three(step_a, both)
        trans_a, trans_b = moved[:, :128], moved[:, 128:] + step_b
    return (
        trans_a,
        trans_b,
        jnp.concatenate(reads_a, axis=0),
        jnp.concatenate(reads_b, axis=0),
    )


def packed_heads(trans_a, trans_b):
    lane = lax.broadcasted_iota(jnp.int32, (64, 128), 1)
    head0 = jnp.where(lane < 64, trans_a[:64], pltpu.roll(trans_b[:64], 64, 1))
    head1 = jnp.where(lane < 64, pltpu.roll(trans_a[64:], 64, 1), trans_b[64:])
    return head0, head1


def combine(later, total):
    lane = lax.broadcasted_iota(jnp.int32, later.shape, 1)
    return three(later[:, :64], total) + jnp.where(lane < 64, 0.0, later)


def kernel(
    tokens,
    norm_gain,
    w0,
    w1,
    w2,
    w3,
    w4,
    w5,
    w6,
    w7,
    out_scan,
    out_conv,
    key_gain,
    removal_gain,
    removal_bias,
    decay_bias,
    extra,
    scan_norm_gain,
    conv_kernel,
    conv_bias,
    conv_norm_gain,
    out,
    weights,
    tok,
    normed,
    proj,
    outw,
    pair_in,
    line_y,
    line_z,
    state_in,
    state_out,
    pair_out,
    rim,
    conv_in,
    conv_pad,
    stats,
    feats_scan,
    feats_conv,
    reads_a,
    reads_b,
    mine,
    load_sem,
    tok_send,
    tok_recv,
    first_send,
    first_recv,
    second_send,
    plus_recv,
    minus_recv,
    cross_send,
    cross_recv,
    outw_send,
    outw_recv,
    outw_load,
    pair_send,
    pair_recv,
    y_send,
    y_recv,
    z_send,
    z_recv,
    state_send,
    state_recv,
    rim_send,
    rim_recv,
    stats_send,
    stats_recv,
    scan_send,
    scan_recv,
    conv_send,
    conv_recv,
):
    z, y, c, x = (lax.axis_index(n) for n in (*SP, "tp"))

    def at(z_=None, y_=None, c_=None, x_=None):
        pick = lambda a, b: a if b is None else b
        return (pick(z, z_), pick(y, y_), pick(c, c_), pick(x, x_))

    def remote(src, dst, send, recv, where):
        return pltpu.make_async_remote_copy(
            src_ref=src, dst_ref=dst, send_sem=send, recv_sem=recv, device_id=where, device_id_type=MESH
        )

    partner = at(c_=1 - c)

    loads = [
        pltpu.make_async_copy(tokens, tok.at[x], load_sem.at[0]),
    ]
    for k, w in enumerate((w0, w1, w2, w3, w4, w5, w6, w7)):
        loads.append(
            pltpu.make_async_copy(
                w, weights.at[z, y, c, :, pl.ds(128 * k, 128)], load_sem.at[k + 1]
            )
        )
    for load in loads:
        load.start()
    weights[z, y, c, :, pl.ds(1024, 128)] = out_scan[...].astype(F32).T.astype(BF16)
    weights[z, y, c, :, pl.ds(1152, 128)] = out_conv[...].astype(F32).T.astype(BF16)

    barrier = pltpu.get_barrier_semaphore()
    greeted = [partner]
    for k in range(1, N):
        greeted.append(at(y_=lax.rem(y + k, N)))
        greeted.append(at(z_=lax.rem(z + k, N)))
    for k in range(1, NX):
        greeted.append(at(x_=lax.rem(x + k, NX)))
    place = (z * N + y) * 2 + c
    size = 2 * N * N
    before = lax.rem(place + size - 1, size)
    after = lax.rem(place + 1, size)
    as_device = lambda s: (s // (2 * N), lax.rem(s // 2, N), lax.rem(s, 2), x)
    greeted.append(as_device(before))
    for device in greeted:
        pl.semaphore_signal(barrier, inc=1, device_id=device, device_id_type=MESH)
    pl.semaphore_wait(barrier, len(greeted))
    for load in loads:
        load.wait()

    tok_copies = []
    for k in (1, 3, 2):
        tok_copies.append(
            remote(tok.at[x], tok.at[x], tok_send.at[k - 1], tok_recv.at[k - 1], at(x_=lax.rem(x + k, NX)))
        )
    a = (1 - c) * y + c * z
    b = (1 - c) * z + c * y

    def along_first(k):
        return at(z_=lax.rem(z + c * k, N), y_=lax.rem(y + (1 - c) * k, N))

    def along_second(k):
        return at(z_=lax.rem(z + (1 - c) * k, N), y_=lax.rem(y + c * k, N))

    def slot(from_first, from_second):
        a_ = lax.rem(a + N - from_first, N)
        b_ = lax.rem(b + N - from_second, N)
        z_ = (1 - c) * b_ + c * a_
        y_ = (1 - c) * a_ + c * b_
        return weights.at[z_, y_, c]

    own = slot(0, 0)
    order = (1, 7, 2, 6, 3, 5, 4)
    for k in order:
        remote(own, own, first_send, first_recv.at[k - 1], along_first(k)).start()
    for copy in tok_copies:
        copy.start()

    def push(k, d, sign, ref):
        recv = (plus_recv if sign > 0 else minus_recv).at[k * 4 + d]
        remote(ref, ref, second_send, recv, along_second(1 if sign > 0 else N - 1)).start()

    def arrived(k, d, sign):
        ref = slot(k, d if sign > 0 else N - d)
        if d == 0:
            if k:
                remote(ref, ref, first_send, first_recv.at[k - 1], along_first(k)).wait_recv()
            push(k, 0, 1, ref)
            push(k, 0, -1, ref)
        else:
            recv = (plus_recv if sign > 0 else minus_recv).at[k * 4 + d - 1]
            remote(ref, ref, second_send, recv, partner).wait_recv()
            if d < 3 or (d == 3 and (k % 2 == 0) == (sign > 0)):
                push(k, d, sign, ref)
        remote(ref, ref, cross_send, cross_recv, partner).start()

    events = []
    for k in range(N):
        near = min(k, N - k)
        events.append((near, 0, k, 1))
        for d in range(1, 5):
            for sign in (1, -1):
                if d < 4 or (k % 2 == 0) == (sign > 0):
                    events.append((near + d, d, k, sign))
    events.sort()

    normed_at = len(events) * 5 // 8
    for number, (_, d, k, sign) in enumerate(events):
        arrived(k, d, sign)
        if number == normed_at:
            for copy in tok_copies:
                copy.wait_recv()
            square = jnp.zeros((ROWS, 1), F32)
            for q in range(NX):
                t = tok[q].astype(F32)
                square = square + jnp.sum(t * t, axis=-1, keepdims=True)
            factor = lax.rsqrt(square * (1.0 / MODEL) + 1e-06)
            for q in range(NX):
                t = tok[q].astype(F32)
                columns = slice(q * 512, (q + 1) * 512)
                normed[:, columns] = (t * factor * norm_gain[:, columns]).astype(BF16)

    everything = weights.at[:, :, 1 - c]
    remote(everything, everything, cross_send, cross_recv, partner).wait_recv()

    outw_copies = []
    for k in (1, 3, 2):
        x_ = lax.rem(x + k, NX)
        outw_copies.append(
            remote(
                weights.at[pl.ds(2 * x_, 2), :, :, :, pl.ds(1024, 256)],
                outw.at[x],
                outw_send.at[k - 1],
                outw_recv.at[k - 1],
                at(x_=x_),
            )
        )
    for copy in outw_copies:
        copy.start()
    outw_own = pltpu.make_async_copy(
        weights.at[pl.ds(2 * x, 2), :, :, :, pl.ds(1024, 256)], outw.at[x], outw_load
    )
    outw_own.start()

    def project(n, carry):
        columns = pl.ds(pl.multiple_of(n * 256, 256), 256)
        w = weights[:, :, :, :, columns].reshape(MODEL, 256)
        proj[:, columns] = jnp.dot(normed[...], w, preferred_element_type=F32).astype(BF16)
        return carry

    lax.fori_loop(0, PROJ // 256, project, 0)

    def part(k):
        return proj[:, 128 * k : 128 * (k + 1)].astype(F32)

    conv_in[...] = (part(6) * sigmoid(part(7))).astype(BF16)
    last = place == size - 1
    start = place == 0
    rim_copy = remote(
        conv_in.at[pl.ds(ROWS - 32, 32)], rim, rim_send, rim_recv, as_device(after)
    )

    @pl.when(jnp.logical_not(last))
    def _():
        rim_copy.start()

    trans_a, trans_b, ra, rb = local_scan(
        part(0),
        part(1),
        part(2),
        part(3),
        part(4),
        key_gain[...],
        removal_gain[...],
        removal_bias[...],
        decay_bias[...],
        extra[...],
    )
    reads_a[...] = ra
    reads_b[...] = rb
    head0, head1 = packed_heads(trans_a, trans_b)
    upper = c == 1
    pair_out[...] = jnp.where(upper, head0, head1)
    mine[...] = jnp.where(upper, head1, head0)
    pair_copy = remote(pair_out, pair_in, pair_send, pair_recv, partner)
    pair_copy.start()
    pair_copy.wait_recv()
    earlier = jnp.where(upper, pair_in[...], mine[...])
    later = jnp.where(upper, mine[...], pair_in[...])
    line_y[y] = combine(later, earlier)
    for k in (4, 3, 5, 2, 6, 1, 7):
        remote(line_y.at[y], line_y.at[y], y_send, y_recv.at[y], at(y_=lax.rem(y + k, N))).start()

    @pl.when(start)
    def _():
        rim[...] = jnp.zeros_like(rim)

    @pl.when(jnp.logical_not(start))
    def _():
        rim_copy.wait_recv()

    conv_pad[pl.ds(0, 32)] = rim[...].astype(F32)
    conv_pad[pl.ds(32, ROWS)] = conv_in[...].astype(F32)
    filtered = conv_bias[...] + conv_kernel[0:1] * conv_pad[pl.ds(2, ROWS)]
    for k in range(1, CONV_K):
        filtered = filtered + conv_kernel[k : k + 1] * conv_pad[pl.ds(2 + k, ROWS)]
    near = jnp.mean(filtered, axis=-1, keepdims=True)
    around = jnp.sum((filtered - near) ** 2, axis=-1, keepdims=True)
    lane = lax.broadcasted_iota(jnp.int32, (ROWS, 128), 1)
    stats[x] = jnp.where(lane < 64, near, around)
    conv_pad[pl.ds(0, ROWS)] = filtered
    stats_copies = [
        remote(stats.at[x], stats.at[x], stats_send.at[k - 1], stats_recv.at[k - 1], at(x_=lax.rem(x + k, NX)))
        for k in (1, 3, 2)
    ]
    for copy in stats_copies:
        copy.start()

    lane = lax.broadcasted_iota(jnp.int32, (64, 128), 1)
    i, j = iotas(64, 128)
    blank = (i == j).astype(F32)
    total = inside = blank
    for k in range(N):

        @pl.when(y != k)
        def _():
            remote(line_y.at[k], line_y.at[k], y_send, y_recv.at[k], partner).wait_recv()

        total = combine(line_y[k], total)
        inside = jnp.where(k < y, total, inside)
    line_z[z] = total
    z_copies = []
    for k in range(N - 1, 0, -1):
        copy = remote(
            line_z.at[z], line_z.at[z], z_send.at[k - 1], z_recv.at[z], at(z_=lax.rem(z + k, N))
        )
        z_copies.append((k, copy))

        @pl.when(z + k < N)
        def _():
            copy.start()

    for copy in stats_copies:
        copy.wait_recv()
    center = jnp.zeros((ROWS, 1), F32)
    for q in range(NX):
        center = center + stats[q][:, 0:1]
    center = center * (1.0 / NX)
    spread = jnp.zeros((ROWS, 1), F32)
    for q in range(NX):
        gap = stats[q][:, 0:1] - center
        spread = spread + stats[q][:, 64:65] + 128.0 * gap * gap
    spread = spread * (1.0 / 512.0)
    normal = (conv_pad[pl.ds(0, ROWS)] - center) * lax.rsqrt(spread + 1e-05) * conv_norm_gain[...]
    feats_conv[x] = (normal * sigmoid(normal)).astype(BF16)
    conv_copies = [
        remote(
            feats_conv.at[x], feats_conv.at[x], conv_send.at[k - 1], conv_recv.at[k - 1], at(x_=lax.rem(x + k, NX))
        )
        for k in (1, 3, 2)
    ]
    for copy in conv_copies:
        copy.start()

    def advance(k, state):
        remote(line_z.at[k], line_z.at[k], z_send.at[0], z_recv.at[k], partner).wait_recv()
        return combine(line_z[k], state)

    state = lax.fori_loop(0, z, advance, jnp.zeros((64, 128), F32))
    state = jnp.where(lane < 64, 0.0, combine(inside, state))
    passed = combine(jnp.where(upper, pair_in[...], mine[...]), state)
    here = jnp.where(upper, passed, state)
    state_out[...] = jnp.where(upper, state, passed)
    state_copy = remote(state_out, state_in, state_send, state_recv, partner)
    state_copy.start()

    for copy in conv_copies:
        copy.wait_recv()
    for copy in outw_copies:
        copy.wait_recv()
    outw_own.wait()
    w_of = lambda q, h: outw[q, :, :, :, :, pl.ds(128 * h, 128)].reshape(512, 128)
    total_out = one_nt(feats_conv[0], w_of(0, 1))
    for q in range(1, NX):
        total_out = total_out + one_nt(feats_conv[q], w_of(q, 1))

    state_copy.wait_recv()
    there = state_in[...]
    state0 = jnp.where(upper, there, here)
    state1 = jnp.where(upper, here, there)
    whole = jnp.concatenate(
        [
            jnp.where(lane < 64, pltpu.roll(state0, 64, 1), 0.0),
            jnp.where(lane < 64, 0.0, state1),
        ],
        axis=0,
    )
    reads = three(reads_a[...], whole) + reads_b[...]
    ones = head_ones()
    reads = reads - right_exact(reads, ones) * (1.0 / 64.0)
    spread = right_exact(reads * reads, ones) * (1.0 / 64.0)
    feats_scan[x] = (
        reads * lax.rsqrt(spread + 0.00064) * scan_norm_gain[...] * sigmoid(part(5))
    ).astype(BF16)
    scan_copies = [
        remote(
            feats_scan.at[x], feats_scan.at[x], scan_send.at[k - 1], scan_recv.at[k - 1], at(x_=lax.rem(x + k, NX))
        )
        for k in (1, 3, 2)
    ]
    for copy in scan_copies:
        copy.start()
    for copy in scan_copies:
        copy.wait_recv()
    for q in range(NX):
        total_out = total_out + one_nt(feats_scan[q], w_of(q, 0))
    out[...] = total_out.astype(BF16)

    for copies in (tok_copies, outw_copies, stats_copies, conv_copies, scan_copies):
        for copy in copies:
            copy.wait_send()
    pair_copy.wait_send()
    state_copy.wait_send()
    seven = weights.at[pl.ds(0, 7), 0, 0]
    remote(seven, seven, first_send, first_recv.at[0], partner).wait_send()
    most = weights.at[pl.ds(0, 7), :, 0]
    remote(most, most, second_send, plus_recv.at[0], partner).wait_send()
    remote(everything, everything, cross_send, cross_recv, partner).wait_send()
    lines = line_y.at[pl.ds(0, 7)]
    remote(lines, lines, y_send, y_recv.at[0], partner).wait_send()

    @pl.when(jnp.logical_not(last))
    def _():
        rim_copy.wait_send()

    for k, copy in z_copies:

        @pl.when(z + k < N)
        def _():
            copy.wait_send()


def shards(
    tokens,
    norm_gain,
    query_weight,
    key_weight,
    value_weight,
    decay_weight,
    removal_weight,
    gate_weight,
    key_gain,
    removal_gain,
    removal_bias,
    decay_bias,
    decay_extra,
    scan_norm_gain,
    conv_value_weight,
    conv_gate_weight,
    conv_kernel,
    conv_bias,
    conv_norm_gain,
    out_scan_weight,
    out_conv_weight,
):
    row = lambda v: v.reshape(1, -1)
    anywhere = pl.BlockSpec(memory_space=pl.ANY)
    inside = pl.BlockSpec(memory_space=pltpu.VMEM)
    dma = pltpu.SemaphoreType.DMA
    return pl.pallas_call(
        kernel,
        out_shape=jax.ShapeDtypeStruct((ROWS, 512), BF16),
        in_specs=[anywhere] + [inside] + [anywhere] * 8 + [inside] * 11,
        out_specs=inside,
        scratch_shapes=[
            pltpu.VMEM((N, N, 2, 16, CHUNK), BF16),
            pltpu.VMEM((NX, ROWS, 512), BF16),
            pltpu.VMEM((ROWS, MODEL), BF16),
            pltpu.VMEM((ROWS, PROJ), BF16),
            pltpu.VMEM((NX, 2, N, 2, 16, 256), BF16),
            pltpu.VMEM((64, 128), F32),
            pltpu.VMEM((N, 64, 128), F32),
            pltpu.VMEM((N, 64, 128), F32),
            pltpu.VMEM((64, 128), F32),
            pltpu.VMEM((64, 128), F32),
            pltpu.VMEM((64, 128), F32),
            pltpu.VMEM((32, 128), BF16),
            pltpu.VMEM((ROWS, 128), BF16),
            pltpu.VMEM((ROWS + 32, 128), F32),
            pltpu.VMEM((NX, ROWS, 128), F32),
            pltpu.VMEM((NX, ROWS, 128), BF16),
            pltpu.VMEM((NX, ROWS, 128), BF16),
            pltpu.VMEM((ROWS, 128), F32),
            pltpu.VMEM((ROWS, 128), F32),
            pltpu.VMEM((64, 128), F32),
            dma((9,)),
            dma((3,)),
            dma((3,)),
            dma(()),
            dma((7,)),
            dma(()),
            dma((32,)),
            dma((32,)),
            dma(()),
            dma(()),
            dma((3,)),
            dma((3,)),
            dma(()),
            dma(()),
            dma(()),
            dma(()),
            dma((N,)),
            dma((N - 1,)),
            dma((N,)),
            dma(()),
            dma(()),
            dma(()),
            dma(()),
            dma((3,)),
            dma((3,)),
            dma((3,)),
            dma((3,)),
            dma((3,)),
            dma((3,)),
        ],
        compiler_params=pltpu.CompilerParams(
            collective_id=0, has_side_effects=True, vmem_limit_bytes=56 * 1024 * 1024
        ),
    )(
        tokens,
        row(norm_gain),
        query_weight,
        key_weight,
        value_weight,
        decay_weight,
        removal_weight,
        gate_weight,
        conv_value_weight,
        conv_gate_weight,
        out_scan_weight,
        out_conv_weight,
        row(key_gain),
        row(removal_gain),
        row(removal_bias),
        row(decay_bias),
        decay_extra,
        row(scan_norm_gain),
        conv_kernel,
        row(conv_bias),
        row(conv_norm_gain),
    )


def solution(mesh):
    torus = Mesh(mesh.devices.reshape(N, N, 2, mesh.shape["tp"]), (*SP, "tp"))
    in_specs = (
        P(SP, "tp"),
        P(),
        P(SP, "tp"),
        P(SP, "tp"),
        P(SP, "tp"),
        P(SP, "tp"),
        P(SP, "tp"),
        P(SP, "tp"),
        P("tp"),
        P("tp"),
        P("tp"),
        P("tp"),
        P(SP, "tp"),
        P("tp"),
        P(SP, "tp"),
        P(SP, "tp"),
        P(None, "tp"),
        P("tp"),
        P("tp"),
        P("tp", SP),
        P("tp", SP),
    )
    return jax.shard_map(
        shards, mesh=torus, in_specs=in_specs, out_specs=P(SP, "tp"), check_vma=False
    )
```

```python
import functools
import math

import jax
import jax.numpy as jnp
from jax import lax
from jax.experimental import pallas as pl
from jax.experimental.pallas import tpu as pltpu
from jax.sharding import Mesh
from jax.sharding import PartitionSpec as P

F32 = jnp.float32
BF16 = jnp.bfloat16
SP = ("sp_0", "sp_1", "sp_2")
MESH = pl.DeviceIdType.MESH
CONV_K = 31
ROWS = 192
BLOCK = 64
BLOCKS = ROWS // BLOCK
MODEL = 2048
NX = 4
PROJ = 1024
N = 8


def split2(a):
    high = a.astype(BF16)
    return high, (a - high.astype(F32)).astype(BF16)


def one(a, b):
    return jnp.dot(a.astype(BF16), b.astype(BF16), preferred_element_type=F32)


def one_nt(a, b):
    return lax.dot_general(
        a.astype(BF16), b.astype(BF16), (((1,), (1,)), ((), ())), preferred_element_type=F32
    )


def three(a, b):
    ah, al = split2(a)
    bh, bl = split2(b)
    return one(ah, bh) + one(al, bh) + one(ah, bl)


def three_nt(a, b):
    ah, al = split2(a)
    bh, bl = split2(b)
    return one_nt(ah, bh) + one_nt(al, bh) + one_nt(ah, bl)


def left_exact(a, b):
    bh, bm = split2(b)
    bl = (b - bh.astype(F32) - bm.astype(F32)).astype(BF16)
    return one(a, bh) + one(a, bm) + one(a, bl)


def right_exact(a, b):
    ah, al = split2(a)
    return one(ah, b) + one(al, b)


def iotas(rows, columns):
    return (
        lax.broadcasted_iota(jnp.int32, (rows, columns), 0),
        lax.broadcasted_iota(jnp.int32, (rows, columns), 1),
    )


def sigmoid(x):
    return 1.0 / (1.0 + jnp.exp(-x))


def head_ones():
    i, j = iotas(128, 128)
    return ((i >> 6) == (j >> 6)).astype(BF16)


def local_scan(
    recept, keys, values, decay_pre, removal_pre, key_gain, removal_gain, removal_bias, decay_bias, extra
):
    ones = head_ones()
    rate = sigmoid(decay_bias + decay_pre) * math.exp(-0.5) + extra
    removal = sigmoid(removal_bias + removal_pre)
    scaled = keys * key_gain
    unit = scaled * lax.rsqrt(right_exact(scaled * scaled, ones) + 1e-06)
    written = keys * (1.0 + (removal - 1.0) * removal_gain)
    beta = unit * removal
    i, j = iotas(BLOCK, BLOCK)
    lower = (i >= j).astype(BF16)

    lane = lax.broadcasted_iota(jnp.int32, (BLOCK, 128), 1)
    first = lane < 64

    def spread(a):
        return jnp.concatenate([jnp.where(first, a, 0.0), jnp.where(first, 0.0, a)], axis=0)

    i, j = iotas(128, 128)
    same_head = (i >> 6) == (j >> 6)
    inclusive = same_head & (i >= j)
    strict = same_head & (i > j)
    eye = (i == j).astype(F32)
    sames = [(i >> s) == (j >> s) for s in (3, 4, 5)] + [same_head]

    parts = []
    for b in range(BLOCKS):
        rows = slice(b * BLOCK, (b + 1) * BLOCK)
        rate_b = rate[rows]
        falling = -left_exact(lower, rate_b)
        before = falling + rate_b
        middle = falling[BLOCK // 2 : BLOCK // 2 + 1]
        ending = falling[BLOCK - 1 :]
        up = jnp.exp(middle - falling)
        alpha_mid = -unit[rows] * jnp.exp(before - middle)
        recept_mid = recept[rows] * jnp.exp(falling - middle)
        beta_mid = beta[rows] * up
        keys_mid = written[rows] * up
        to_end = jnp.exp(ending - falling)
        end_decay = jnp.exp(ending)
        start_alpha = spread(-unit[rows] * jnp.exp(before))
        start_recept = spread(recept[rows] * jnp.exp(falling))
        end_beta = spread(beta[rows] * to_end)
        end_keys = spread(written[rows] * to_end)
        values_b = spread(values[rows])
        left = jnp.concatenate([spread(alpha_mid), spread(recept_mid)], axis=0)
        right = jnp.concatenate([beta_mid, beta_mid, keys_mid, keys_mid], axis=0)
        pairs = three_nt(left, right)
        alpha_beta = jnp.where(strict, pairs[:128, :128], 0.0)
        alpha_keys = jnp.where(strict, pairs[:128, 128:], 0.0)
        recept_beta = jnp.where(inclusive, pairs[128:, :128], 0.0)
        recept_keys = jnp.where(inclusive, pairs[128:, 128:], 0.0)
        local = three(jnp.concatenate([alpha_keys, recept_keys], axis=0), values_b)
        base = jnp.where(sames[0], alpha_beta, 0.0)
        inverse = eye + base
        power = three(base, base)
        inverse = inverse + three(inverse, power)
        power = three(power, power)
        inverse = inverse + three(inverse, power)
        for s in range(3):
            off = jnp.where(sames[s + 1] & ~sames[s], alpha_beta, 0.0)
            inverse = inverse + three(inverse, three(off, inverse))
        gathered = three(inverse, jnp.concatenate([start_alpha, local[:128]], axis=1))
        step = three(end_beta.T, gathered)
        step_a = step[:, :128] + jnp.where(i == j, end_decay, 0.0)
        step_b = step[:, 128:] + three(end_keys.T, values_b)
        reads = three(recept_beta, gathered)
        read_a = reads[:, :128] + start_recept
        read_b = reads[:, 128:] + local[128:]
        parts.append(
            (step_a, step_b, read_a[:64] + read_a[64:], read_b[:64] + read_b[64:])
        )
    trans_a, trans_b = parts[0][0], parts[0][1]
    reads_a, reads_b = [parts[0][2]], [parts[0][3]]
    for b in range(1, BLOCKS):
        step_a, step_b, read_a, read_b = parts[b]
        both = jnp.concatenate([trans_a, trans_b], axis=1)
        seen = three(read_a, both)
        reads_a.append(seen[:, :128])
        reads_b.append(seen[:, 128:] + read_b)
        moved = three(step_a, both)
        trans_a, trans_b = moved[:, :128], moved[:, 128:] + step_b
    return (
        trans_a,
        trans_b,
        jnp.concatenate(reads_a, axis=0),
        jnp.concatenate(reads_b, axis=0),
    )


def packed_heads(trans_a, trans_b):
    lane = lax.broadcasted_iota(jnp.int32, (64, 128), 1)
    head0 = jnp.where(lane < 64, trans_a[:64], pltpu.roll(trans_b[:64], 64, 1))
    head1 = jnp.where(lane < 64, pltpu.roll(trans_a[64:], 64, 1), trans_b[64:])
    return head0, head1


def combine(later, total):
    lane = lax.broadcasted_iota(jnp.int32, later.shape, 1)
    return three(later[:, :64], total) + jnp.where(lane < 64, 0.0, later)


def kernel(
    tokens,
    norm_gain,
    w0,
    w1,
    w2,
    w3,
    w4,
    w5,
    w6,
    w7,
    out_scan,
    out_conv,
    key_gain,
    removal_gain,
    removal_bias,
    decay_bias,
    extra,
    scan_norm_gain,
    conv_kernel,
    conv_bias,
    conv_norm_gain,
    out,
    weights,
    outs,
    extra_v,
    norm_gain_v,
    conv_kernel_v,
    tok,
    normed,
    proj,
    outw0,
    outw1,
    pair_in,
    line_y,
    line_z,
    state_in,
    state_out,
    pair_out,
    rim,
    conv_in,
    conv_pad,
    stats,
    feats_scan,
    feats_conv,
    reads_a,
    reads_b,
    mine,
    load_sem,
    tok_send,
    tok_recv,
    first_send,
    first_recv,
    second_send,
    plus_recv,
    minus_recv,
    cross_send,
    cross_recv,
    first_send2,
    first_recv2,
    second_send2,
    plus_recv2,
    minus_recv2,
    outw_cross_send,
    outw_cross_recv,
    outw_send,
    outw_recv,
    outw_load,
    pair_send,
    pair_recv,
    y_send,
    y_recv,
    z_send,
    z_recv,
    state_send,
    state_recv,
    rim_send,
    rim_recv,
    stats_send,
    stats_recv,
    scan_send,
    scan_recv,
    conv_send,
    conv_recv,
):
    z, y, c, x = (lax.axis_index(n) for n in (*SP, "tp"))

    def at(z_=None, y_=None, c_=None, x_=None):
        pick = lambda a, b: a if b is None else b
        return (pick(z, z_), pick(y, y_), pick(c, c_), pick(x, x_))

    def remote(src, dst, send, recv, where):
        return pltpu.make_async_remote_copy(
            src_ref=src, dst_ref=dst, send_sem=send, recv_sem=recv, device_id=where, device_id_type=MESH
        )

    partner = at(c_=1 - c)

    a = (1 - c) * y + c * z
    b = (1 - c) * z + c * y

    loads = [
        pltpu.make_async_copy(tokens, tok.at[x], load_sem.at[0]),
    ]
    for k, w in enumerate((w0, w1, w2, w3, w4, w5, w6, w7)):
        loads.append(
            pltpu.make_async_copy(w, weights.at[c, b, a, :, pl.ds(128 * k, 128)], load_sem.at[k + 1])
        )
    for k, w in enumerate((out_scan, out_conv)):
        loads.append(
            pltpu.make_async_copy(w, outs.at[c, b, a, :, pl.ds(128 * k, 128)], load_sem.at[k + 9])
        )
    loads.append(pltpu.make_async_copy(extra, extra_v, load_sem.at[11]))
    loads.append(pltpu.make_async_copy(norm_gain, norm_gain_v, load_sem.at[12]))
    loads.append(pltpu.make_async_copy(conv_kernel, conv_kernel_v, load_sem.at[13]))
    for load in loads:
        load.start()

    barrier = pltpu.get_barrier_semaphore()
    greeted = [partner]
    for k in range(1, N):
        greeted.append(at(y_=lax.rem(y + k, N)))
        greeted.append(at(z_=lax.rem(z + k, N)))
    for k in range(1, NX):
        greeted.append(at(x_=lax.rem(x + k, NX)))
    place = (z * N + y) * 2 + c
    size = 2 * N * N
    before = lax.rem(place + size - 1, size)
    after = lax.rem(place + 1, size)
    as_device = lambda s: (s // (2 * N), lax.rem(s // 2, N), lax.rem(s, 2), x)
    greeted.append(as_device(before))
    for device in greeted:
        pl.semaphore_signal(barrier, inc=1, device_id=device, device_id_type=MESH)
    pl.semaphore_wait(barrier, len(greeted))
    for load in loads:
        load.wait()

    tok_copies = []
    for k in (1, 3, 2):
        tok_copies.append(
            remote(tok.at[x], tok.at[x], tok_send.at[k - 1], tok_recv.at[k - 1], at(x_=lax.rem(x + k, NX)))
        )
    def along_first(k):
        return at(z_=lax.rem(z + c * k, N), y_=lax.rem(y + (1 - c) * k, N))

    def along_second(k):
        return at(z_=lax.rem(z + (1 - c) * k, N), y_=lax.rem(y + c * k, N))

    class Gather:
        def __init__(self, ref, first_send, first_recv, second_send, plus_recv, minus_recv):
            self.ref, self.first_send, self.first_recv = ref, first_send, first_recv
            self.second_send, self.recvs = second_send, {1: plus_recv, -1: minus_recv}
            self.own_half = (a // 4) * 4

        def start(self):
            own = self.ref.at[c, b, a]
            for k in (1, 7, 2, 6, 3, 5, 4):
                remote(own, own, self.first_send, self.first_recv.at[a], along_first(k)).start()

        def half(self, h, distance):
            low = self.own_half if h == 0 else 4 - self.own_half
            return self.ref.at[c, lax.rem(b + distance + N, N), pl.ds(low, 4)]

        def copy(self, h, distance, sign, hop):
            piece = self.half(h, distance)
            recv = self.recvs[sign].at[h * 4 + hop]
            return remote(piece, piece, self.second_send, recv, along_second(1 if sign > 0 else N - 1))

        def collect(self, h):
            low = self.own_half if h == 0 else 4 - self.own_half
            for k in range(4):
                a_ = low + k

                @pl.when(a_ != a)
                def _():
                    piece = self.ref.at[c, b, a_]
                    remote(piece, piece, self.first_send, self.first_recv.at[a_], partner).wait_recv()

            for sign in (1, -1):
                self.copy(h, 0, sign, 0).start()
            return self.half(h, 0)

        def moved(self, h, hop, sign):
            self.copy(h, -sign * hop, sign, hop - 1).wait_recv()
            if hop < 3 or (hop == 3 and (h == 0) == (sign > 0)):
                self.copy(h, -sign * hop, sign, hop).start()
            return self.half(h, -sign * hop)

        def step(self, hop):
            for h in (0, 1):
                if hop == 0:
                    yield self.collect(h)
                    continue
                for sign in (1, -1):
                    if hop < 4 or (h == 0) == (sign > 0):
                        yield self.moved(h, hop, sign)

        def drain(self):
            seven = self.ref.at[0, 0, pl.ds(0, 7)]
            remote(seven, seven, self.first_send, self.first_recv.at[0], partner).wait_send()
            most = self.ref.at[0, pl.ds(0, 7)]
            remote(most, most, self.second_send, self.first_recv.at[0], partner).wait_send()

    wide = Gather(weights, first_send, first_recv, second_send, plus_recv, minus_recv)
    thin = Gather(outs, first_send2, first_recv2, second_send2, plus_recv2, minus_recv2)
    wide.start()
    for copy in tok_copies:
        copy.start()
    thin.start()

    for hop in range(5):
        for piece in wide.step(hop):
            remote(piece, piece, cross_send, cross_recv, partner).start()
        if hop == 2:
            for copy in tok_copies:
                copy.wait_recv()
            square = jnp.zeros((ROWS, 1), F32)
            for q in range(NX):
                t = tok[q].astype(F32)
                square = square + jnp.sum(t * t, axis=-1, keepdims=True)
            factor = lax.rsqrt(square * (1.0 / MODEL) + 1e-06)
            for q in range(NX):
                t = tok[q].astype(F32)
                columns = slice(q * 512, (q + 1) * 512)
                normed[:, columns] = (t * factor * norm_gain_v[:, columns]).astype(BF16)
        if hop == 3:
            for _ in thin.step(0):
                pass

    everything = weights.at[1 - c]
    remote(everything, everything, cross_send, cross_recv, partner).wait_recv()
    for _ in thin.step(1):
        pass

    def project_mark():
        pass

    def project(n, carry):
        columns = pl.ds(pl.multiple_of(n * 256, 256), 256)
        w = jnp.concatenate(
            [
                weights[p, j if p else i, i if p else j, :, columns]
                for i in range(N)
                for j in range(N)
                for p in range(2)
            ],
            axis=0,
        )
        proj[:, columns] = jnp.dot(normed[...], w, preferred_element_type=F32).astype(BF16)
        return carry

    lax.fori_loop(0, PROJ // 256, project, 0)
    for _ in thin.step(2):
        pass

    def part(k):
        return proj[:, 128 * k : 128 * (k + 1)].astype(F32)

    conv_in[...] = (part(6) * sigmoid(part(7))).astype(BF16)
    last = place == size - 1
    start = place == 0
    rim_copy = remote(
        conv_in.at[pl.ds(ROWS - 32, 32)], rim, rim_send, rim_recv, as_device(after)
    )

    @pl.when(jnp.logical_not(last))
    def _():
        rim_copy.start()

    trans_a, trans_b, ra, rb = local_scan(
        part(0),
        part(1),
        part(2),
        part(3),
        part(4),
        key_gain[...],
        removal_gain[...],
        removal_bias[...],
        decay_bias[...],
        extra_v[...],
    )
    for _ in thin.step(3):
        pass
    reads_a[...] = ra
    reads_b[...] = rb
    head0, head1 = packed_heads(trans_a, trans_b)
    upper = c == 1
    pair_out[...] = jnp.where(upper, head0, head1)
    mine[...] = jnp.where(upper, head1, head0)
    pair_copy = remote(pair_out, pair_in, pair_send, pair_recv, partner)
    pair_copy.start()
    pair_copy.wait_recv()
    earlier = jnp.where(upper, pair_in[...], mine[...])
    later = jnp.where(upper, mine[...], pair_in[...])
    line_y[y] = combine(later, earlier)
    for k in (4, 3, 5, 2, 6, 1, 7):
        remote(line_y.at[y], line_y.at[y], y_send, y_recv.at[y], at(y_=lax.rem(y + k, N))).start()

    for _ in thin.step(4):
        pass
    def outw_copies(p):
        for k in (1, 3, 2, 0):
            x_ = lax.rem(x + k, NX)
            if p:
                src, dst = outs.at[1, :, pl.ds(2 * x_, 2)], outw1.at[x]
            else:
                src, dst = outs.at[0, pl.ds(2 * x_, 2)], outw0.at[x]
            if k:
                yield remote(src, dst, outw_send.at[k - 1], outw_recv.at[k - 1], at(x_=x_))
            else:
                yield pltpu.make_async_copy(src, dst, outw_load)

    for p in range(2):

        @pl.when(c == p)
        def _():
            for copy in outw_copies(p):
                copy.start()

    outw_waits = list(outw_copies(0))

    @pl.when(start)
    def _():
        rim[...] = jnp.zeros_like(rim)

    @pl.when(jnp.logical_not(start))
    def _():
        rim_copy.wait_recv()

    conv_pad[pl.ds(0, 32)] = rim[...].astype(F32)
    conv_pad[pl.ds(32, ROWS)] = conv_in[...].astype(F32)
    filtered = conv_bias[...] + conv_kernel_v[0:1] * conv_pad[pl.ds(2, ROWS)]
    for k in range(1, CONV_K):
        filtered = filtered + conv_kernel_v[k : k + 1] * conv_pad[pl.ds(2 + k, ROWS)]
    near = jnp.mean(filtered, axis=-1, keepdims=True)
    around = jnp.sum((filtered - near) ** 2, axis=-1, keepdims=True)
    lane = lax.broadcasted_iota(jnp.int32, (ROWS, 128), 1)
    stats[x] = jnp.where(lane < 64, near, around)
    conv_pad[pl.ds(0, ROWS)] = filtered
    stats_copies = [
        remote(stats.at[x], stats.at[x], stats_send.at[k - 1], stats_recv.at[k - 1], at(x_=lax.rem(x + k, NX)))
        for k in (1, 3, 2)
    ]
    for copy in stats_copies:
        copy.start()

    lane = lax.broadcasted_iota(jnp.int32, (64, 128), 1)
    i, j = iotas(64, 128)
    blank = (i == j).astype(F32)
    total = inside = blank
    for k in range(N):

        @pl.when(y != k)
        def _():
            remote(line_y.at[k], line_y.at[k], y_send, y_recv.at[k], partner).wait_recv()

        total = combine(line_y[k], total)
        inside = jnp.where(k < y, total, inside)
    line_z[z] = total
    z_copies = []
    for k in range(N - 1, 0, -1):
        copy = remote(
            line_z.at[z], line_z.at[z], z_send.at[k - 1], z_recv.at[z], at(z_=lax.rem(z + k, N))
        )
        z_copies.append((k, copy))

        @pl.when(z + k < N)
        def _():
            copy.start()

    for copy in outw_waits[:3]:
        copy.wait_recv()
    outw_waits[3].wait()
    for p, ref in enumerate((outw0, outw1)):

        @pl.when(c == p)
        def _():
            remote(ref, ref, outw_cross_send, outw_cross_recv, partner).start()

    for copy in stats_copies:
        copy.wait_recv()
    center = jnp.zeros((ROWS, 1), F32)
    for q in range(NX):
        center = center + stats[q][:, 0:1]
    center = center * (1.0 / NX)
    spread = jnp.zeros((ROWS, 1), F32)
    for q in range(NX):
        gap = stats[q][:, 0:1] - center
        spread = spread + stats[q][:, 64:65] + 128.0 * gap * gap
    spread = spread * (1.0 / 512.0)
    normal = (conv_pad[pl.ds(0, ROWS)] - center) * lax.rsqrt(spread + 1e-05) * conv_norm_gain[...]
    feats_conv[x] = (normal * sigmoid(normal)).astype(BF16)
    conv_copies = [
        remote(
            feats_conv.at[x], feats_conv.at[x], conv_send.at[k - 1], conv_recv.at[k - 1], at(x_=lax.rem(x + k, NX))
        )
        for k in (1, 3, 2)
    ]
    for copy in conv_copies:
        copy.start()

    def advance(k, state):
        remote(line_z.at[k], line_z.at[k], z_send.at[0], z_recv.at[k], partner).wait_recv()
        return combine(line_z[k], state)

    state = lax.fori_loop(0, z, advance, jnp.zeros((64, 128), F32))
    state = jnp.where(lane < 64, 0.0, combine(inside, state))
    passed = combine(jnp.where(upper, pair_in[...], mine[...]), state)
    here = jnp.where(upper, passed, state)
    state_out[...] = jnp.where(upper, state, passed)
    state_copy = remote(state_out, state_in, state_send, state_recv, partner)
    state_copy.start()

    for copy in conv_copies:
        copy.wait_recv()
    outw_cross = remote(outw0, outw0, outw_cross_send, outw_cross_recv, partner)
    outw_cross.wait_recv()

    def w_of(q, h):
        columns = pl.ds(128 * h, 128)
        return jnp.concatenate(
            [
                (outw1[q, j, i, :, columns] if p else outw0[q, i, j, :, columns])
                for i in range(2)
                for j in range(N)
                for p in range(2)
            ],
            axis=0,
        )

    total_out = one_nt(feats_conv[0], w_of(0, 1))
    for q in range(1, NX):
        total_out = total_out + one_nt(feats_conv[q], w_of(q, 1))

    state_copy.wait_recv()
    there = state_in[...]
    state0 = jnp.where(upper, there, here)
    state1 = jnp.where(upper, here, there)
    whole = jnp.concatenate(
        [
            jnp.where(lane < 64, pltpu.roll(state0, 64, 1), 0.0),
            jnp.where(lane < 64, 0.0, state1),
        ],
        axis=0,
    )
    reads = three(reads_a[...], whole) + reads_b[...]
    ones = head_ones()
    reads = reads - right_exact(reads, ones) * (1.0 / 64.0)
    spread = right_exact(reads * reads, ones) * (1.0 / 64.0)
    feats_scan[x] = (
        reads * lax.rsqrt(spread + 0.00064) * scan_norm_gain[...] * sigmoid(part(5))
    ).astype(BF16)
    scan_copies = [
        remote(
            feats_scan.at[x], feats_scan.at[x], scan_send.at[k - 1], scan_recv.at[k - 1], at(x_=lax.rem(x + k, NX))
        )
        for k in (1, 3, 2)
    ]
    for copy in scan_copies:
        copy.start()
    for copy in scan_copies:
        copy.wait_recv()
    for q in range(NX):
        total_out = total_out + one_nt(feats_scan[q], w_of(q, 0))
    out[...] = total_out.astype(BF16)

    for copies in (tok_copies, outw_waits[:3], stats_copies, conv_copies, scan_copies):
        for copy in copies:
            copy.wait_send()
    pair_copy.wait_send()
    state_copy.wait_send()
    wide.drain()
    thin.drain()
    outw_cross.wait_send()
    remote(everything, everything, cross_send, cross_recv, partner).wait_send()
    lines = line_y.at[pl.ds(0, 7)]
    remote(lines, lines, y_send, y_recv.at[0], partner).wait_send()

    @pl.when(jnp.logical_not(last))
    def _():
        rim_copy.wait_send()

    for k, copy in z_copies:

        @pl.when(z + k < N)
        def _():
            copy.wait_send()


def shards(
    tokens,
    norm_gain,
    query_weight,
    key_weight,
    value_weight,
    decay_weight,
    removal_weight,
    gate_weight,
    key_gain,
    removal_gain,
    removal_bias,
    decay_bias,
    decay_extra,
    scan_norm_gain,
    conv_value_weight,
    conv_gate_weight,
    conv_kernel,
    conv_bias,
    conv_norm_gain,
    out_scan_weight,
    out_conv_weight,
):
    row = lambda v: v.reshape(1, -1)
    anywhere = pl.BlockSpec(memory_space=pl.ANY)
    inside = pl.BlockSpec(memory_space=pltpu.VMEM)
    dma = pltpu.SemaphoreType.DMA
    return pl.pallas_call(
        kernel,
        out_shape=jax.ShapeDtypeStruct((ROWS, 512), BF16),
        in_specs=[anywhere] * 12 + [inside] * 4 + [anywhere] + [inside] + [anywhere] + [inside] * 2,
        out_specs=inside,
        scratch_shapes=[
            pltpu.VMEM((2, N, N, 16, PROJ), BF16),
            pltpu.VMEM((2, N, N, 16, 256), BF16),
            pltpu.VMEM((ROWS, 128), F32),
            pltpu.VMEM((1, MODEL), F32),
            pltpu.VMEM((CONV_K, 128), F32),
            pltpu.VMEM((NX, ROWS, 512), BF16),
            pltpu.VMEM((ROWS, MODEL), BF16),
            pltpu.VMEM((ROWS, PROJ), BF16),
            pltpu.VMEM((NX, 2, N, 16, 256), BF16),
            pltpu.VMEM((NX, N, 2, 16, 256), BF16),
            pltpu.VMEM((64, 128), F32),
            pltpu.VMEM((N, 64, 128), F32),
            pltpu.VMEM((N, 64, 128), F32),
            pltpu.VMEM((64, 128), F32),
            pltpu.VMEM((64, 128), F32),
            pltpu.VMEM((64, 128), F32),
            pltpu.VMEM((32, 128), BF16),
            pltpu.VMEM((ROWS, 128), BF16),
            pltpu.VMEM((ROWS + 32, 128), F32),
            pltpu.VMEM((NX, ROWS, 128), F32),
            pltpu.VMEM((NX, ROWS, 128), BF16),
            pltpu.VMEM((NX, ROWS, 128), BF16),
            pltpu.VMEM((ROWS, 128), F32),
            pltpu.VMEM((ROWS, 128), F32),
            pltpu.VMEM((64, 128), F32),
            dma((14,)),
            dma((3,)),
            dma((3,)),
            dma(()),
            dma((8,)),
            dma(()),
            dma((8,)),
            dma((8,)),
            dma(()),
            dma(()),
            dma(()),
            dma((8,)),
            dma(()),
            dma((8,)),
            dma((8,)),
            dma(()),
            dma(()),
            dma((3,)),
            dma((3,)),
            dma(()),
            dma(()),
            dma(()),
            dma(()),
            dma((N,)),
            dma((N - 1,)),
            dma((N,)),
            dma(()),
            dma(()),
            dma(()),
            dma(()),
            dma((3,)),
            dma((3,)),
            dma((3,)),
            dma((3,)),
            dma((3,)),
            dma((3,)),
        ],
        compiler_params=pltpu.CompilerParams(
            collective_id=0, has_side_effects=True, vmem_limit_bytes=56 * 1024 * 1024
        ),
    )(
        tokens,
        row(norm_gain),
        query_weight,
        key_weight,
        value_weight,
        decay_weight,
        removal_weight,
        gate_weight,
        conv_value_weight,
        conv_gate_weight,
        out_scan_weight.T,
        out_conv_weight.T,
        row(key_gain),
        row(removal_gain),
        row(removal_bias),
        row(decay_bias),
        decay_extra,
        row(scan_norm_gain),
        conv_kernel,
        row(conv_bias),
        row(conv_norm_gain),
    )


def solution(mesh):
    torus = Mesh(mesh.devices.reshape(N, N, 2, mesh.shape["tp"]), (*SP, "tp"))
    in_specs = (
        P(SP, "tp"),
        P(),
        P(SP, "tp"),
        P(SP, "tp"),
        P(SP, "tp"),
        P(SP, "tp"),
        P(SP, "tp"),
        P(SP, "tp"),
        P("tp"),
        P("tp"),
        P("tp"),
        P("tp"),
        P(SP, "tp"),
        P("tp"),
        P(SP, "tp"),
        P(SP, "tp"),
        P(None, "tp"),
        P("tp"),
        P("tp"),
        P("tp", SP),
        P("tp", SP),
    )
    return jax.shard_map(
        shards, mesh=torus, in_specs=in_specs, out_specs=P(SP, "tp"), check_vma=False
    )
```

```python
import functools
import math

import jax
import jax.numpy as jnp
from jax import lax
from jax.experimental import pallas as pl
from jax.experimental.pallas import tpu as pltpu
from jax.sharding import Mesh
from jax.sharding import PartitionSpec as P

F32 = jnp.float32
BF16 = jnp.bfloat16
SP = ("sp_0", "sp_1", "sp_2")
MESH = pl.DeviceIdType.MESH
CONV_K = 31
ROWS = 192
BLOCK = 64
BLOCKS = ROWS // BLOCK
MODEL = 2048
NX = 4
PROJ = 1024
N = 8


def split2(a):
    high = a.astype(BF16)
    return high, (a - high.astype(F32)).astype(BF16)


def one(a, b):
    return jnp.dot(a.astype(BF16), b.astype(BF16), preferred_element_type=F32)


def one_nt(a, b):
    return lax.dot_general(
        a.astype(BF16), b.astype(BF16), (((1,), (1,)), ((), ())), preferred_element_type=F32
    )


def three(a, b):
    ah, al = split2(a)
    bh, bl = split2(b)
    return one(ah, bh) + one(al, bh) + one(ah, bl)


def three_nt(a, b):
    ah, al = split2(a)
    bh, bl = split2(b)
    return one_nt(ah, bh) + one_nt(al, bh) + one_nt(ah, bl)


def left_exact(a, b):
    bh, bm = split2(b)
    bl = (b - bh.astype(F32) - bm.astype(F32)).astype(BF16)
    return one(a, bh) + one(a, bm) + one(a, bl)


def right_exact(a, b):
    ah, al = split2(a)
    return one(ah, b) + one(al, b)


def iotas(rows, columns):
    return (
        lax.broadcasted_iota(jnp.int32, (rows, columns), 0),
        lax.broadcasted_iota(jnp.int32, (rows, columns), 1),
    )


def sigmoid(x):
    return 1.0 / (1.0 + jnp.exp(-x))


def head_ones():
    i, j = iotas(128, 128)
    return ((i >> 6) == (j >> 6)).astype(BF16)


PAIRS, INVERSE, GATHERED, STEP, READ, CHAIN = three, three, three, three, three, three
PAIRS_NT = three_nt


def spread(a):
    first = lax.broadcasted_iota(jnp.int32, a.shape, 1) < 64
    return jnp.concatenate([jnp.where(first, a, 0.0), jnp.where(first, 0.0, a)], axis=0)


def masks():
    i, j = iotas(128, 128)
    same_head = (i >> 6) == (j >> 6)
    return i, j, same_head


def prepared(keys, values, decay_pre, removal_pre, key_gain, removal_gain, removal_bias, decay_bias, extra):
    ones = head_ones()
    rate = sigmoid(decay_bias + decay_pre) * math.exp(-0.5) + extra
    removal = sigmoid(removal_bias + removal_pre)
    scaled = keys * key_gain
    unit = scaled * lax.rsqrt(right_exact(scaled * scaled, ones) + 1e-06)
    written = keys * (1.0 + (removal - 1.0) * removal_gain)
    beta = unit * removal
    i, j = iotas(BLOCK, BLOCK)
    lower = (i >= j).astype(BF16)
    blocks = []
    for b in range(BLOCKS):
        rows = slice(b * BLOCK, (b + 1) * BLOCK)
        rate_b = rate[rows]
        falling = -left_exact(lower, rate_b)
        before = falling + rate_b
        middle = falling[BLOCK // 2 : BLOCK // 2 + 1]
        ending = falling[BLOCK - 1 :]
        up = jnp.exp(middle - falling)
        to_end = jnp.exp(ending - falling)
        beta_mid = beta[rows] * up
        keys_mid = written[rows] * up
        blocks.append(
            dict(
                falling=falling,
                middle=middle,
                end_decay=jnp.exp(ending),
                left=spread(-unit[rows] * jnp.exp(before - middle)),
                right=jnp.concatenate([beta_mid, beta_mid, keys_mid, keys_mid], axis=0),
                start_alpha=spread(-unit[rows] * jnp.exp(before)),
                end_beta=spread(beta[rows] * to_end).T,
                end_keys=spread(written[rows] * to_end).T,
                values=spread(values[rows]),
            )
        )
    return blocks


def inverted(blocks):
    i, j, same_head = masks()
    strict = same_head & (i > j)
    eye = (i == j).astype(F32)
    sames = [(i >> s) == (j >> s) for s in (3, 4, 5)] + [same_head]
    for block in blocks:
        pairs = PAIRS_NT(block["left"], block["right"])
        block["links"] = jnp.where(strict, pairs[:, :128], 0.0)
        alpha_keys = jnp.where(strict, pairs[:, 128:], 0.0)
        block["local"] = PAIRS(alpha_keys, block["values"])
        block["power"] = base = jnp.where(sames[0], block["links"], 0.0)
        block["inverse"] = eye + base
    for _ in range(2):
        for block in blocks:
            block["power"] = INVERSE(block["power"], block["power"])
        for block in blocks:
            block["inverse"] = block["inverse"] + INVERSE(block["inverse"], block["power"])
    for s in range(3):
        for block in blocks:
            off = jnp.where(sames[s + 1] & ~sames[s], block["links"], 0.0)
            block["part"] = INVERSE(off, block["inverse"])
        for block in blocks:
            block["inverse"] = block["inverse"] + INVERSE(block["inverse"], block["part"])


def transition(blocks):
    i, j, same_head = masks()
    for block in blocks:
        block["gathered"] = GATHERED(
            block["inverse"], jnp.concatenate([block["start_alpha"], block["local"]], axis=1)
        )
    for block in blocks:
        step = STEP(block["end_beta"], block["gathered"])
        block["step_a"] = step[:, :128] + jnp.where(i == j, block["end_decay"], 0.0)
        block["step_b"] = step[:, 128:] + STEP(block["end_keys"], block["values"])
    both = jnp.concatenate([blocks[0]["step_a"], blocks[0]["step_b"]], axis=1)
    for block in blocks[1:]:
        block["start"] = both
        moved = CHAIN(block["step_a"], both)
        both = jnp.concatenate([moved[:, :128], moved[:, 128:] + block["step_b"]], axis=1)
    return both[:, :128], both[:, 128:]


def read_parts(blocks, recept):
    i, j, same_head = masks()
    inclusive = same_head & (i >= j)
    reads_a, reads_b = [], []
    for b, block in enumerate(blocks):
        rows = slice(b * BLOCK, (b + 1) * BLOCK)
        left = spread(recept[rows] * jnp.exp(block["falling"] - block["middle"]))
        pairs = PAIRS_NT(left, block["right"])
        recept_beta = jnp.where(inclusive, pairs[:, :128], 0.0)
        recept_keys = jnp.where(inclusive, pairs[:, 128:], 0.0)
        reads = READ(recept_beta, block["gathered"])
        read_a = reads[:64, :128] + reads[64:, :128] + recept[rows] * jnp.exp(block["falling"])
        read_b = reads[:, 128:] + READ(recept_keys, block["values"])
        read_b = read_b[:64] + read_b[64:]
        if b:
            seen = READ(read_a, block["start"])
            read_a, read_b = seen[:, :128], seen[:, 128:] + read_b
        reads_a.append(read_a)
        reads_b.append(read_b)
    return jnp.concatenate(reads_a, axis=0), jnp.concatenate(reads_b, axis=0)


def local_scan(recept, keys, values, decay_pre, removal_pre, *rest):
    blocks = prepared(keys, values, decay_pre, removal_pre, *rest)
    inverted(blocks)
    trans = transition(blocks)
    return (*trans, *read_parts(blocks, recept))


def packed_heads(trans_a, trans_b):
    lane = lax.broadcasted_iota(jnp.int32, (64, 128), 1)
    head0 = jnp.where(lane < 64, trans_a[:64], pltpu.roll(trans_b[:64], 64, 1))
    head1 = jnp.where(lane < 64, pltpu.roll(trans_a[64:], 64, 1), trans_b[64:])
    return head0, head1


def coded(both):
    i, j = iotas(64, 128)
    on = i == j
    diagonal = jnp.sum(jnp.where(on, both, 0.0), axis=0, keepdims=True)
    high, rest = split2(diagonal)
    low = (diagonal - high.astype(F32) - rest.astype(F32)).astype(BF16)
    row = lax.broadcasted_iota(jnp.int32, (16, 128), 0)
    below = jnp.where(
        row == 0,
        high.astype(F32),
        jnp.where(row == 1, rest.astype(F32), jnp.where(row == 2, low.astype(F32), 0.0)),
    )
    return jnp.concatenate([jnp.where(on, 0.0, both), below], axis=0).astype(BF16)


def decoded(code):
    code = code.astype(F32)
    i, j = iotas(64, 128)
    diagonal = code[64:65] + code[65:66] + code[66:67]
    return jnp.where(i == j, diagonal, code[:64])


def combine(later, total):
    lane = lax.broadcasted_iota(jnp.int32, later.shape, 1)
    return three(later[:, :64], total) + jnp.where(lane < 64, 0.0, later)


NORM_AT = 11
THIN_AT = 3


def kernel(
    tokens,
    norm_gain,
    w0,
    w1,
    w2,
    w3,
    w4,
    w5,
    w6,
    w7,
    out_scan,
    out_conv,
    key_gain,
    removal_gain,
    removal_bias,
    decay_bias,
    extra,
    scan_norm_gain,
    conv_kernel,
    conv_bias,
    conv_norm_gain,
    out,
    weights,
    outs,
    extra_v,
    norm_gain_v,
    conv_kernel_v,
    tok,
    normed,
    proj,
    outw0,
    outw1,
    pair_in,
    line_y,
    line_z,
    state_in,
    state_out,
    pair_out,
    rim,
    conv_in,
    conv_pad,
    stats,
    feats_scan,
    feats_conv,
    reads_a,
    reads_b,
    mine,
    load_sem,
    tok_send,
    tok_recv,
    first_send,
    first_recv,
    second_send,
    plus_recv,
    minus_recv,
    cross_send,
    cross_recv,
    first_send2,
    first_recv2,
    second_send2,
    plus_recv2,
    minus_recv2,
    outw_cross_send,
    outw_cross_recv,
    late_send,
    late_recv,
    outw_send,
    outw_recv,
    outw_load,
    pair_send,
    pair_recv,
    y_send,
    y_recv,
    z_send,
    z_recv,
    state_send,
    state_recv,
    rim_send,
    rim_recv,
    stats_send,
    stats_recv,
    scan_send,
    scan_recv,
    conv_send,
    conv_recv,
):
    z, y, c, x = (lax.axis_index(n) for n in (*SP, "tp"))

    def at(z_=None, y_=None, c_=None, x_=None):
        pick = lambda a, b: a if b is None else b
        return (pick(z, z_), pick(y, y_), pick(c, c_), pick(x, x_))

    def remote(src, dst, send, recv, where):
        return pltpu.make_async_remote_copy(
            src_ref=src, dst_ref=dst, send_sem=send, recv_sem=recv, device_id=where, device_id_type=MESH
        )

    partner = at(c_=1 - c)

    a = (1 - c) * y + c * z
    b = (1 - c) * z + c * y

    loads = [
        pltpu.make_async_copy(tokens, tok.at[x], load_sem.at[0]),
    ]
    for k, w in enumerate((w1, w2, w3, w4)):
        loads.append(
            pltpu.make_async_copy(w, weights.at[c, b, a, :, pl.ds(128 * k, 128)], load_sem.at[k + 1])
        )
    for k, w in enumerate((w0, w5, w6, w7, out_scan, out_conv)):
        loads.append(
            pltpu.make_async_copy(w, outs.at[c, b, a, :, pl.ds(128 * k, 128)], load_sem.at[k + 5])
        )
    loads.append(pltpu.make_async_copy(extra, extra_v, load_sem.at[11]))
    loads.append(pltpu.make_async_copy(norm_gain, norm_gain_v, load_sem.at[12]))
    loads.append(pltpu.make_async_copy(conv_kernel, conv_kernel_v, load_sem.at[13]))
    for load in loads:
        load.start()

    barrier = pltpu.get_barrier_semaphore()
    greeted = [partner]
    for k in range(1, N):
        greeted.append(at(y_=lax.rem(y + k, N)))
        greeted.append(at(z_=lax.rem(z + k, N)))
    for k in range(1, NX):
        greeted.append(at(x_=lax.rem(x + k, NX)))
    place = (z * N + y) * 2 + c
    size = 2 * N * N
    before = lax.rem(place + size - 1, size)
    after = lax.rem(place + 1, size)
    as_device = lambda s: (s // (2 * N), lax.rem(s // 2, N), lax.rem(s, 2), x)
    greeted.append(as_device(before))
    for device in greeted:
        pl.semaphore_signal(barrier, inc=1, device_id=device, device_id_type=MESH)
    pl.semaphore_wait(barrier, len(greeted))
    for load in loads:
        load.wait()

    tok_copies = []
    for k in (1, 3, 2):
        tok_copies.append(
            remote(tok.at[x], tok.at[x], tok_send.at[k - 1], tok_recv.at[k - 1], at(x_=lax.rem(x + k, NX)))
        )
    def along_first(k):
        return at(z_=lax.rem(z + c * k, N), y_=lax.rem(y + (1 - c) * k, N))

    def along_second(k):
        return at(z_=lax.rem(z + (1 - c) * k, N), y_=lax.rem(y + c * k, N))

    class Gather:
        def __init__(self, ref, first_send, first_recv, second_send, plus_recv, minus_recv):
            self.ref, self.first_send, self.first_recv = ref, first_send, first_recv
            self.second_send, self.recvs = second_send, {1: plus_recv, -1: minus_recv}

        def start(self):
            own = self.ref.at[c, b, a]
            for k in (1, 7, 2, 6, 3, 5, 4):
                remote(own, own, self.first_send, self.first_recv.at[a], along_first(k)).start()

        def low(self, h):
            return lax.rem(a // 2 + h, 4) * 2

        def piece(self, h, distance):
            return self.ref.at[c, lax.rem(b + distance + N, N), pl.ds(self.low(h), 2)]

        def copy(self, h, source, sign, reach):
            piece = self.piece(h, -sign * source)
            recv = self.recvs[sign].at[h * 4 + source + reach - 1]
            target = along_second(reach if sign > 0 else N - reach)
            return remote(piece, piece, self.second_send, recv, target)

        def collect(self, h):
            for k in range(2):
                a_ = self.low(h) + k

                def wait():
                    piece = self.ref.at[c, b, a_]
                    remote(piece, piece, self.first_send, self.first_recv.at[a_], partner).wait_recv()

                if h:
                    wait()
                else:
                    pl.when(a_ != a)(wait)

            for reach in (2, 1):
                for sign in (1, -1):
                    self.copy(h, 0, sign, reach).start()
            return [self.piece(h, 0)]

        def has_far(self, h, sign):
            return (h % 2 == 0) == (sign > 0)

        def arrive(self, h, d, sign):
            self.copy(h, 0, sign, d).wait_recv()
            return self.piece(h, -sign * d)

        def relay(self, h):
            pieces = []
            for sign in (1, -1):
                pieces.append(self.arrive(h, 2, sign))
                if self.has_far(h, sign):
                    self.copy(h, 2, sign, 2).start()
                self.copy(h, 2, sign, 1).start()
            return pieces

        def near(self, h):
            return [self.arrive(h, 1, sign) for sign in (1, -1)]

        def far(self, h):
            pieces = [self.arrive(h, 4, sign) for sign in (1, -1) if self.has_far(h, sign)]
            return pieces + [self.arrive(h, 3, sign) for sign in (1, -1)]

        def drain(self):
            seven = self.ref.at[0, 0, pl.ds(0, 7)]
            remote(seven, seven, self.first_send, self.first_recv.at[0], partner).wait_send()
            most = self.ref.at[0, pl.ds(0, 7)]
            remote(most, most, self.second_send, self.first_recv.at[0], partner).wait_send()

    wide = Gather(weights, first_send, first_recv, second_send, plus_recv, minus_recv)
    thin = Gather(outs, first_send2, first_recv2, second_send2, plus_recv2, minus_recv2)
    wide.start()
    for copy in tok_copies:
        copy.start()

    order = (0, 1, 3, 2)
    events = [(wide.collect, h) for h in order]
    for h in order:
        events += [(wide.relay, h), (wide.near, h)]
    events += [(wide.far, h) for h in order]
    for number, (event, h) in enumerate(events):
        for piece in event(h):
            remote(piece, piece, cross_send, cross_recv, partner).start()
        if number == THIN_AT:
            thin.start()
        if number == NORM_AT:
            for copy in tok_copies:
                copy.wait_recv()
            square = jnp.zeros((ROWS, 1), F32)
            for q in range(NX):
                t = tok[q].astype(F32)
                square = square + jnp.sum(t * t, axis=-1, keepdims=True)
            factor = lax.rsqrt(square * (1.0 / MODEL) + 1e-06)
            for q in range(NX):
                t = tok[q].astype(F32)
                columns = slice(q * 512, (q + 1) * 512)
                normed[:, columns] = (t * factor * norm_gain_v[:, columns]).astype(BF16)

    everything = weights.at[1 - c]
    remote(everything, everything, cross_send, cross_recv, partner).wait_recv()
    for h in order:
        thin.collect(h)

    def project(ref, base):
        def columns_of(n, carry):
            columns = pl.ds(pl.multiple_of(n * 256, 256), 256)
            w = jnp.concatenate(
                [
                    ref[p, j if p else i, i if p else j, :, columns]
                    for i in range(N)
                    for j in range(N)
                    for p in range(2)
                ],
                axis=0,
            )
            proj[:, pl.ds(pl.multiple_of(base + n * 256, 256), 256)] = jnp.dot(
                normed[...], w, preferred_element_type=F32
            ).astype(BF16)
            return carry

        lax.fori_loop(0, 2, columns_of, 0)

    project(weights, 0)

    def part(k):
        return proj[:, 128 * k : 128 * (k + 1)].astype(F32)

    blocks = prepared(
        part(0),
        part(1),
        part(2),
        part(3),
        key_gain[...],
        removal_gain[...],
        removal_bias[...],
        decay_bias[...],
        extra_v[...],
    )
    inverted(blocks)
    trans_a, trans_b = transition(blocks)
    for h in order:
        thin.relay(h)
    head0, head1 = packed_heads(trans_a, trans_b)
    upper = c == 1
    pair_out[...] = jnp.where(upper, head0, head1)
    mine[...] = jnp.where(upper, head1, head0)
    pair_copy = remote(pair_out, pair_in, pair_send, pair_recv, partner)
    pair_copy.start()
    pair_copy.wait_recv()
    earlier = jnp.where(upper, pair_in[...], mine[...])
    later = jnp.where(upper, mine[...], pair_in[...])
    line_y[y] = coded(combine(later, earlier))
    for k in (4, 3, 5, 2, 6, 1, 7):
        remote(line_y.at[y], line_y.at[y], y_send, y_recv.at[y], at(y_=lax.rem(y + k, N))).start()

    for h in order:
        thin.near(h)
        thin.far(h)
    own_paths = outs.at[c, :, :, :, pl.ds(0, 512)]
    other_paths = outs.at[1 - c, :, :, :, pl.ds(0, 512)]
    late_cross = remote(own_paths, own_paths, late_send, late_recv, partner)
    late_cross.start()
    def outw_copies(p):
        for k in (1, 3, 2, 0):
            x_ = lax.rem(x + k, NX)
            if p:
                src, dst = outs.at[1, :, pl.ds(2 * x_, 2), :, pl.ds(512, 256)], outw1.at[x]
            else:
                src, dst = outs.at[0, pl.ds(2 * x_, 2), :, :, pl.ds(512, 256)], outw0.at[x]
            if k:
                yield remote(src, dst, outw_send.at[k - 1], outw_recv.at[k - 1], at(x_=x_))
            else:
                yield pltpu.make_async_copy(src, dst, outw_load)

    for p in range(2):

        @pl.when(c == p)
        def _():
            for copy in outw_copies(p):
                copy.start()

    outw_waits = list(outw_copies(0))

    remote(other_paths, other_paths, late_send, late_recv, partner).wait_recv()
    project(outs, 512)

    conv_in[...] = (part(6) * sigmoid(part(7))).astype(BF16)
    last = place == size - 1
    start = place == 0
    rim_copy = remote(conv_in.at[pl.ds(ROWS - 32, 32)], rim, rim_send, rim_recv, as_device(after))

    @pl.when(jnp.logical_not(last))
    def _():
        rim_copy.start()

    reads_a[...], reads_b[...] = read_parts(blocks, part(4))

    @pl.when(start)
    def _():
        rim[...] = jnp.zeros_like(rim)

    @pl.when(jnp.logical_not(start))
    def _():
        rim_copy.wait_recv()

    conv_pad[pl.ds(0, 32)] = rim[...].astype(F32)
    conv_pad[pl.ds(32, ROWS)] = conv_in[...].astype(F32)
    filtered = conv_bias[...] + conv_kernel_v[0:1] * conv_pad[pl.ds(2, ROWS)]
    for k in range(1, CONV_K):
        filtered = filtered + conv_kernel_v[k : k + 1] * conv_pad[pl.ds(2 + k, ROWS)]
    near = jnp.mean(filtered, axis=-1, keepdims=True)
    around = jnp.sum((filtered - near) ** 2, axis=-1, keepdims=True)
    lane = lax.broadcasted_iota(jnp.int32, (ROWS, 128), 1)
    stats[x] = jnp.where(lane < 64, near, around)
    conv_pad[pl.ds(0, ROWS)] = filtered
    stats_copies = [
        remote(stats.at[x], stats.at[x], stats_send.at[k - 1], stats_recv.at[k - 1], at(x_=lax.rem(x + k, NX)))
        for k in (1, 3, 2)
    ]
    for copy in stats_copies:
        copy.start()

    lane = lax.broadcasted_iota(jnp.int32, (64, 128), 1)
    i, j = iotas(64, 128)
    blank = (i == j).astype(F32)
    total = inside = blank
    for k in range(N):

        @pl.when(y != k)
        def _():
            remote(line_y.at[k], line_y.at[k], y_send, y_recv.at[k], partner).wait_recv()

        total = combine(decoded(line_y[k]), total)
        inside = jnp.where(k < y, total, inside)
    line_z[z] = coded(total)
    z_copies = []
    for k in range(N - 1, 0, -1):
        copy = remote(
            line_z.at[z], line_z.at[z], z_send.at[k - 1], z_recv.at[z], at(z_=lax.rem(z + k, N))
        )
        z_copies.append((k, copy))

        @pl.when(z + k < N)
        def _():
            copy.start()

    for copy in outw_waits[:3]:
        copy.wait_recv()
    outw_waits[3].wait()
    for p, ref in enumerate((outw0, outw1)):

        @pl.when(c == p)
        def _():
            remote(ref, ref, outw_cross_send, outw_cross_recv, partner).start()

    for copy in stats_copies:
        copy.wait_recv()
    center = jnp.zeros((ROWS, 1), F32)
    for q in range(NX):
        center = center + stats[q][:, 0:1]
    center = center * (1.0 / NX)
    spread = jnp.zeros((ROWS, 1), F32)
    for q in range(NX):
        gap = stats[q][:, 0:1] - center
        spread = spread + stats[q][:, 64:65] + 128.0 * gap * gap
    spread = spread * (1.0 / 512.0)
    normal = (conv_pad[pl.ds(0, ROWS)] - center) * lax.rsqrt(spread + 1e-05) * conv_norm_gain[...]
    feats_conv[x] = (normal * sigmoid(normal)).astype(BF16)
    conv_copies = [
        remote(
            feats_conv.at[x], feats_conv.at[x], conv_send.at[k - 1], conv_recv.at[k - 1], at(x_=lax.rem(x + k, NX))
        )
        for k in (1, 3, 2)
    ]
    for copy in conv_copies:
        copy.start()

    def advance(k, state):
        remote(line_z.at[k], line_z.at[k], z_send.at[0], z_recv.at[k], partner).wait_recv()
        return combine(decoded(line_z[k]), state)

    state = lax.fori_loop(0, z, advance, jnp.zeros((64, 128), F32))
    state = jnp.where(lane < 64, 0.0, combine(inside, state))
    passed = combine(jnp.where(upper, pair_in[...], mine[...]), state)
    here = jnp.where(upper, passed, state)
    state_out[...] = jnp.where(upper, state, passed)
    state_copy = remote(state_out, state_in, state_send, state_recv, partner)
    state_copy.start()

    for copy in conv_copies:
        copy.wait_recv()
    outw_cross = remote(outw0, outw0, outw_cross_send, outw_cross_recv, partner)
    outw_cross.wait_recv()

    def w_of(q, h):
        columns = pl.ds(128 * h, 128)
        return jnp.concatenate(
            [
                (outw1[q, j, i, :, columns] if p else outw0[q, i, j, :, columns])
                for i in range(2)
                for j in range(N)
                for p in range(2)
            ],
            axis=0,
        )

    total_out = one_nt(feats_conv[0], w_of(0, 1))
    for q in range(1, NX):
        total_out = total_out + one_nt(feats_conv[q], w_of(q, 1))

    state_copy.wait_recv()
    there = state_in[...]
    state0 = jnp.where(upper, there, here)
    state1 = jnp.where(upper, here, there)
    whole = jnp.concatenate(
        [
            jnp.where(lane < 64, pltpu.roll(state0, 64, 1), 0.0),
            jnp.where(lane < 64, 0.0, state1),
        ],
        axis=0,
    )
    reads = three(reads_a[...], whole) + reads_b[...]
    ones = head_ones()
    reads = reads - right_exact(reads, ones) * (1.0 / 64.0)
    spread = right_exact(reads * reads, ones) * (1.0 / 64.0)
    feats_scan[x] = (
        reads * lax.rsqrt(spread + 0.00064) * scan_norm_gain[...] * sigmoid(part(5))
    ).astype(BF16)
    scan_copies = [
        remote(
            feats_scan.at[x], feats_scan.at[x], scan_send.at[k - 1], scan_recv.at[k - 1], at(x_=lax.rem(x + k, NX))
        )
        for k in (1, 3, 2)
    ]
    for copy in scan_copies:
        copy.start()
    for copy in scan_copies:
        copy.wait_recv()
    for q in range(NX):
        total_out = total_out + one_nt(feats_scan[q], w_of(q, 0))
    out[...] = total_out.astype(BF16)

    for copies in (tok_copies, outw_waits[:3], stats_copies, conv_copies, scan_copies):
        for copy in copies:
            copy.wait_send()
    pair_copy.wait_send()
    state_copy.wait_send()
    wide.drain()
    thin.drain()
    outw_cross.wait_send()
    late_cross.wait_send()
    remote(everything, everything, cross_send, cross_recv, partner).wait_send()
    lines = line_y.at[pl.ds(0, 7)]
    remote(lines, lines, y_send, y_recv.at[0], partner).wait_send()

    @pl.when(jnp.logical_not(last))
    def _():
        rim_copy.wait_send()

    for k, copy in z_copies:

        @pl.when(z + k < N)
        def _():
            copy.wait_send()


def shards(
    tokens,
    norm_gain,
    query_weight,
    key_weight,
    value_weight,
    decay_weight,
    removal_weight,
    gate_weight,
    key_gain,
    removal_gain,
    removal_bias,
    decay_bias,
    decay_extra,
    scan_norm_gain,
    conv_value_weight,
    conv_gate_weight,
    conv_kernel,
    conv_bias,
    conv_norm_gain,
    out_scan_weight,
    out_conv_weight,
):
    row = lambda v: v.reshape(1, -1)
    anywhere = pl.BlockSpec(memory_space=pl.ANY)
    inside = pl.BlockSpec(memory_space=pltpu.VMEM)
    dma = pltpu.SemaphoreType.DMA
    return pl.pallas_call(
        kernel,
        out_shape=jax.ShapeDtypeStruct((ROWS, 512), BF16),
        in_specs=[anywhere] * 12 + [inside] * 4 + [anywhere] + [inside] + [anywhere] + [inside] * 2,
        out_specs=inside,
        scratch_shapes=[
            pltpu.VMEM((2, N, N, 16, 512), BF16),
            pltpu.VMEM((2, N, N, 16, 768), BF16),
            pltpu.VMEM((ROWS, 128), F32),
            pltpu.VMEM((1, MODEL), F32),
            pltpu.VMEM((CONV_K, 128), F32),
            pltpu.VMEM((NX, ROWS, 512), BF16),
            pltpu.VMEM((ROWS, MODEL), BF16),
            pltpu.VMEM((ROWS, PROJ), BF16),
            pltpu.VMEM((NX, 2, N, 16, 256), BF16),
            pltpu.VMEM((NX, N, 2, 16, 256), BF16),
            pltpu.VMEM((64, 128), F32),
            pltpu.VMEM((N, 80, 128), BF16),
            pltpu.VMEM((N, 80, 128), BF16),
            pltpu.VMEM((64, 128), F32),
            pltpu.VMEM((64, 128), F32),
            pltpu.VMEM((64, 128), F32),
            pltpu.VMEM((32, 128), BF16),
            pltpu.VMEM((ROWS, 128), BF16),
            pltpu.VMEM((ROWS + 32, 128), F32),
            pltpu.VMEM((NX, ROWS, 128), F32),
            pltpu.VMEM((NX, ROWS, 128), BF16),
            pltpu.VMEM((NX, ROWS, 128), BF16),
            pltpu.VMEM((ROWS, 128), F32),
            pltpu.VMEM((ROWS, 128), F32),
            pltpu.VMEM((64, 128), F32),
            dma((14,)),
            dma((3,)),
            dma((3,)),
            dma(()),
            dma((8,)),
            dma(()),
            dma((16,)),
            dma((16,)),
            dma(()),
            dma(()),
            dma(()),
            dma((8,)),
            dma(()),
            dma((16,)),
            dma((16,)),
            dma(()),
            dma(()),
            dma(()),
            dma(()),
            dma((3,)),
            dma((3,)),
            dma(()),
            dma(()),
            dma(()),
            dma(()),
            dma((N,)),
            dma((N - 1,)),
            dma((N,)),
            dma(()),
            dma(()),
            dma(()),
            dma(()),
            dma((3,)),
            dma((3,)),
            dma((3,)),
            dma((3,)),
            dma((3,)),
            dma((3,)),
        ],
        compiler_params=pltpu.CompilerParams(
            collective_id=0, has_side_effects=True, vmem_limit_bytes=56 * 1024 * 1024
        ),
    )(
        tokens,
        row(norm_gain),
        query_weight,
        key_weight,
        value_weight,
        decay_weight,
        removal_weight,
        gate_weight,
        conv_value_weight,
        conv_gate_weight,
        out_scan_weight.T,
        out_conv_weight.T,
        row(key_gain),
        row(removal_gain),
        row(removal_bias),
        row(decay_bias),
        decay_extra,
        row(scan_norm_gain),
        conv_kernel,
        row(conv_bias),
        row(conv_norm_gain),
    )


def solution(mesh):
    torus = Mesh(mesh.devices.reshape(N, N, 2, mesh.shape["tp"]), (*SP, "tp"))
    in_specs = (
        P(SP, "tp"),
        P(),
        P(SP, "tp"),
        P(SP, "tp"),
        P(SP, "tp"),
        P(SP, "tp"),
        P(SP, "tp"),
        P(SP, "tp"),
        P("tp"),
        P("tp"),
        P("tp"),
        P("tp"),
        P(SP, "tp"),
        P("tp"),
        P(SP, "tp"),
        P(SP, "tp"),
        P(None, "tp"),
        P("tp"),
        P("tp"),
        P("tp", SP),
        P("tp", SP),
    )
    return jax.shard_map(
        shards, mesh=torus, in_specs=in_specs, out_specs=P(SP, "tp"), check_vma=False
    )
```

```python
import functools
import math

import jax
import jax.numpy as jnp
from jax import lax
from jax.experimental import pallas as pl
from jax.experimental.pallas import tpu as pltpu
from jax.sharding import Mesh
from jax.sharding import PartitionSpec as P

F32 = jnp.float32
BF16 = jnp.bfloat16
SP = ("sp_0", "sp_1", "sp_2")
MESH = pl.DeviceIdType.MESH
CONV_K = 31
ROWS = 192
BLOCK = 64
BLOCKS = ROWS // BLOCK
MODEL = 2048
NX = 4
PROJ = 1024
N = 8


def split2(a):
    high = a.astype(BF16)
    return high, (a - high.astype(F32)).astype(BF16)


def one(a, b):
    return jnp.dot(a.astype(BF16), b.astype(BF16), preferred_element_type=F32)


def one_nt(a, b):
    return lax.dot_general(
        a.astype(BF16), b.astype(BF16), (((1,), (1,)), ((), ())), preferred_element_type=F32
    )


def three(a, b):
    ah, al = split2(a)
    bh, bl = split2(b)
    return one(ah, bh) + one(al, bh) + one(ah, bl)


def three_nt(a, b):
    ah, al = split2(a)
    bh, bl = split2(b)
    return one_nt(ah, bh) + one_nt(al, bh) + one_nt(ah, bl)


def left_exact(a, b):
    bh, bm = split2(b)
    bl = (b - bh.astype(F32) - bm.astype(F32)).astype(BF16)
    return one(a, bh) + one(a, bm) + one(a, bl)


def right_exact(a, b):
    ah, al = split2(a)
    return one(ah, b) + one(al, b)


def iotas(rows, columns):
    return (
        lax.broadcasted_iota(jnp.int32, (rows, columns), 0),
        lax.broadcasted_iota(jnp.int32, (rows, columns), 1),
    )


def sigmoid(x):
    return 1.0 / (1.0 + jnp.exp(-x))


def head_ones():
    i, j = iotas(128, 128)
    return ((i >> 6) == (j >> 6)).astype(BF16)


PAIRS, INVERSE, GATHERED, STEP, READ, CHAIN = one, one, one, one, one, three
PAIRS_NT = one_nt


def spread(a):
    first = lax.broadcasted_iota(jnp.int32, a.shape, 1) < 64
    return jnp.concatenate([jnp.where(first, a, 0.0), jnp.where(first, 0.0, a)], axis=0)


def masks():
    i, j = iotas(128, 128)
    same_head = (i >> 6) == (j >> 6)
    return i, j, same_head


def prepared(keys, values, decay_pre, removal_pre, key_gain, removal_gain, removal_bias, decay_bias, extra):
    ones = head_ones()
    rate = sigmoid(decay_bias + decay_pre) * math.exp(-0.5) + extra
    removal = sigmoid(removal_bias + removal_pre)
    scaled = keys * key_gain
    unit = scaled * lax.rsqrt(right_exact(scaled * scaled, ones) + 1e-06)
    written = keys * (1.0 + (removal - 1.0) * removal_gain)
    beta = unit * removal
    i, j = iotas(BLOCK, BLOCK)
    lower = (i >= j).astype(BF16)
    blocks = []
    for b in range(BLOCKS):
        rows = slice(b * BLOCK, (b + 1) * BLOCK)
        rate_b = rate[rows]
        falling = -left_exact(lower, rate_b)
        before = falling + rate_b
        middle = falling[BLOCK // 2 : BLOCK // 2 + 1]
        ending = falling[BLOCK - 1 :]
        up = jnp.exp(middle - falling)
        to_end = jnp.exp(ending - falling)
        beta_mid = beta[rows] * up
        keys_mid = written[rows] * up
        blocks.append(
            dict(
                falling=falling,
                middle=middle,
                end_decay=jnp.exp(ending),
                left=spread(-unit[rows] * jnp.exp(before - middle)),
                right=jnp.concatenate([beta_mid, beta_mid, keys_mid, keys_mid], axis=0),
                start_alpha=spread(-unit[rows] * jnp.exp(before)),
                end_beta=spread(beta[rows] * to_end).T,
                end_keys=spread(written[rows] * to_end).T,
                values=spread(values[rows]),
            )
        )
    return blocks


def inverted(blocks):
    i, j, same_head = masks()
    strict = same_head & (i > j)
    eye = (i == j).astype(F32)
    sames = [(i >> s) == (j >> s) for s in (3, 4, 5)] + [same_head]
    for block in blocks:
        pairs = PAIRS_NT(block["left"], block["right"])
        block["links"] = jnp.where(strict, pairs[:, :128], 0.0)
        alpha_keys = jnp.where(strict, pairs[:, 128:], 0.0)
        block["local"] = PAIRS(alpha_keys, block["values"])
        block["power"] = base = jnp.where(sames[0], block["links"], 0.0)
        block["inverse"] = eye + base
    for _ in range(2):
        for block in blocks:
            block["power"] = INVERSE(block["power"], block["power"])
        for block in blocks:
            block["inverse"] = block["inverse"] + INVERSE(block["inverse"], block["power"])
    for s in range(3):
        for block in blocks:
            off = jnp.where(sames[s + 1] & ~sames[s], block["links"], 0.0)
            block["part"] = INVERSE(off, block["inverse"])
        for block in blocks:
            block["inverse"] = block["inverse"] + INVERSE(block["inverse"], block["part"])


def transition(blocks):
    i, j, same_head = masks()
    for block in blocks:
        block["gathered"] = GATHERED(
            block["inverse"], jnp.concatenate([block["start_alpha"], block["local"]], axis=1)
        )
    for block in blocks:
        step = STEP(block["end_beta"], block["gathered"])
        block["step_a"] = step[:, :128] + jnp.where(i == j, block["end_decay"], 0.0)
        block["step_b"] = step[:, 128:] + STEP(block["end_keys"], block["values"])
    both = jnp.concatenate([blocks[0]["step_a"], blocks[0]["step_b"]], axis=1)
    for block in blocks[1:]:
        block["start"] = both
        moved = CHAIN(block["step_a"], both)
        both = jnp.concatenate([moved[:, :128], moved[:, 128:] + block["step_b"]], axis=1)
    return both[:, :128], both[:, 128:]


def read_parts(blocks, recept):
    i, j, same_head = masks()
    inclusive = same_head & (i >= j)
    reads_a, reads_b = [], []
    for b, block in enumerate(blocks):
        rows = slice(b * BLOCK, (b + 1) * BLOCK)
        left = spread(recept[rows] * jnp.exp(block["falling"] - block["middle"]))
        pairs = PAIRS_NT(left, block["right"])
        recept_beta = jnp.where(inclusive, pairs[:, :128], 0.0)
        recept_keys = jnp.where(inclusive, pairs[:, 128:], 0.0)
        reads = READ(recept_beta, block["gathered"])
        read_a = reads[:64, :128] + reads[64:, :128] + recept[rows] * jnp.exp(block["falling"])
        read_b = reads[:, 128:] + READ(recept_keys, block["values"])
        read_b = read_b[:64] + read_b[64:]
        if b:
            seen = READ(read_a, block["start"])
            read_a, read_b = seen[:, :128], seen[:, 128:] + read_b
        reads_a.append(read_a)
        reads_b.append(read_b)
    return jnp.concatenate(reads_a, axis=0), jnp.concatenate(reads_b, axis=0)


def local_scan(recept, keys, values, decay_pre, removal_pre, *rest):
    blocks = prepared(keys, values, decay_pre, removal_pre, *rest)
    inverted(blocks)
    trans = transition(blocks)
    return (*trans, *read_parts(blocks, recept))


def packed_heads(trans_a, trans_b):
    lane = lax.broadcasted_iota(jnp.int32, (64, 128), 1)
    head0 = jnp.where(lane < 64, trans_a[:64], pltpu.roll(trans_b[:64], 64, 1))
    head1 = jnp.where(lane < 64, pltpu.roll(trans_a[64:], 64, 1), trans_b[64:])
    return head0, head1


def coded(both):
    i, j = iotas(64, 128)
    on = i == j
    diagonal = jnp.sum(jnp.where(on, both, 0.0), axis=0, keepdims=True)
    high, rest = split2(diagonal)
    low = (diagonal - high.astype(F32) - rest.astype(F32)).astype(BF16)
    row = lax.broadcasted_iota(jnp.int32, (16, 128), 0)
    below = jnp.where(
        row == 0,
        high.astype(F32),
        jnp.where(row == 1, rest.astype(F32), jnp.where(row == 2, low.astype(F32), 0.0)),
    )
    return jnp.concatenate([jnp.where(on, 0.0, both), below], axis=0).astype(BF16)


def decoded(code):
    code = code.astype(F32)
    i, j = iotas(64, 128)
    diagonal = code[64:65] + code[65:66] + code[66:67]
    return jnp.where(i == j, diagonal, code[:64])


def combine(later, total):
    lane = lax.broadcasted_iota(jnp.int32, later.shape, 1)
    return three(later[:, :64], total) + jnp.where(lane < 64, 0.0, later)


NORM_AT = 11
THIN_AT = 3


def kernel(
    tokens,
    norm_gain,
    w0,
    w1,
    w2,
    w3,
    w4,
    w5,
    w6,
    w7,
    out_scan,
    out_conv,
    key_gain,
    removal_gain,
    removal_bias,
    decay_bias,
    extra,
    scan_norm_gain,
    conv_kernel,
    conv_bias,
    conv_norm_gain,
    out,
    weights,
    outs,
    extra_v,
    norm_gain_v,
    conv_kernel_v,
    tok,
    normed,
    proj,
    outw0,
    outw1,
    pair_in,
    line_y,
    line_z,
    state_in,
    state_out,
    pair_out,
    rim,
    conv_in,
    conv_pad,
    stats,
    feats_scan,
    feats_conv,
    reads_a,
    reads_b,
    mine,
    load_sem,
    tok_send,
    tok_recv,
    first_send,
    first_recv,
    second_send,
    plus_recv,
    minus_recv,
    cross_send,
    cross_recv,
    first_send2,
    first_recv2,
    second_send2,
    plus_recv2,
    minus_recv2,
    outw_cross_send,
    outw_cross_recv,
    late_send,
    late_recv,
    outw_send,
    outw_recv,
    outw_load,
    pair_send,
    pair_recv,
    y_send,
    y_recv,
    z_send,
    z_recv,
    state_send,
    state_recv,
    rim_send,
    rim_recv,
    stats_send,
    stats_recv,
    scan_send,
    scan_recv,
    conv_send,
    conv_recv,
):
    z, y, c, x = (lax.axis_index(n) for n in (*SP, "tp"))

    def at(z_=None, y_=None, c_=None, x_=None):
        pick = lambda a, b: a if b is None else b
        return (pick(z, z_), pick(y, y_), pick(c, c_), pick(x, x_))

    def remote(src, dst, send, recv, where):
        return pltpu.make_async_remote_copy(
            src_ref=src, dst_ref=dst, send_sem=send, recv_sem=recv, device_id=where, device_id_type=MESH
        )

    partner = at(c_=1 - c)

    a = (1 - c) * y + c * z
    b = (1 - c) * z + c * y

    loads = [
        pltpu.make_async_copy(tokens, tok.at[x], load_sem.at[0]),
    ]
    for k, w in enumerate((w1, w2, w3, w4)):
        loads.append(
            pltpu.make_async_copy(w, weights.at[c, b, a, :, pl.ds(128 * k, 128)], load_sem.at[k + 1])
        )
    for k, w in enumerate((w0, w5, w6, w7, out_scan, out_conv)):
        loads.append(
            pltpu.make_async_copy(w, outs.at[c, b, a, :, pl.ds(128 * k, 128)], load_sem.at[k + 5])
        )
    loads.append(pltpu.make_async_copy(extra, extra_v, load_sem.at[11]))
    loads.append(pltpu.make_async_copy(norm_gain, norm_gain_v, load_sem.at[12]))
    loads.append(pltpu.make_async_copy(conv_kernel, conv_kernel_v, load_sem.at[13]))
    for load in loads:
        load.start()

    barrier = pltpu.get_barrier_semaphore()
    greeted = [partner]
    for k in range(1, N):
        greeted.append(at(y_=lax.rem(y + k, N)))
        greeted.append(at(z_=lax.rem(z + k, N)))
    for k in range(1, NX):
        greeted.append(at(x_=lax.rem(x + k, NX)))
    place = (z * N + y) * 2 + c
    size = 2 * N * N
    before = lax.rem(place + size - 1, size)
    after = lax.rem(place + 1, size)
    as_device = lambda s: (s // (2 * N), lax.rem(s // 2, N), lax.rem(s, 2), x)
    greeted.append(as_device(before))
    for device in greeted:
        pl.semaphore_signal(barrier, inc=1, device_id=device, device_id_type=MESH)
    pl.semaphore_wait(barrier, len(greeted))
    for load in loads:
        load.wait()

    tok_copies = []
    for k in (1, 3, 2):
        tok_copies.append(
            remote(tok.at[x], tok.at[x], tok_send.at[k - 1], tok_recv.at[k - 1], at(x_=lax.rem(x + k, NX)))
        )
    def along_first(k):
        return at(z_=lax.rem(z + c * k, N), y_=lax.rem(y + (1 - c) * k, N))

    def along_second(k):
        return at(z_=lax.rem(z + (1 - c) * k, N), y_=lax.rem(y + c * k, N))

    class Gather:
        def __init__(self, ref, first_send, first_recv, second_send, plus_recv, minus_recv):
            self.ref, self.first_send, self.first_recv = ref, first_send, first_recv
            self.second_send, self.recvs = second_send, {1: plus_recv, -1: minus_recv}

        def start(self):
            own = self.ref.at[c, b, a]
            for k in (1, 7, 2, 6, 3, 5, 4):
                remote(own, own, self.first_send, self.first_recv.at[a], along_first(k)).start()

        def low(self, h):
            return lax.rem(a // 2 + h, 4) * 2

        def piece(self, h, distance):
            return self.ref.at[c, lax.rem(b + distance + N, N), pl.ds(self.low(h), 2)]

        def copy(self, h, source, sign, reach):
            piece = self.piece(h, -sign * source)
            recv = self.recvs[sign].at[h * 4 + source + reach - 1]
            target = along_second(reach if sign > 0 else N - reach)
            return remote(piece, piece, self.second_send, recv, target)

        def collect(self, h):
            for k in range(2):
                a_ = self.low(h) + k

                def wait():
                    piece = self.ref.at[c, b, a_]
                    remote(piece, piece, self.first_send, self.first_recv.at[a_], partner).wait_recv()

                if h:
                    wait()
                else:
                    pl.when(a_ != a)(wait)

            for reach in (2, 1):
                for sign in (1, -1):
                    self.copy(h, 0, sign, reach).start()
            return [self.piece(h, 0)]

        def has_far(self, h, sign):
            return (h % 2 == 0) == (sign > 0)

        def arrive(self, h, d, sign):
            self.copy(h, 0, sign, d).wait_recv()
            return self.piece(h, -sign * d)

        def relay(self, h):
            pieces = []
            for sign in (1, -1):
                pieces.append(self.arrive(h, 2, sign))
                if self.has_far(h, sign):
                    self.copy(h, 2, sign, 2).start()
                self.copy(h, 2, sign, 1).start()
            return pieces

        def near(self, h):
            return [self.arrive(h, 1, sign) for sign in (1, -1)]

        def far(self, h):
            pieces = [self.arrive(h, 4, sign) for sign in (1, -1) if self.has_far(h, sign)]
            return pieces + [self.arrive(h, 3, sign) for sign in (1, -1)]

        def drain(self):
            seven = self.ref.at[0, 0, pl.ds(0, 7)]
            remote(seven, seven, self.first_send, self.first_recv.at[0], partner).wait_send()
            most = self.ref.at[0, pl.ds(0, 7)]
            remote(most, most, self.second_send, self.first_recv.at[0], partner).wait_send()

    wide = Gather(weights, first_send, first_recv, second_send, plus_recv, minus_recv)
    thin = Gather(outs, first_send2, first_recv2, second_send2, plus_recv2, minus_recv2)
    wide.start()
    for copy in tok_copies:
        copy.start()

    order = (0, 1, 3, 2)
    events = [(wide.collect, h) for h in order]
    for h in order:
        events += [(wide.relay, h), (wide.near, h)]
    events += [(thin.collect, h) for h in order]
    events += [(wide.far, h) for h in order]
    for number, (event, h) in enumerate(events):
        for piece in event(h):
            if event.__self__ is wide:
                remote(piece, piece, cross_send, cross_recv, partner).start()
        if number == THIN_AT:
            thin.start()
        if number == NORM_AT:
            for copy in tok_copies:
                copy.wait_recv()
            square = jnp.zeros((ROWS, 1), F32)
            for q in range(NX):
                t = tok[q].astype(F32)
                square = square + jnp.sum(t * t, axis=-1, keepdims=True)
            factor = lax.rsqrt(square * (1.0 / MODEL) + 1e-06)
            for q in range(NX):
                t = tok[q].astype(F32)
                columns = slice(q * 512, (q + 1) * 512)
                normed[:, columns] = (t * factor * norm_gain_v[:, columns]).astype(BF16)

    everything = weights.at[1 - c]
    remote(everything, everything, cross_send, cross_recv, partner).wait_recv()

    def project(ref, base):
        def columns_of(n, carry):
            columns = pl.ds(pl.multiple_of(n * 256, 256), 256)
            w = jnp.concatenate(
                [
                    ref[p, j if p else i, i if p else j, :, columns]
                    for i in range(N)
                    for j in range(N)
                    for p in range(2)
                ],
                axis=0,
            )
            proj[:, pl.ds(pl.multiple_of(base + n * 256, 256), 256)] = jnp.dot(
                normed[...], w, preferred_element_type=F32
            ).astype(BF16)
            return carry

        lax.fori_loop(0, 2, columns_of, 0)

    project(weights, 0)

    def part(k):
        return proj[:, 128 * k : 128 * (k + 1)].astype(F32)

    blocks = prepared(
        part(0),
        part(1),
        part(2),
        part(3),
        key_gain[...],
        removal_gain[...],
        removal_bias[...],
        decay_bias[...],
        extra_v[...],
    )
    inverted(blocks)
    trans_a, trans_b = transition(blocks)
    head0, head1 = packed_heads(trans_a, trans_b)
    upper = c == 1
    pair_out[...] = jnp.where(upper, head0, head1)
    mine[...] = jnp.where(upper, head1, head0)
    pair_copy = remote(pair_out, pair_in, pair_send, pair_recv, partner)
    pair_copy.start()
    pair_copy.wait_recv()
    earlier = jnp.where(upper, pair_in[...], mine[...])
    later = jnp.where(upper, mine[...], pair_in[...])
    line_y[y] = coded(combine(later, earlier))
    for k in (4, 3, 5, 2, 6, 1, 7):
        remote(line_y.at[y], line_y.at[y], y_send, y_recv.at[y], at(y_=lax.rem(y + k, N))).start()

    for h in order:
        thin.relay(h)

    lane = lax.broadcasted_iota(jnp.int32, (64, 128), 1)
    i, j = iotas(64, 128)
    blank = (i == j).astype(F32)
    total = inside = blank
    for k in range(N):

        @pl.when(y != k)
        def _():
            remote(line_y.at[k], line_y.at[k], y_send, y_recv.at[k], partner).wait_recv()

        total = combine(decoded(line_y[k]), total)
        inside = jnp.where(k < y, total, inside)
    line_z[z] = coded(total)
    z_copies = []
    for k in range(N - 1, 0, -1):
        copy = remote(
            line_z.at[z], line_z.at[z], z_send.at[k - 1], z_recv.at[z], at(z_=lax.rem(z + k, N))
        )
        z_copies.append((k, copy))

        @pl.when(z + k < N)
        def _():
            copy.start()

    for h in order:
        thin.near(h)
        thin.far(h)
    own_paths = outs.at[c, :, :, :, pl.ds(0, 512)]
    other_paths = outs.at[1 - c, :, :, :, pl.ds(0, 512)]
    late_cross = remote(own_paths, own_paths, late_send, late_recv, partner)
    late_cross.start()
    def outw_copies(p):
        for k in (1, 3, 2, 0):
            x_ = lax.rem(x + k, NX)
            if p:
                src, dst = outs.at[1, :, pl.ds(2 * x_, 2), :, pl.ds(512, 256)], outw1.at[x]
            else:
                src, dst = outs.at[0, pl.ds(2 * x_, 2), :, :, pl.ds(512, 256)], outw0.at[x]
            if k:
                yield remote(src, dst, outw_send.at[k - 1], outw_recv.at[k - 1], at(x_=x_))
            else:
                yield pltpu.make_async_copy(src, dst, outw_load)

    for p in range(2):

        @pl.when(c == p)
        def _():
            for copy in outw_copies(p):
                copy.start()

    outw_waits = list(outw_copies(0))

    remote(other_paths, other_paths, late_send, late_recv, partner).wait_recv()
    project(outs, 512)

    conv_in[...] = (part(6) * sigmoid(part(7))).astype(BF16)
    last = place == size - 1
    start = place == 0
    rim_copy = remote(conv_in.at[pl.ds(ROWS - 32, 32)], rim, rim_send, rim_recv, as_device(after))

    @pl.when(jnp.logical_not(last))
    def _():
        rim_copy.start()

    reads_a[...], reads_b[...] = read_parts(blocks, part(4))

    @pl.when(start)
    def _():
        rim[...] = jnp.zeros_like(rim)

    @pl.when(jnp.logical_not(start))
    def _():
        rim_copy.wait_recv()

    conv_pad[pl.ds(0, 32)] = rim[...].astype(F32)
    conv_pad[pl.ds(32, ROWS)] = conv_in[...].astype(F32)
    filtered = conv_bias[...] + conv_kernel_v[0:1] * conv_pad[pl.ds(2, ROWS)]
    for k in range(1, CONV_K):
        filtered = filtered + conv_kernel_v[k : k + 1] * conv_pad[pl.ds(2 + k, ROWS)]
    near = jnp.mean(filtered, axis=-1, keepdims=True)
    around = jnp.sum((filtered - near) ** 2, axis=-1, keepdims=True)
    lane = lax.broadcasted_iota(jnp.int32, (ROWS, 128), 1)
    stats[x] = jnp.where(lane == 0, near, jnp.where(lane == 1, around, 0.0)).T[:8]
    conv_pad[pl.ds(0, ROWS)] = filtered
    stats_copies = [
        remote(stats.at[x], stats.at[x], stats_send.at[k - 1], stats_recv.at[k - 1], at(x_=lax.rem(x + k, NX)))
        for k in (1, 3, 2)
    ]
    for copy in stats_copies:
        copy.start()

    for copy in outw_waits[:3]:
        copy.wait_recv()
    outw_waits[3].wait()
    for p, ref in enumerate((outw0, outw1)):

        @pl.when(c == p)
        def _():
            remote(ref, ref, outw_cross_send, outw_cross_recv, partner).start()

    lane = lax.broadcasted_iota(jnp.int32, (64, 128), 1)

    for copy in stats_copies:
        copy.wait_recv()
    center = sum(stats[q][0:1] for q in range(NX)) * (1.0 / NX)
    spread_row = jnp.zeros((1, ROWS), F32)
    for q in range(NX):
        gap = stats[q][0:1] - center
        spread_row = spread_row + stats[q][1:2] + 128.0 * gap * gap
    row = lax.broadcasted_iota(jnp.int32, (8, ROWS), 0)
    scale_row = lax.rsqrt(spread_row * (1.0 / 512.0) + 1e-05)
    column = jnp.where(row == 0, center, jnp.where(row == 1, scale_row, 0.0)).T
    normal = (conv_pad[pl.ds(0, ROWS)] - column[:, 0:1]) * column[:, 1:2] * conv_norm_gain[...]
    feats_conv[x] = (normal * sigmoid(normal)).astype(BF16)
    conv_copies = [
        remote(
            feats_conv.at[x], feats_conv.at[x], conv_send.at[k - 1], conv_recv.at[k - 1], at(x_=lax.rem(x + k, NX))
        )
        for k in (1, 3, 2)
    ]
    for copy in conv_copies:
        copy.start()

    def advance(k, state):
        remote(line_z.at[k], line_z.at[k], z_send.at[0], z_recv.at[k], partner).wait_recv()
        return combine(decoded(line_z[k]), state)

    state = lax.fori_loop(0, z, advance, jnp.zeros((64, 128), F32))
    state = jnp.where(lane < 64, 0.0, combine(inside, state))
    passed = combine(jnp.where(upper, pair_in[...], mine[...]), state)
    here = jnp.where(upper, passed, state)
    state_out[...] = jnp.where(upper, state, passed)
    state_copy = remote(state_out, state_in, state_send, state_recv, partner)
    state_copy.start()

    for copy in conv_copies:
        copy.wait_recv()
    outw_cross = remote(outw0, outw0, outw_cross_send, outw_cross_recv, partner)
    outw_cross.wait_recv()

    def w_of(q, h):
        columns = pl.ds(128 * h, 128)
        return jnp.concatenate(
            [
                (outw1[q, j, i, :, columns] if p else outw0[q, i, j, :, columns])
                for i in range(2)
                for j in range(N)
                for p in range(2)
            ],
            axis=0,
        )

    total_out = one_nt(feats_conv[0], w_of(0, 1))
    for q in range(1, NX):
        total_out = total_out + one_nt(feats_conv[q], w_of(q, 1))

    state_copy.wait_recv()
    there = state_in[...]
    state0 = jnp.where(upper, there, here)
    state1 = jnp.where(upper, here, there)
    whole = jnp.concatenate(
        [
            jnp.where(lane < 64, pltpu.roll(state0, 64, 1), 0.0),
            jnp.where(lane < 64, 0.0, state1),
        ],
        axis=0,
    )
    reads = three(reads_a[...], whole) + reads_b[...]
    ones = head_ones()
    reads = reads - right_exact(reads, ones) * (1.0 / 64.0)
    spread = right_exact(reads * reads, ones) * (1.0 / 64.0)
    feats_scan[x] = (
        reads * lax.rsqrt(spread + 0.00064) * scan_norm_gain[...] * sigmoid(part(5))
    ).astype(BF16)
    scan_copies = [
        remote(
            feats_scan.at[x], feats_scan.at[x], scan_send.at[k - 1], scan_recv.at[k - 1], at(x_=lax.rem(x + k, NX))
        )
        for k in (1, 3, 2)
    ]
    for copy in scan_copies:
        copy.start()
    for copy in scan_copies:
        copy.wait_recv()
    for q in range(NX):
        total_out = total_out + one_nt(feats_scan[q], w_of(q, 0))
    out[...] = total_out.astype(BF16)

    for copies in (tok_copies, outw_waits[:3], stats_copies, conv_copies, scan_copies):
        for copy in copies:
            copy.wait_send()
    pair_copy.wait_send()
    state_copy.wait_send()
    wide.drain()
    thin.drain()
    outw_cross.wait_send()
    late_cross.wait_send()
    remote(everything, everything, cross_send, cross_recv, partner).wait_send()
    lines = line_y.at[pl.ds(0, 7)]
    remote(lines, lines, y_send, y_recv.at[0], partner).wait_send()

    @pl.when(jnp.logical_not(last))
    def _():
        rim_copy.wait_send()

    for k, copy in z_copies:

        @pl.when(z + k < N)
        def _():
            copy.wait_send()


def shards(
    tokens,
    norm_gain,
    query_weight,
    key_weight,
    value_weight,
    decay_weight,
    removal_weight,
    gate_weight,
    key_gain,
    removal_gain,
    removal_bias,
    decay_bias,
    decay_extra,
    scan_norm_gain,
    conv_value_weight,
    conv_gate_weight,
    conv_kernel,
    conv_bias,
    conv_norm_gain,
    out_scan_weight,
    out_conv_weight,
):
    row = lambda v: v.reshape(1, -1)
    anywhere = pl.BlockSpec(memory_space=pl.ANY)
    inside = pl.BlockSpec(memory_space=pltpu.VMEM)
    dma = pltpu.SemaphoreType.DMA
    return pl.pallas_call(
        kernel,
        out_shape=jax.ShapeDtypeStruct((ROWS, 512), BF16),
        in_specs=[anywhere] * 12 + [inside] * 4 + [anywhere] + [inside] + [anywhere] + [inside] * 2,
        out_specs=inside,
        scratch_shapes=[
            pltpu.VMEM((2, N, N, 16, 512), BF16),
            pltpu.VMEM((2, N, N, 16, 768), BF16),
            pltpu.VMEM((ROWS, 128), F32),
            pltpu.VMEM((1, MODEL), F32),
            pltpu.VMEM((CONV_K, 128), F32),
            pltpu.VMEM((NX, ROWS, 512), BF16),
            pltpu.VMEM((ROWS, MODEL), BF16),
            pltpu.VMEM((ROWS, PROJ), BF16),
            pltpu.VMEM((NX, 2, N, 16, 256), BF16),
            pltpu.VMEM((NX, N, 2, 16, 256), BF16),
            pltpu.VMEM((64, 128), F32),
            pltpu.VMEM((N, 80, 128), BF16),
            pltpu.VMEM((N, 80, 128), BF16),
            pltpu.VMEM((64, 128), F32),
            pltpu.VMEM((64, 128), F32),
            pltpu.VMEM((64, 128), F32),
            pltpu.VMEM((32, 128), BF16),
            pltpu.VMEM((ROWS, 128), BF16),
            pltpu.VMEM((ROWS + 32, 128), F32),
            pltpu.VMEM((NX, 8, ROWS), F32),
            pltpu.VMEM((NX, ROWS, 128), BF16),
            pltpu.VMEM((NX, ROWS, 128), BF16),
            pltpu.VMEM((ROWS, 128), F32),
            pltpu.VMEM((ROWS, 128), F32),
            pltpu.VMEM((64, 128), F32),
            dma((14,)),
            dma((3,)),
            dma((3,)),
            dma(()),
            dma((8,)),
            dma(()),
            dma((16,)),
            dma((16,)),
            dma(()),
            dma(()),
            dma(()),
            dma((8,)),
            dma(()),
            dma((16,)),
            dma((16,)),
            dma(()),
            dma(()),
            dma(()),
            dma(()),
            dma((3,)),
            dma((3,)),
            dma(()),
            dma(()),
            dma(()),
            dma(()),
            dma((N,)),
            dma((N - 1,)),
            dma((N,)),
            dma(()),
            dma(()),
            dma(()),
            dma(()),
            dma((3,)),
            dma((3,)),
            dma((3,)),
            dma((3,)),
            dma((3,)),
            dma((3,)),
        ],
        compiler_params=pltpu.CompilerParams(
            collective_id=0, has_side_effects=True, vmem_limit_bytes=56 * 1024 * 1024
        ),
    )(
        tokens,
        row(norm_gain),
        query_weight,
        key_weight,
        value_weight,
        decay_weight,
        removal_weight,
        gate_weight,
        conv_value_weight,
        conv_gate_weight,
        out_scan_weight.T,
        out_conv_weight.T,
        row(key_gain),
        row(removal_gain),
        row(removal_bias),
        row(decay_bias),
        decay_extra,
        row(scan_norm_gain),
        conv_kernel,
        row(conv_bias),
        row(conv_norm_gain),
    )


def solution(mesh):
    torus = Mesh(mesh.devices.reshape(N, N, 2, mesh.shape["tp"]), (*SP, "tp"))
    in_specs = (
        P(SP, "tp"),
        P(),
        P(SP, "tp"),
        P(SP, "tp"),
        P(SP, "tp"),
        P(SP, "tp"),
        P(SP, "tp"),
        P(SP, "tp"),
        P("tp"),
        P("tp"),
        P("tp"),
        P("tp"),
        P(SP, "tp"),
        P("tp"),
        P(SP, "tp"),
        P(SP, "tp"),
        P(None, "tp"),
        P("tp"),
        P("tp"),
        P("tp", SP),
        P("tp", SP),
    )
    return jax.shard_map(
        shards, mesh=torus, in_specs=in_specs, out_specs=P(SP, "tp"), check_vma=False
    )
```

```python
import functools
import math

import jax
import jax.numpy as jnp
from jax import lax
from jax.experimental import pallas as pl
from jax.experimental.pallas import tpu as pltpu
from jax.sharding import Mesh
from jax.sharding import PartitionSpec as P

F32 = jnp.float32
BF16 = jnp.bfloat16
SP = ("sp_0", "sp_1", "sp_2")
MESH = pl.DeviceIdType.MESH
CONV_K = 31
ROWS = 192
BLOCK = 64
BLOCKS = ROWS // BLOCK
MODEL = 2048
NX = 4
PROJ = 1024
N = 8


def split2(a):
    high = a.astype(BF16)
    return high, (a - high.astype(F32)).astype(BF16)


def one(a, b):
    return jnp.dot(a.astype(BF16), b.astype(BF16), preferred_element_type=F32)


def one_nt(a, b):
    return lax.dot_general(
        a.astype(BF16), b.astype(BF16), (((1,), (1,)), ((), ())), preferred_element_type=F32
    )


def three(a, b):
    ah, al = split2(a)
    bh, bl = split2(b)
    return one(ah, bh) + one(al, bh) + one(ah, bl)


def three_nt(a, b):
    ah, al = split2(a)
    bh, bl = split2(b)
    return one_nt(ah, bh) + one_nt(al, bh) + one_nt(ah, bl)


def left_exact(a, b):
    bh, bm = split2(b)
    bl = (b - bh.astype(F32) - bm.astype(F32)).astype(BF16)
    return one(a, bh) + one(a, bm) + one(a, bl)


def right_exact(a, b):
    ah, al = split2(a)
    return one(ah, b) + one(al, b)


def iotas(rows, columns):
    return (
        lax.broadcasted_iota(jnp.int32, (rows, columns), 0),
        lax.broadcasted_iota(jnp.int32, (rows, columns), 1),
    )


def sigmoid(x):
    return 1.0 / (1.0 + jnp.exp(-x))


def head_ones():
    i, j = iotas(128, 128)
    return ((i >> 6) == (j >> 6)).astype(BF16)


PAIRS, INVERSE, GATHERED, STEP, READ, CHAIN = one, one, one, one, one, three
PAIRS_NT = one_nt


def spread(a):
    first = lax.broadcasted_iota(jnp.int32, a.shape, 1) < 64
    return jnp.concatenate([jnp.where(first, a, 0.0), jnp.where(first, 0.0, a)], axis=0)


def masks():
    i, j = iotas(128, 128)
    same_head = (i >> 6) == (j >> 6)
    return i, j, same_head


def prepared(keys, values, decay_pre, removal_pre, key_gain, removal_gain, removal_bias, decay_bias, extra):
    ones = head_ones()
    rate = sigmoid(decay_bias + decay_pre) * math.exp(-0.5) + extra
    removal = sigmoid(removal_bias + removal_pre)
    scaled = keys * key_gain
    unit = scaled * lax.rsqrt(right_exact(scaled * scaled, ones) + 1e-06)
    written = keys * (1.0 + (removal - 1.0) * removal_gain)
    beta = unit * removal
    i, j = iotas(BLOCK, BLOCK)
    lower = (i >= j).astype(BF16)
    blocks = []
    for b in range(BLOCKS):
        rows = slice(b * BLOCK, (b + 1) * BLOCK)
        rate_b = rate[rows]
        falling = -left_exact(lower, rate_b)
        before = falling + rate_b
        middle = falling[BLOCK // 2 : BLOCK // 2 + 1]
        ending = falling[BLOCK - 1 :]
        up = jnp.exp(middle - falling)
        to_end = jnp.exp(ending - falling)
        beta_mid = beta[rows] * up
        keys_mid = written[rows] * up
        blocks.append(
            dict(
                falling=falling,
                middle=middle,
                end_decay=jnp.exp(ending),
                left=spread(-unit[rows] * jnp.exp(before - middle)),
                right=jnp.concatenate([beta_mid, beta_mid, keys_mid, keys_mid], axis=0),
                start_alpha=spread(-unit[rows] * jnp.exp(before)),
                end_beta=spread(beta[rows] * to_end).T,
                end_keys=spread(written[rows] * to_end).T,
                values=spread(values[rows]),
            )
        )
    return blocks


def inverted(blocks):
    i, j, same_head = masks()
    strict = same_head & (i > j)
    eye = (i == j).astype(F32)
    sames = [(i >> s) == (j >> s) for s in (3, 4, 5)] + [same_head]
    for block in blocks:
        pairs = PAIRS_NT(block["left"], block["right"])
        block["links"] = jnp.where(strict, pairs[:, :128], 0.0)
        alpha_keys = jnp.where(strict, pairs[:, 128:], 0.0)
        block["local"] = PAIRS(alpha_keys, block["values"])
        block["power"] = base = jnp.where(sames[0], block["links"], 0.0)
        block["inverse"] = eye + base
    for _ in range(2):
        for block in blocks:
            block["power"] = INVERSE(block["power"], block["power"])
        for block in blocks:
            block["inverse"] = block["inverse"] + INVERSE(block["inverse"], block["power"])
    for s in range(3):
        for block in blocks:
            off = jnp.where(sames[s + 1] & ~sames[s], block["links"], 0.0)
            block["part"] = INVERSE(off, block["inverse"])
        for block in blocks:
            block["inverse"] = block["inverse"] + INVERSE(block["inverse"], block["part"])


def transition(blocks):
    i, j, same_head = masks()
    for block in blocks:
        block["gathered"] = GATHERED(
            block["inverse"], jnp.concatenate([block["start_alpha"], block["local"]], axis=1)
        )
    for block in blocks:
        step = STEP(block["end_beta"], block["gathered"])
        block["step_a"] = step[:, :128] + jnp.where(i == j, block["end_decay"], 0.0)
        block["step_b"] = step[:, 128:] + STEP(block["end_keys"], block["values"])
    both = jnp.concatenate([blocks[0]["step_a"], blocks[0]["step_b"]], axis=1)
    for block in blocks[1:]:
        block["start"] = both
        moved = CHAIN(block["step_a"], both)
        both = jnp.concatenate([moved[:, :128], moved[:, 128:] + block["step_b"]], axis=1)
    return both[:, :128], both[:, 128:]


def read_parts(blocks, recept):
    i, j, same_head = masks()
    inclusive = same_head & (i >= j)
    reads_a, reads_b = [], []
    for b, block in enumerate(blocks):
        rows = slice(b * BLOCK, (b + 1) * BLOCK)
        left = spread(recept[rows] * jnp.exp(block["falling"] - block["middle"]))
        pairs = PAIRS_NT(left, block["right"])
        recept_beta = jnp.where(inclusive, pairs[:, :128], 0.0)
        recept_keys = jnp.where(inclusive, pairs[:, 128:], 0.0)
        reads = READ(recept_beta, block["gathered"])
        read_a = reads[:64, :128] + reads[64:, :128] + recept[rows] * jnp.exp(block["falling"])
        read_b = reads[:, 128:] + READ(recept_keys, block["values"])
        read_b = read_b[:64] + read_b[64:]
        if b:
            seen = READ(read_a, block["start"])
            read_a, read_b = seen[:, :128], seen[:, 128:] + read_b
        reads_a.append(read_a)
        reads_b.append(read_b)
    return jnp.concatenate(reads_a, axis=0), jnp.concatenate(reads_b, axis=0)


def local_scan(recept, keys, values, decay_pre, removal_pre, *rest):
    blocks = prepared(keys, values, decay_pre, removal_pre, *rest)
    inverted(blocks)
    trans = transition(blocks)
    return (*trans, *read_parts(blocks, recept))


def packed_heads(trans_a, trans_b):
    lane = lax.broadcasted_iota(jnp.int32, (64, 128), 1)
    head0 = jnp.where(lane < 64, trans_a[:64], pltpu.roll(trans_b[:64], 64, 1))
    head1 = jnp.where(lane < 64, pltpu.roll(trans_a[64:], 64, 1), trans_b[64:])
    return head0, head1


def coded(both):
    i, j = iotas(64, 128)
    on = i == j
    diagonal = jnp.sum(jnp.where(on, both, 0.0), axis=0, keepdims=True)
    high, rest = split2(diagonal)
    low = (diagonal - high.astype(F32) - rest.astype(F32)).astype(BF16)
    row = lax.broadcasted_iota(jnp.int32, (16, 128), 0)
    below = jnp.where(
        row == 0,
        high.astype(F32),
        jnp.where(row == 1, rest.astype(F32), jnp.where(row == 2, low.astype(F32), 0.0)),
    )
    return jnp.concatenate([jnp.where(on, 0.0, both), below], axis=0).astype(BF16)


def decoded(code):
    code = code.astype(F32)
    i, j = iotas(64, 128)
    diagonal = code[64:65] + code[65:66] + code[66:67]
    return jnp.where(i == j, diagonal, code[:64])


def combine(later, total):
    lane = lax.broadcasted_iota(jnp.int32, later.shape, 1)
    return three(later[:, :64], total) + jnp.where(lane < 64, 0.0, later)


FIRST = 256
SECOND = 384


def joined(ref, base, c, first):
    columns = pl.ds(base, first)
    rows = []
    for i in range(N):
        for j in range(N):
            b_ = (1 - c) * i + c * j
            a_ = (1 - c) * j + c * i
            rows.append(ref[b_, a_, :, :, columns].reshape(32, first))
    return jnp.concatenate(rows, axis=0)


def kernel(
    tokens,
    norm_gain,
    w0,
    w1,
    w2,
    w3,
    w4,
    w5,
    w6,
    w7,
    out_scan,
    out_conv,
    key_gain,
    removal_gain,
    removal_bias,
    decay_bias,
    extra,
    scan_norm_gain,
    conv_kernel,
    conv_bias,
    conv_norm_gain,
    out,
    mine1,
    mine2,
    weights,
    later,
    extras,
    norm_gain_v,
    tok,
    normed,
    proj,
    outw0,
    outw1,
    line_y,
    line_z,
    rim,
    conv_in,
    conv_pad,
    stats,
    send_scan,
    send_conv,
    feats_scan,
    feats_conv,
    reads_a,
    reads_b,
    load_sem,
    tok_send,
    tok_recv,
    share_send,
    share_recv,
    wide_sems,
    wide_first,
    wide_plus,
    wide_minus,
    thin_sems,
    thin_first,
    thin_plus,
    thin_minus,
    outw_send,
    outw_recv,
    outw_load,
    outw_cross_send,
    outw_cross_recv,
    y_send,
    y_recv,
    z_send,
    z_recv,
    rim_send,
    rim_recv,
    stats_send,
    stats_recv,
    scan_send,
    scan_recv,
    conv_send,
    conv_recv,
):
    z, y, c, x = (lax.axis_index(n) for n in (*SP, "tp"))
    upper = c == 1

    def at(z_=None, y_=None, c_=None, x_=None):
        pick = lambda a, b: a if b is None else b
        return (pick(z, z_), pick(y, y_), pick(c, c_), pick(x, x_))

    def remote(src, dst, send, recv, where):
        return pltpu.make_async_remote_copy(
            src_ref=src, dst_ref=dst, send_sem=send, recv_sem=recv, device_id=where, device_id_type=MESH
        )

    partner = at(c_=1 - c)
    a = (1 - c) * y + c * z
    b = (1 - c) * z + c * y

    loads = [
        pltpu.make_async_copy(tokens, tok.at[x], load_sem.at[0]),
        pltpu.make_async_copy(extra, extras.at[c], load_sem.at[1]),
        pltpu.make_async_copy(norm_gain, norm_gain_v, load_sem.at[2]),
    ]
    for load in loads:
        load.start()

    barrier = pltpu.get_barrier_semaphore()
    greeted = [partner]
    for k in range(1, N):
        for core in range(2):
            greeted.append(at(y_=lax.rem(y + k, N), c_=core))
            greeted.append(at(z_=lax.rem(z + k, N), c_=core))
    for k in range(1, NX):
        for core in range(2):
            greeted.append(at(x_=lax.rem(x + k, NX), c_=core))
    chip = z * N + y
    before = lax.rem(chip + N * N - 1, N * N)
    after = lax.rem(chip + 1, N * N)
    greeted.append((before // N, lax.rem(before, N), c, x))
    for device in greeted:
        pl.semaphore_signal(barrier, inc=1, device_id=device, device_id_type=MESH)

    lane16 = lax.broadcasted_iota(jnp.int32, (16, 128), 1) < 64

    def halves(left, right):
        left, right = left.astype(F32), right.astype(F32)
        first = jnp.where(lane16, left, pltpu.roll(right, 64, 1))
        return first.astype(BF16), jnp.where(lane16, pltpu.roll(left, 64, 1), right).astype(BF16)

    for k, (left, right) in enumerate(((w1, w2), (w3, w4))):
        for core, part_ in enumerate(halves(left[...], right[...])):
            mine1[core, :, 128 * k : 128 * (k + 1)] = part_
    for k, (left, right) in enumerate(((w0, w5), (w6, w7))):
        for core, part_ in enumerate(halves(left[...], right[...])):
            mine2[core, :, 128 * k : 128 * (k + 1)] = part_
    mine2[0, :, 256:384] = out_scan[...]
    mine2[1, :, 256:384] = out_conv[...]

    pl.semaphore_wait(barrier, len(greeted))

    class Gather:
        def __init__(self, own, ref, sems, first_recv, plus_recv, minus_recv):
            self.own, self.ref, self.first_recv = own, ref, first_recv
            self.first_send, self.second_send, self.keep, self.pair_send = (sems.at[k] for k in range(4))
            self.recvs = {1: plus_recv, -1: minus_recv}

        def start(self):
            for k in (0, 1, 7, 2, 6, 3, 5, 4):
                for core in range(2):
                    a_, b_ = (y, z) if core == 0 else (z, y)
                    target = (z, lax.rem(y + k, N), 0, x) if core == 0 else (lax.rem(z + k, N), y, 1, x)
                    src, dst = self.own.at[core], self.ref.at[b_, a_, c]
                    recv = self.first_recv.at[2 * a_ + c]
                    copy = remote(src, dst, self.first_send if k else self.pair_send, recv, target)
                    if k:
                        copy.start()
                    else:

                        @pl.when(c != core)
                        def _():
                            copy.start()

                        @pl.when(c == core)
                        def _():
                            pltpu.make_async_copy(src, dst, self.keep).start()

        def low(self, h):
            return lax.rem(a // 2 + h, 4) * 2

        def piece(self, h, distance):
            return self.ref.at[lax.rem(b + distance + N, N), pl.ds(self.low(h), 2)]

        def copy(self, h, source, sign, reach):
            piece = self.piece(h, -sign * source)
            recv = self.recvs[sign].at[h * 4 + source + reach - 1]
            k = reach if sign > 0 else N - reach
            target = at(z_=lax.rem(z + (1 - c) * k, N), y_=lax.rem(y + c * k, N))
            return remote(piece, piece, self.second_send, recv, target)

        def collect(self, h):
            for k in range(2):
                a_ = self.low(h) + k
                for core in range(2):
                    piece = self.ref.at[b, a_, core]

                    def wait():
                        recv = self.first_recv.at[2 * a_ + core]
                        remote(piece, piece, self.first_send, recv, partner).wait_recv()

                    if h:
                        wait()
                    else:
                        own = jnp.logical_and(a_ == a, c == core)
                        pl.when(jnp.logical_not(own))(wait)
            if h == 0:
                own = self.ref.at[b, a, c]
                pltpu.make_async_copy(own, own, self.keep).wait()
            for reach in (2, 1):
                for sign in (1, -1):
                    self.copy(h, 0, sign, reach).start()

        def has_far(self, h, sign):
            return (h % 2 == 0) == (sign > 0)

        def arrive(self, h, d, sign):
            self.copy(h, 0, sign, d).wait_recv()

        def relay(self, h):
            for sign in (1, -1):
                self.arrive(h, 2, sign)
                if self.has_far(h, sign):
                    self.copy(h, 2, sign, 2).start()
                self.copy(h, 2, sign, 1).start()

        def near(self, h):
            for sign in (1, -1):
                self.arrive(h, 1, sign)

        def far(self, h):
            for sign in (1, -1):
                if self.has_far(h, sign):
                    self.arrive(h, 4, sign)
                self.arrive(h, 3, sign)

        def drain(self):
            fourteen = self.ref.at[0, pl.ds(0, 7)]
            remote(fourteen, fourteen, self.first_send, self.first_recv.at[0], partner).wait_send()
            single = self.ref.at[0, 7, 0]
            remote(single, single, self.pair_send, self.first_recv.at[0], partner).wait_send()
            most = self.ref.at[pl.ds(0, 7)]
            remote(most, most, self.second_send, self.first_recv.at[0], partner).wait_send()

    wide = Gather(mine1, weights, wide_sems, wide_first, wide_plus, wide_minus)
    thin = Gather(mine2, later, thin_sems, thin_first, thin_plus, thin_minus)
    wide.start()
    for load in loads:
        load.wait()
    tok_copies = [
        remote(tok.at[x], tok.at[x], tok_send.at[k - 1], tok_recv.at[k - 1], at(x_=lax.rem(x + k, NX)))
        for k in (1, 3, 2)
    ]
    for copy in tok_copies:
        copy.start()
    extra_copy = remote(extras.at[c], extras.at[c], share_send.at[0], share_recv.at[0], partner)
    extra_copy.start()
    normed_copy = remote(normed.at[c], normed.at[c], share_send.at[1], share_recv.at[1], partner)

    order = (0, 1, 3, 2)
    for h in order:
        wide.collect(h)
    thin.start()
    for h in order:
        wide.relay(h)
    for copy in tok_copies:
        copy.wait_recv()
    square = jnp.zeros((ROWS, 1), F32)
    for q in range(NX):
        t = tok[q].astype(F32)
        square = square + jnp.sum(t * t, axis=-1, keepdims=True)
    factor = lax.rsqrt(square * (1.0 / MODEL) + 1e-06)
    for q in range(NX):
        t = tok[q].astype(F32)
        columns = slice(q * 512, (q + 1) * 512)
        normed[c, :, columns] = (t * factor * norm_gain_v[:, columns]).astype(BF16)
    normed_copy.start()
    for h in order:
        thin.collect(h)
    for h in order:
        wide.near(h)
    extra_copy.wait_recv()
    normed_copy.wait_recv()
    for h in order:
        wide.far(h)

    lane = lax.broadcasted_iota(jnp.int32, (ROWS, 128), 1) < 64

    def turned(v):
        return pltpu.roll(v, 64, 1)

    def own_head(v):
        low = lax.broadcasted_iota(jnp.int32, v.shape, 1) < 64
        other = turned(v)
        return jnp.where(upper, jnp.where(low, other, v), jnp.where(low, v, other))

    def project(ref, base, width, target):
        w = joined(ref, base, c, width)
        for half in range(2):
            proj[half, :, target : target + width] = jnp.dot(
                normed[half], w, preferred_element_type=F32
            ).astype(BF16)

    def parts(k):
        columns = slice(128 * k, 128 * (k + 1))
        p0, p1 = proj[0, :, columns].astype(F32), proj[1, :, columns].astype(F32)
        return jnp.where(lane, p0, turned(p1)), jnp.where(lane, turned(p0), p1)

    project(weights, 0, FIRST, 0)
    keys, values = parts(0)
    decay_pre, removal_pre = parts(1)
    e0, e1 = extras[0], extras[1]
    own_extra = jnp.where(
        upper, jnp.where(lane, turned(e0), e1), jnp.where(lane, e0, turned(e1))
    )
    blocks = prepared(
        keys,
        values,
        decay_pre,
        removal_pre,
        own_head(key_gain[...]),
        own_head(removal_gain[...]),
        own_head(removal_bias[...]),
        own_head(decay_bias[...]),
        own_extra,
    )
    inverted(blocks)
    half0, half1 = packed_heads(*transition(blocks))
    line_y[y] = coded(combine(half1, half0))
    for k in (4, 3, 5, 2, 6, 1, 7):
        remote(line_y.at[y], line_y.at[y], y_send, y_recv.at[y], at(y_=lax.rem(y + k, N))).start()
    for h in order:
        thin.relay(h)

    lane64 = lax.broadcasted_iota(jnp.int32, (64, 128), 1)
    i, j = iotas(64, 128)
    total = inside = (i == j).astype(F32)
    for k in range(N):

        @pl.when(y != k)
        def _():
            remote(line_y.at[k], line_y.at[k], y_send, y_recv.at[k], partner).wait_recv()

        total = combine(decoded(line_y[k]), total)
        inside = jnp.where(k < y, total, inside)
    line_z[z] = coded(total)
    z_copies = []
    for k in range(N - 1, 0, -1):
        copy = remote(
            line_z.at[z], line_z.at[z], z_send.at[k - 1], z_recv.at[z], at(z_=lax.rem(z + k, N))
        )
        z_copies.append((k, copy))

        @pl.when(z + k < N)
        def _():
            copy.start()

    for h in order:
        thin.near(h)
        thin.far(h)

    def outw_copies(p):
        for k in (1, 3, 2, 0):
            x_ = lax.rem(x + k, NX)
            if p:
                src, dst = later.at[:, pl.ds(2 * x_, 2), :, :, pl.ds(256, 128)], outw1.at[x]
            else:
                src, dst = later.at[pl.ds(2 * x_, 2), :, :, :, pl.ds(256, 128)], outw0.at[x]
            if k:
                yield remote(src, dst, outw_send.at[k - 1], outw_recv.at[k - 1], at(x_=x_))
            else:
                yield pltpu.make_async_copy(src, dst, outw_load)

    for p in range(2):

        @pl.when(c == p)
        def _():
            for copy in outw_copies(p):
                copy.start()

    outw_waits = list(outw_copies(0))

    project(later, 0, 256, 256)
    conv_value, conv_gate = parts(3)
    conv_in[...] = (conv_value * sigmoid(conv_gate)).astype(BF16)
    last = chip == N * N - 1
    start = chip == 0
    rim_copy = remote(
        conv_in.at[pl.ds(ROWS - 32, 32)], rim, rim_send, rim_recv, (after // N, lax.rem(after, N), c, x)
    )

    @pl.when(jnp.logical_not(last))
    def _():
        rim_copy.start()

    recept, gate_pre = parts(2)
    reads_a[...], reads_b[...] = read_parts(blocks, recept)

    @pl.when(start)
    def _():
        rim[...] = jnp.zeros_like(rim)

    @pl.when(jnp.logical_not(start))
    def _():
        rim_copy.wait_recv()

    ending = conv_in[pl.ds(ROWS - 32, 32)].astype(F32)
    conv_pad[pl.ds(0, 32)] = turned(jnp.where(lane[:32], ending, rim[...].astype(F32)))
    conv_pad[pl.ds(32, ROWS)] = conv_in[...].astype(F32)
    taps = own_head(conv_kernel[...])
    filtered = own_head(conv_bias[...]) + taps[0:1] * conv_pad[pl.ds(2, ROWS)]
    for k in range(1, CONV_K):
        filtered = filtered + taps[k : k + 1] * conv_pad[pl.ds(2 + k, ROWS)]
    ones = head_ones()
    near = right_exact(filtered, ones) * (1.0 / 64.0)
    around = right_exact((filtered - near) ** 2, ones)
    spot = lax.broadcasted_iota(jnp.int32, (ROWS, 128), 1) & 63
    table = jnp.where(spot == 0, near, jnp.where(spot == 1, around, 0.0)).T
    stats[x, c, 0:8] = table[0:8]
    stats[x, c, 8:16] = table[64:72]
    conv_pad[pl.ds(0, ROWS)] = filtered

    mates = [(k, core) for k in (1, 3, 2, 0) for core in range(2)]

    def to_mates(copy_of, send, recv):
        copies = []
        for k, core in mates:
            src, dst = copy_of(core)
            copy = remote(src, dst, send.at[2 * k + core], recv.at[2 * k + c], at(x_=lax.rem(x + k, NX), c_=core))
            copies.append((k, core, copy))
        return copies

    def start_all(copies, keep):
        for k, core, copy in copies:
            if k:
                copy.start()
            else:

                @pl.when(c != core)
                def _():
                    copy.start()

                if keep is not None:

                    @pl.when(c == core)
                    def _():
                        keep(core)

    def wait_all(copies, recv):
        for k, core, copy in copies:
            src, dst = copy.src_ref, copy.dst_ref
            arriving = remote(dst, dst, recv.at[2 * k + core], recv.at[2 * k + core], partner)
            if k:
                arriving.wait_recv()
            else:

                @pl.when(c != core)
                def _():
                    arriving.wait_recv()

    def sent_all(copies):
        for k, core, copy in copies:
            if k:
                copy.wait_send()
            else:

                @pl.when(c != core)
                def _():
                    copy.wait_send()

    stats_copies = to_mates(lambda core: (stats.at[x, c], stats.at[x, c]), stats_send, stats_recv)
    start_all(stats_copies, None)

    for copy in outw_waits[:3]:
        copy.wait_recv()
    outw_waits[3].wait()
    for p, ref in enumerate((outw0, outw1)):

        @pl.when(c == p)
        def _():
            remote(ref, ref, outw_cross_send, outw_cross_recv, partner).start()

    wait_all(stats_copies, stats_recv)
    sides = []
    for half in range(2):
        rows = [stats[q, core, 8 * half : 8 * half + 2] for q in range(NX) for core in range(2)]
        center = sum(r[0:1] for r in rows) * (1.0 / 8.0)
        around_row = sum(r[1:2] + 64.0 * (r[0:1] - center) ** 2 for r in rows)
        sides.append((center, lax.rsqrt(around_row * (1.0 / 512.0) + 1e-05)))
    row = lax.broadcasted_iota(jnp.int32, (8, ROWS), 0)
    column = jnp.where(
        row == 0,
        sides[0][0],
        jnp.where(row == 1, sides[0][1], jnp.where(row == 2, sides[1][0], sides[1][1])),
    ).T
    center = jnp.where(lane, column[:, 0:1], column[:, 2:3])
    scale = jnp.where(lane, column[:, 1:2], column[:, 3:4])
    normal = (conv_pad[pl.ds(0, ROWS)] - center) * scale * own_head(conv_norm_gain[...])

    def by_half(v, ref):
        upper_rows, lower_rows = v[:96], v[96:]
        low = lane[:96]
        ref[0] = jnp.where(low, upper_rows, turned(lower_rows)).astype(BF16)
        ref[1] = jnp.where(low, turned(upper_rows), lower_rows).astype(BF16)

    def natural(ref, q):
        f0, f1 = ref[q, 0].astype(F32), ref[q, 1].astype(F32)
        low = lane[:96]
        rows = [jnp.where(low, f0, turned(f1)), jnp.where(low, turned(f0), f1)]
        return jnp.concatenate(rows, axis=0).astype(BF16)

    by_half(normal * sigmoid(normal), send_conv)
    conv_copies = to_mates(lambda core: (send_conv.at[core], feats_conv.at[x, c]), conv_send, conv_recv)

    def keep_conv(core):
        feats_conv[x, c] = send_conv[core]

    start_all(conv_copies, keep_conv)

    def advance(k, state):
        remote(line_z.at[k], line_z.at[k], z_send.at[0], z_recv.at[k], partner).wait_recv()
        return combine(decoded(line_z[k]), state)

    state = lax.fori_loop(0, z, advance, jnp.zeros((64, 128), F32))
    state0 = jnp.where(lane64 < 64, 0.0, combine(inside, state))
    state1 = combine(half0, state0)
    whole = jnp.concatenate(
        [
            jnp.where(lane64 < 64, turned(state0), 0.0),
            jnp.where(lane64 < 64, 0.0, state1),
        ],
        axis=0,
    )
    reads = three(reads_a[...], whole) + reads_b[...]
    reads = reads - right_exact(reads, ones) * (1.0 / 64.0)
    spread_ = right_exact(reads * reads, ones) * (1.0 / 64.0)
    by_half(
        reads * lax.rsqrt(spread_ + 0.00064) * own_head(scan_norm_gain[...]) * sigmoid(gate_pre), send_scan
    )
    scan_copies = to_mates(lambda core: (send_scan.at[core], feats_scan.at[x, c]), scan_send, scan_recv)

    def keep_scan(core):
        feats_scan[x, c] = send_scan[core]

    start_all(scan_copies, keep_scan)

    outw_cross = remote(outw0, outw0, outw_cross_send, outw_cross_recv, partner)
    outw_cross.wait_recv()
    wait_all(conv_copies, conv_recv)

    def w_scan(q):
        return outw0[q].reshape(512, 128)

    def w_conv(q):
        rows = [outw1[q, j, i].reshape(32, 128) for i in range(2) for j in range(N)]
        return jnp.concatenate(rows, axis=0)

    total_out = one_nt(natural(feats_conv, 0), w_conv(0))
    for q in range(1, NX):
        total_out = total_out + one_nt(natural(feats_conv, q), w_conv(q))
    wait_all(scan_copies, scan_recv)
    for q in range(NX):
        total_out = total_out + one_nt(natural(feats_scan, q), w_scan(q))
    out[...] = total_out.astype(BF16)

    for copies in (tok_copies, outw_waits[:3], [extra_copy, normed_copy, outw_cross]):
        for copy in copies:
            copy.wait_send()
    for copies in (stats_copies, conv_copies, scan_copies):
        sent_all(copies)
    wide.drain()
    thin.drain()
    lines = line_y.at[pl.ds(0, 7)]
    remote(lines, lines, y_send, y_recv.at[0], partner).wait_send()

    @pl.when(jnp.logical_not(last))
    def _():
        rim_copy.wait_send()

    for k, copy in z_copies:

        @pl.when(z + k < N)
        def _():
            copy.wait_send()


def shards(
    tokens,
    norm_gain,
    query_weight,
    key_weight,
    value_weight,
    decay_weight,
    removal_weight,
    gate_weight,
    key_gain,
    removal_gain,
    removal_bias,
    decay_bias,
    decay_extra,
    scan_norm_gain,
    conv_value_weight,
    conv_gate_weight,
    conv_kernel,
    conv_bias,
    conv_norm_gain,
    out_scan_weight,
    out_conv_weight,
):
    row = lambda v: v.reshape(1, -1)
    anywhere = pl.BlockSpec(memory_space=pl.ANY)
    inside = pl.BlockSpec(memory_space=pltpu.VMEM)
    dma = pltpu.SemaphoreType.DMA
    vmem = pltpu.VMEM
    return pl.pallas_call(
        kernel,
        out_shape=jax.ShapeDtypeStruct((ROWS, 512), BF16),
        in_specs=[anywhere] * 2 + [inside] * 14 + [anywhere] + [inside] * 4,
        out_specs=inside,
        scratch_shapes=[
            vmem((2, 16, FIRST), BF16),
            vmem((2, 16, SECOND), BF16),
            vmem((N, N, 2, 16, FIRST), BF16),
            vmem((N, N, 2, 16, SECOND), BF16),
            vmem((2, ROWS, 128), F32),
            vmem((1, MODEL), F32),
            vmem((NX, ROWS, 512), BF16),
            vmem((2, ROWS, MODEL), BF16),
            vmem((2, ROWS, 512), BF16),
            vmem((NX, 2, N, 2, 16, 128), BF16),
            vmem((NX, N, 2, 2, 16, 128), BF16),
            vmem((N, 80, 128), BF16),
            vmem((N, 80, 128), BF16),
            vmem((32, 128), BF16),
            vmem((ROWS, 128), BF16),
            vmem((ROWS + 32, 128), F32),
            vmem((NX, 2, 16, ROWS), F32),
            vmem((2, 96, 128), BF16),
            vmem((2, 96, 128), BF16),
            vmem((NX, 2, 96, 128), BF16),
            vmem((NX, 2, 96, 128), BF16),
            vmem((ROWS, 128), F32),
            vmem((ROWS, 128), F32),
            dma((3,)),
            dma((3,)),
            dma((3,)),
            dma((2,)),
            dma((2,)),
            dma((4,)),
            dma((16,)),
            dma((16,)),
            dma((16,)),
            dma((4,)),
            dma((16,)),
            dma((16,)),
            dma((16,)),
            dma((3,)),
            dma((3,)),
            dma(()),
            dma(()),
            dma(()),
            dma(()),
            dma((N,)),
            dma((N - 1,)),
            dma((N,)),
            dma(()),
            dma(()),
            dma((8,)),
            dma((8,)),
            dma((8,)),
            dma((8,)),
            dma((8,)),
            dma((8,)),
        ],
        compiler_params=pltpu.CompilerParams(
            collective_id=0, has_side_effects=True, vmem_limit_bytes=56 * 1024 * 1024
        ),
    )(
        tokens,
        row(norm_gain),
        query_weight,
        key_weight,
        value_weight,
        decay_weight,
        removal_weight,
        gate_weight,
        conv_value_weight,
        conv_gate_weight,
        out_scan_weight.T,
        out_conv_weight.T,
        row(key_gain),
        row(removal_gain),
        row(removal_bias),
        row(decay_bias),
        decay_extra,
        row(scan_norm_gain),
        conv_kernel,
        row(conv_bias),
        row(conv_norm_gain),
    )


def solution(mesh):
    torus = Mesh(mesh.devices.reshape(N, N, 2, mesh.shape["tp"]), (*SP, "tp"))
    in_specs = (
        P(SP, "tp"),
        P(),
        P(SP, "tp"),
        P(SP, "tp"),
        P(SP, "tp"),
        P(SP, "tp"),
        P(SP, "tp"),
        P(SP, "tp"),
        P("tp"),
        P("tp"),
        P("tp"),
        P("tp"),
        P(SP, "tp"),
        P("tp"),
        P(SP, "tp"),
        P(SP, "tp"),
        P(None, "tp"),
        P("tp"),
        P("tp"),
        P("tp", SP),
        P("tp", SP),
    )
    return jax.shard_map(
        shards, mesh=torus, in_specs=in_specs, out_specs=P(SP, "tp"), check_vma=False
    )
```

```python
import functools
import math

import jax
import jax.numpy as jnp
from jax import lax
from jax.experimental import pallas as pl
from jax.experimental.pallas import tpu as pltpu
from jax.sharding import Mesh
from jax.sharding import PartitionSpec as P

F32 = jnp.float32
BF16 = jnp.bfloat16
SP = ("sp_0", "sp_1", "sp_2")
MESH = pl.DeviceIdType.MESH
CONV_K = 31
ROWS = 192
BLOCK = 64
BLOCKS = ROWS // BLOCK
MODEL = 2048
NX = 4
PROJ = 1024
N = 8


def split2(a):
    high = a.astype(BF16)
    return high, (a - high.astype(F32)).astype(BF16)


def one(a, b):
    return jnp.dot(a.astype(BF16), b.astype(BF16), preferred_element_type=F32)


def one_nt(a, b):
    return lax.dot_general(
        a.astype(BF16), b.astype(BF16), (((1,), (1,)), ((), ())), preferred_element_type=F32
    )


def three(a, b):
    ah, al = split2(a)
    bh, bl = split2(b)
    return one(ah, bh) + one(al, bh) + one(ah, bl)


def three_nt(a, b):
    ah, al = split2(a)
    bh, bl = split2(b)
    return one_nt(ah, bh) + one_nt(al, bh) + one_nt(ah, bl)


def left_exact(a, b):
    bh, bm = split2(b)
    bl = (b - bh.astype(F32) - bm.astype(F32)).astype(BF16)
    return one(a, bh) + one(a, bm) + one(a, bl)


def right_exact(a, b):
    ah, al = split2(a)
    return one(ah, b) + one(al, b)


def iotas(rows, columns):
    return (
        lax.broadcasted_iota(jnp.int32, (rows, columns), 0),
        lax.broadcasted_iota(jnp.int32, (rows, columns), 1),
    )


def sigmoid(x):
    return 1.0 / (1.0 + jnp.exp(-x))


def head_ones():
    i, j = iotas(128, 128)
    return ((i >> 6) == (j >> 6)).astype(BF16)


PAIRS, INVERSE, GATHERED, STEP, READ, CHAIN = one, one, one, one, one, three
PAIRS_NT = one_nt


def spread(a):
    first = lax.broadcasted_iota(jnp.int32, a.shape, 1) < 64
    return jnp.concatenate([jnp.where(first, a, 0.0), jnp.where(first, 0.0, a)], axis=0)


def masks():
    i, j = iotas(128, 128)
    same_head = (i >> 6) == (j >> 6)
    return i, j, same_head


def prepared(keys, values, decay_pre, removal_pre, key_gain, removal_gain, removal_bias, decay_bias, extra):
    ones = head_ones()
    rate = sigmoid(decay_bias + decay_pre) * math.exp(-0.5) + extra
    removal = sigmoid(removal_bias + removal_pre)
    scaled = keys * key_gain
    unit = scaled * lax.rsqrt(right_exact(scaled * scaled, ones) + 1e-06)
    written = keys * (1.0 + (removal - 1.0) * removal_gain)
    beta = unit * removal
    i, j = iotas(BLOCK, BLOCK)
    lower = (i >= j).astype(BF16)
    blocks = []
    for b in range(BLOCKS):
        rows = slice(b * BLOCK, (b + 1) * BLOCK)
        rate_b = rate[rows]
        falling = -left_exact(lower, rate_b)
        before = falling + rate_b
        middle = falling[BLOCK // 2 : BLOCK // 2 + 1]
        ending = falling[BLOCK - 1 :]
        up = jnp.exp(middle - falling)
        to_end = jnp.exp(ending - falling)
        beta_mid = beta[rows] * up
        keys_mid = written[rows] * up
        blocks.append(
            dict(
                falling=falling,
                middle=middle,
                end_decay=jnp.exp(ending),
                left=spread(-unit[rows] * jnp.exp(before - middle)),
                right=jnp.concatenate([beta_mid, beta_mid, keys_mid, keys_mid], axis=0),
                start_alpha=spread(-unit[rows] * jnp.exp(before)),
                end_beta=spread(beta[rows] * to_end).T,
                end_keys=spread(written[rows] * to_end).T,
                values=spread(values[rows]),
            )
        )
    return blocks


def inverted(blocks):
    i, j, same_head = masks()
    strict = same_head & (i > j)
    eye = (i == j).astype(F32)
    sames = [(i >> s) == (j >> s) for s in (3, 4, 5)] + [same_head]
    for block in blocks:
        pairs = PAIRS_NT(block["left"], block["right"])
        block["links"] = jnp.where(strict, pairs[:, :128], 0.0)
        alpha_keys = jnp.where(strict, pairs[:, 128:], 0.0)
        block["local"] = PAIRS(alpha_keys, block["values"])
        block["power"] = base = jnp.where(sames[0], block["links"], 0.0)
        block["inverse"] = eye + base
    for _ in range(2):
        for block in blocks:
            block["power"] = INVERSE(block["power"], block["power"])
        for block in blocks:
            block["inverse"] = block["inverse"] + INVERSE(block["inverse"], block["power"])
    for s in range(3):
        for block in blocks:
            off = jnp.where(sames[s + 1] & ~sames[s], block["links"], 0.0)
            block["part"] = INVERSE(off, block["inverse"])
        for block in blocks:
            block["inverse"] = block["inverse"] + INVERSE(block["inverse"], block["part"])


def transition(blocks):
    i, j, same_head = masks()
    for block in blocks:
        block["gathered"] = GATHERED(
            block["inverse"], jnp.concatenate([block["start_alpha"], block["local"]], axis=1)
        )
    for block in blocks:
        step = STEP(block["end_beta"], block["gathered"])
        block["step_a"] = step[:, :128] + jnp.where(i == j, block["end_decay"], 0.0)
        block["step_b"] = step[:, 128:] + STEP(block["end_keys"], block["values"])
    both = jnp.concatenate([blocks[0]["step_a"], blocks[0]["step_b"]], axis=1)
    for block in blocks[1:]:
        block["start"] = both
        moved = CHAIN(block["step_a"], both)
        both = jnp.concatenate([moved[:, :128], moved[:, 128:] + block["step_b"]], axis=1)
    return both[:, :128], both[:, 128:]


def read_parts(blocks, recept):
    i, j, same_head = masks()
    inclusive = same_head & (i >= j)
    reads_a, reads_b = [], []
    for b, block in enumerate(blocks):
        rows = slice(b * BLOCK, (b + 1) * BLOCK)
        left = spread(recept[rows] * jnp.exp(block["falling"] - block["middle"]))
        pairs = PAIRS_NT(left, block["right"])
        recept_beta = jnp.where(inclusive, pairs[:, :128], 0.0)
        recept_keys = jnp.where(inclusive, pairs[:, 128:], 0.0)
        reads = READ(recept_beta, block["gathered"])
        read_a = reads[:64, :128] + reads[64:, :128] + recept[rows] * jnp.exp(block["falling"])
        read_b = reads[:, 128:] + READ(recept_keys, block["values"])
        read_b = read_b[:64] + read_b[64:]
        if b:
            seen = READ(read_a, block["start"])
            read_a, read_b = seen[:, :128], seen[:, 128:] + read_b
        reads_a.append(read_a)
        reads_b.append(read_b)
    return jnp.concatenate(reads_a, axis=0), jnp.concatenate(reads_b, axis=0)


def local_scan(recept, keys, values, decay_pre, removal_pre, *rest):
    blocks = prepared(keys, values, decay_pre, removal_pre, *rest)
    inverted(blocks)
    trans = transition(blocks)
    return (*trans, *read_parts(blocks, recept))


def packed_heads(trans_a, trans_b):
    lane = lax.broadcasted_iota(jnp.int32, (64, 128), 1)
    head0 = jnp.where(lane < 64, trans_a[:64], pltpu.roll(trans_b[:64], 64, 1))
    head1 = jnp.where(lane < 64, pltpu.roll(trans_a[64:], 64, 1), trans_b[64:])
    return head0, head1


def coded(both):
    i, j = iotas(64, 128)
    on = i == j
    diagonal = jnp.sum(jnp.where(on, both, 0.0), axis=0, keepdims=True)
    high, rest = split2(diagonal)
    low = (diagonal - high.astype(F32) - rest.astype(F32)).astype(BF16)
    row = lax.broadcasted_iota(jnp.int32, (16, 128), 0)
    below = jnp.where(
        row == 0,
        high.astype(F32),
        jnp.where(row == 1, rest.astype(F32), jnp.where(row == 2, low.astype(F32), 0.0)),
    )
    return jnp.concatenate([jnp.where(on, 0.0, both), below], axis=0).astype(BF16)


def decoded(code):
    code = code.astype(F32)
    i, j = iotas(64, 128)
    diagonal = code[64:65] + code[65:66] + code[66:67]
    return jnp.where(i == j, diagonal, code[:64])


def combine(later, total):
    lane = lax.broadcasted_iota(jnp.int32, later.shape, 1)
    return three(later[:, :64], total) + jnp.where(lane < 64, 0.0, later)


FIRST = 256
SECOND = 256
THIRD = 128


def joined(ref, base, c, first):
    columns = pl.ds(base, first)
    rows = []
    for i in range(N):
        for j in range(N):
            b_ = (1 - c) * i + c * j
            a_ = (1 - c) * j + c * i
            rows.append(ref[b_, a_, :, :, columns].reshape(32, first))
    return jnp.concatenate(rows, axis=0)


def kernel(
    tokens,
    norm_gain,
    w0,
    w1,
    w2,
    w3,
    w4,
    w5,
    w6,
    w7,
    out_scan,
    out_conv,
    key_gain,
    removal_gain,
    removal_bias,
    decay_bias,
    extra,
    scan_norm_gain,
    conv_kernel,
    conv_bias,
    conv_norm_gain,
    out,
    mine1,
    mine2,
    mine3,
    weights,
    later,
    last_w,
    extras,
    norm_gain_v,
    tok,
    normed,
    proj,
    outw0,
    outw1,
    line_y,
    line_z,
    rim,
    conv_in,
    conv_pad,
    stats,
    send_scan,
    send_conv,
    feats_scan,
    feats_conv,
    reads_a,
    reads_b,
    load_sem,
    tok_send,
    tok_recv,
    share_send,
    share_recv,
    wide_sems,
    wide_first,
    wide_plus,
    wide_minus,
    thin_sems,
    thin_first,
    thin_plus,
    thin_minus,
    third_sems,
    third_first,
    third_plus,
    third_minus,
    outw_send,
    outw_recv,
    outw_load,
    outw_cross_send,
    outw_cross_recv,
    y_send,
    y_recv,
    z_send,
    z_recv,
    rim_send,
    rim_recv,
    stats_send,
    stats_recv,
    scan_send,
    scan_recv,
    conv_send,
    conv_recv,
):
    z, y, c, x = (lax.axis_index(n) for n in (*SP, "tp"))
    upper = c == 1

    def at(z_=None, y_=None, c_=None, x_=None):
        pick = lambda a, b: a if b is None else b
        return (pick(z, z_), pick(y, y_), pick(c, c_), pick(x, x_))

    def remote(src, dst, send, recv, where):
        return pltpu.make_async_remote_copy(
            src_ref=src, dst_ref=dst, send_sem=send, recv_sem=recv, device_id=where, device_id_type=MESH
        )

    partner = at(c_=1 - c)
    a = (1 - c) * y + c * z
    b = (1 - c) * z + c * y

    loads = [
        pltpu.make_async_copy(tokens, tok.at[x], load_sem.at[0]),
        pltpu.make_async_copy(extra, extras.at[c], load_sem.at[1]),
        pltpu.make_async_copy(norm_gain, norm_gain_v, load_sem.at[2]),
    ]
    for load in loads:
        load.start()

    barrier = pltpu.get_barrier_semaphore()
    greeted = [partner]
    for k in range(1, N):
        for core in range(2):
            greeted.append(at(y_=lax.rem(y + k, N), c_=core))
            greeted.append(at(z_=lax.rem(z + k, N), c_=core))
    for k in range(1, NX):
        for core in range(2):
            greeted.append(at(x_=lax.rem(x + k, NX), c_=core))
    chip = z * N + y
    before = lax.rem(chip + N * N - 1, N * N)
    after = lax.rem(chip + 1, N * N)
    greeted.append((before // N, lax.rem(before, N), c, x))
    for device in greeted:
        pl.semaphore_signal(barrier, inc=1, device_id=device, device_id_type=MESH)

    lane16 = lax.broadcasted_iota(jnp.int32, (16, 128), 1) < 64

    def halves(left, right):
        left, right = left.astype(F32), right.astype(F32)
        first = jnp.where(lane16, left, pltpu.roll(right, 64, 1))
        return first.astype(BF16), jnp.where(lane16, pltpu.roll(left, 64, 1), right).astype(BF16)

    for k, (left, right) in enumerate(((w1, w2), (w3, w4))):
        for core, part_ in enumerate(halves(left[...], right[...])):
            mine1[core, :, 128 * k : 128 * (k + 1)] = part_
    for core, part_ in enumerate(halves(w6[...], w7[...])):
        mine2[core, :, 0:128] = part_
    for core, part_ in enumerate(halves(w0[...], w5[...])):
        mine3[core] = part_
    mine2[0, :, 128:256] = out_scan[...]
    mine2[1, :, 128:256] = out_conv[...]

    pl.semaphore_wait(barrier, len(greeted))

    class Gather:
        def __init__(self, own, ref, sems, first_recv, plus_recv, minus_recv):
            self.own, self.ref, self.first_recv = own, ref, first_recv
            self.first_send, self.second_send, self.keep, self.pair_send = (sems.at[k] for k in range(4))
            self.recvs = {1: plus_recv, -1: minus_recv}

        def start(self):
            for k in (0, 1, 7, 2, 6, 3, 5, 4):
                for core in range(2):
                    a_, b_ = (y, z) if core == 0 else (z, y)
                    target = (z, lax.rem(y + k, N), 0, x) if core == 0 else (lax.rem(z + k, N), y, 1, x)
                    src, dst = self.own.at[core], self.ref.at[b_, a_, c]
                    recv = self.first_recv.at[2 * a_ + c]
                    copy = remote(src, dst, self.first_send if k else self.pair_send, recv, target)
                    if k:
                        copy.start()
                    else:

                        @pl.when(c != core)
                        def _():
                            copy.start()

                        @pl.when(c == core)
                        def _():
                            pltpu.make_async_copy(src, dst, self.keep).start()

        def low(self, h):
            return lax.rem(a // 2 + h, 4) * 2

        def piece(self, h, distance):
            return self.ref.at[lax.rem(b + distance + N, N), pl.ds(self.low(h), 2)]

        def copy(self, h, source, sign, reach):
            piece = self.piece(h, -sign * source)
            recv = self.recvs[sign].at[h * 4 + source + reach - 1]
            k = reach if sign > 0 else N - reach
            target = at(z_=lax.rem(z + (1 - c) * k, N), y_=lax.rem(y + c * k, N))
            return remote(piece, piece, self.second_send, recv, target)

        def collect(self, h):
            for k in range(2):
                a_ = self.low(h) + k
                for core in range(2):
                    piece = self.ref.at[b, a_, core]

                    def wait():
                        recv = self.first_recv.at[2 * a_ + core]
                        remote(piece, piece, self.first_send, recv, partner).wait_recv()

                    if h:
                        wait()
                    else:
                        own = jnp.logical_and(a_ == a, c == core)
                        pl.when(jnp.logical_not(own))(wait)
            if h == 0:
                own = self.ref.at[b, a, c]
                pltpu.make_async_copy(own, own, self.keep).wait()
            for reach in (2, 1):
                for sign in (1, -1):
                    self.copy(h, 0, sign, reach).start()

        def has_far(self, h, sign):
            return (h % 2 == 0) == (sign > 0)

        def arrive(self, h, d, sign):
            self.copy(h, 0, sign, d).wait_recv()

        def relay(self, h):
            for sign in (1, -1):
                self.arrive(h, 2, sign)
                if self.has_far(h, sign):
                    self.copy(h, 2, sign, 2).start()
                self.copy(h, 2, sign, 1).start()

        def near(self, h):
            for sign in (1, -1):
                self.arrive(h, 1, sign)

        def far(self, h):
            for sign in (1, -1):
                if self.has_far(h, sign):
                    self.arrive(h, 4, sign)
                self.arrive(h, 3, sign)

        def drain(self):
            fourteen = self.ref.at[0, pl.ds(0, 7)]
            remote(fourteen, fourteen, self.first_send, self.first_recv.at[0], partner).wait_send()
            single = self.ref.at[0, 7, 0]
            remote(single, single, self.pair_send, self.first_recv.at[0], partner).wait_send()
            most = self.ref.at[pl.ds(0, 7)]
            remote(most, most, self.second_send, self.first_recv.at[0], partner).wait_send()

    wide = Gather(mine1, weights, wide_sems, wide_first, wide_plus, wide_minus)
    thin = Gather(mine2, later, thin_sems, thin_first, thin_plus, thin_minus)
    third = Gather(mine3, last_w, third_sems, third_first, third_plus, third_minus)
    wide.start()
    for load in loads:
        load.wait()
    tok_copies = [
        remote(tok.at[x], tok.at[x], tok_send.at[k - 1], tok_recv.at[k - 1], at(x_=lax.rem(x + k, NX)))
        for k in (1, 3, 2)
    ]
    for copy in tok_copies:
        copy.start()
    extra_copy = remote(extras.at[c], extras.at[c], share_send.at[0], share_recv.at[0], partner)
    extra_copy.start()
    normed_copy = remote(normed.at[c], normed.at[c], share_send.at[1], share_recv.at[1], partner)

    order = (0, 1, 3, 2)
    for h in order:
        wide.collect(h)
    thin.start()
    for h in order:
        wide.relay(h)
    third.start()
    for copy in tok_copies:
        copy.wait_recv()
    square = jnp.zeros((ROWS, 1), F32)
    for q in range(NX):
        t = tok[q].astype(F32)
        square = square + jnp.sum(t * t, axis=-1, keepdims=True)
    factor = lax.rsqrt(square * (1.0 / MODEL) + 1e-06)
    for q in range(NX):
        t = tok[q].astype(F32)
        columns = slice(q * 512, (q + 1) * 512)
        normed[c, :, columns] = (t * factor * norm_gain_v[:, columns]).astype(BF16)
    normed_copy.start()
    for h in order:
        thin.collect(h)
    for h in order:
        wide.near(h)
    extra_copy.wait_recv()
    normed_copy.wait_recv()
    for h in order:
        wide.far(h)

    lane = lax.broadcasted_iota(jnp.int32, (ROWS, 128), 1) < 64

    def turned(v):
        return pltpu.roll(v, 64, 1)

    def own_head(v):
        low = lax.broadcasted_iota(jnp.int32, v.shape, 1) < 64
        other = turned(v)
        return jnp.where(upper, jnp.where(low, other, v), jnp.where(low, v, other))

    def project(ref, base, width, target):
        w = joined(ref, base, c, width)
        for half in range(2):
            proj[half, :, target : target + width] = jnp.dot(
                normed[half], w, preferred_element_type=F32
            ).astype(BF16)

    def parts(k):
        columns = slice(128 * k, 128 * (k + 1))
        p0, p1 = proj[0, :, columns].astype(F32), proj[1, :, columns].astype(F32)
        return jnp.where(lane, p0, turned(p1)), jnp.where(lane, turned(p0), p1)

    project(weights, 0, FIRST, 0)
    keys, values = parts(0)
    decay_pre, removal_pre = parts(1)
    e0, e1 = extras[0], extras[1]
    own_extra = jnp.where(
        upper, jnp.where(lane, turned(e0), e1), jnp.where(lane, e0, turned(e1))
    )
    blocks = prepared(
        keys,
        values,
        decay_pre,
        removal_pre,
        own_head(key_gain[...]),
        own_head(removal_gain[...]),
        own_head(removal_bias[...]),
        own_head(decay_bias[...]),
        own_extra,
    )
    inverted(blocks)
    half0, half1 = packed_heads(*transition(blocks))
    line_y[y] = coded(combine(half1, half0))
    for k in (4, 3, 5, 2, 6, 1, 7):
        remote(line_y.at[y], line_y.at[y], y_send, y_recv.at[y], at(y_=lax.rem(y + k, N))).start()
    for h in order:
        thin.relay(h)
    for h in order:
        third.collect(h)
    for h in order:
        thin.near(h)
        thin.far(h)

    def outw_copies(p):
        for k in (1, 3, 2, 0):
            x_ = lax.rem(x + k, NX)
            if p:
                src, dst = later.at[:, pl.ds(2 * x_, 2), :, :, pl.ds(128, 128)], outw1.at[x]
            else:
                src, dst = later.at[pl.ds(2 * x_, 2), :, :, :, pl.ds(128, 128)], outw0.at[x]
            if k:
                yield remote(src, dst, outw_send.at[k - 1], outw_recv.at[k - 1], at(x_=x_))
            else:
                yield pltpu.make_async_copy(src, dst, outw_load)

    for p in range(2):

        @pl.when(c == p)
        def _():
            for copy in outw_copies(p):
                copy.start()

    outw_waits = list(outw_copies(0))

    project(later, 0, 128, 384)
    conv_value, conv_gate = parts(3)
    conv_in[...] = (conv_value * sigmoid(conv_gate)).astype(BF16)
    last = chip == N * N - 1
    start = chip == 0
    rim_copy = remote(
        conv_in.at[pl.ds(ROWS - 32, 32)], rim, rim_send, rim_recv, (after // N, lax.rem(after, N), c, x)
    )

    @pl.when(jnp.logical_not(last))
    def _():
        rim_copy.start()

    lane64 = lax.broadcasted_iota(jnp.int32, (64, 128), 1)
    i, j = iotas(64, 128)
    nothing = (i == j).astype(F32)
    for k in range(N):

        @pl.when(y != k)
        def _():
            remote(line_y.at[k], line_y.at[k], y_send, y_recv.at[k], partner).wait_recv()

    each = [decoded(line_y[k]) for k in range(N)]
    pairs = [combine(each[2 * k + 1], each[2 * k]) for k in range(4)]
    quads = [combine(pairs[1], pairs[0]), combine(pairs[3], pairs[2])]
    line_z[z] = coded(combine(quads[1], quads[0]))
    z_copies = []
    for k in range(N - 1, 0, -1):
        copy = remote(
            line_z.at[z], line_z.at[z], z_send.at[k - 1], z_recv.at[z], at(z_=lax.rem(z + k, N))
        )
        z_copies.append((k, copy))

        @pl.when(z + k < N)
        def _():
            copy.start()

    for h in order:
        third.relay(h)
    inside = jnp.where(y >= 4, quads[0], nothing)
    inside = jnp.where(lax.rem(y, 4) >= 2, combine(jnp.where(y >= 4, pairs[2], pairs[0]), inside), inside)
    previous = decoded(line_y[jnp.maximum(y - 1, 0)])
    inside = jnp.where(lax.rem(y, 2) == 1, combine(previous, inside), inside)

    @pl.when(start)
    def _():
        rim[...] = jnp.zeros_like(rim)

    @pl.when(jnp.logical_not(start))
    def _():
        rim_copy.wait_recv()

    ending = conv_in[pl.ds(ROWS - 32, 32)].astype(F32)
    conv_pad[pl.ds(0, 32)] = turned(jnp.where(lane[:32], ending, rim[...].astype(F32)))
    conv_pad[pl.ds(32, ROWS)] = conv_in[...].astype(F32)
    taps = own_head(conv_kernel[...])
    filtered = own_head(conv_bias[...]) + taps[0:1] * conv_pad[pl.ds(2, ROWS)]
    for k in range(1, CONV_K):
        filtered = filtered + taps[k : k + 1] * conv_pad[pl.ds(2 + k, ROWS)]
    ones = head_ones()
    near = right_exact(filtered, ones) * (1.0 / 64.0)
    around = right_exact((filtered - near) ** 2, ones)
    spot = lax.broadcasted_iota(jnp.int32, (ROWS, 128), 1) & 63
    table = jnp.where(spot == 0, near, jnp.where(spot == 1, around, 0.0)).T
    stats[x, c, 0:8] = table[0:8]
    stats[x, c, 8:16] = table[64:72]
    conv_pad[pl.ds(0, ROWS)] = filtered

    mates = [(k, core) for k in (1, 3, 2, 0) for core in range(2)]

    def to_mates(copy_of, send, recv):
        copies = []
        for k, core in mates:
            src, dst = copy_of(core)
            copy = remote(src, dst, send.at[2 * k + core], recv.at[2 * k + c], at(x_=lax.rem(x + k, NX), c_=core))
            copies.append((k, core, copy))
        return copies

    def start_all(copies, keep):
        for k, core, copy in copies:
            if k:
                copy.start()
            else:

                @pl.when(c != core)
                def _():
                    copy.start()

                if keep is not None:

                    @pl.when(c == core)
                    def _():
                        keep(core)

    def wait_all(copies, recv):
        for k, core, copy in copies:
            src, dst = copy.src_ref, copy.dst_ref
            arriving = remote(dst, dst, recv.at[2 * k + core], recv.at[2 * k + core], partner)
            if k:
                arriving.wait_recv()
            else:

                @pl.when(c != core)
                def _():
                    arriving.wait_recv()

    def sent_all(copies):
        for k, core, copy in copies:
            if k:
                copy.wait_send()
            else:

                @pl.when(c != core)
                def _():
                    copy.wait_send()

    stats_copies = to_mates(lambda core: (stats.at[x, c], stats.at[x, c]), stats_send, stats_recv)
    start_all(stats_copies, None)

    for h in order:
        third.near(h)
        third.far(h)
    project(last_w, 0, 128, 256)
    recept, gate_pre = parts(2)
    reads_a[...], reads_b[...] = read_parts(blocks, recept)

    for copy in outw_waits[:3]:
        copy.wait_recv()
    outw_waits[3].wait()
    for p, ref in enumerate((outw0, outw1)):

        @pl.when(c == p)
        def _():
            remote(ref, ref, outw_cross_send, outw_cross_recv, partner).start()

    wait_all(stats_copies, stats_recv)
    sides = []
    for half in range(2):
        rows = [stats[q, core, 8 * half : 8 * half + 2] for q in range(NX) for core in range(2)]
        center = sum(r[0:1] for r in rows) * (1.0 / 8.0)
        around_row = sum(r[1:2] + 64.0 * (r[0:1] - center) ** 2 for r in rows)
        sides.append((center, lax.rsqrt(around_row * (1.0 / 512.0) + 1e-05)))
    row = lax.broadcasted_iota(jnp.int32, (8, ROWS), 0)
    column = jnp.where(
        row == 0,
        sides[0][0],
        jnp.where(row == 1, sides[0][1], jnp.where(row == 2, sides[1][0], sides[1][1])),
    ).T
    center = jnp.where(lane, column[:, 0:1], column[:, 2:3])
    scale = jnp.where(lane, column[:, 1:2], column[:, 3:4])
    normal = (conv_pad[pl.ds(0, ROWS)] - center) * scale * own_head(conv_norm_gain[...])

    def by_half(v, ref):
        upper_rows, lower_rows = v[:96], v[96:]
        low = lane[:96]
        ref[0] = jnp.where(low, upper_rows, turned(lower_rows)).astype(BF16)
        ref[1] = jnp.where(low, turned(upper_rows), lower_rows).astype(BF16)

    def natural(ref, q):
        f0, f1 = ref[q, 0].astype(F32), ref[q, 1].astype(F32)
        low = lane[:96]
        rows = [jnp.where(low, f0, turned(f1)), jnp.where(low, turned(f0), f1)]
        return jnp.concatenate(rows, axis=0).astype(BF16)

    by_half(normal * sigmoid(normal), send_conv)
    conv_copies = to_mates(lambda core: (send_conv.at[core], feats_conv.at[x, c]), conv_send, conv_recv)

    def keep_conv(core):
        feats_conv[x, c] = send_conv[core]

    start_all(conv_copies, keep_conv)

    for k in range(N - 1):

        @pl.when(k < z)
        def _():
            remote(line_z.at[k], line_z.at[k], z_send.at[0], z_recv.at[k], partner).wait_recv()

    each = [jnp.where(k < z, decoded(line_z[k]), nothing) for k in range(N - 1)]
    pairs = [combine(each[2 * k + 1], each[2 * k]) for k in range(3)]
    state = combine(combine(each[6], pairs[2]), combine(pairs[1], pairs[0]))
    state = jnp.where(lane64 < 64, 0.0, state)
    state0 = jnp.where(lane64 < 64, 0.0, combine(inside, state))
    state1 = combine(half0, state0)
    whole = jnp.concatenate(
        [
            jnp.where(lane64 < 64, turned(state0), 0.0),
            jnp.where(lane64 < 64, 0.0, state1),
        ],
        axis=0,
    )
    reads = three(reads_a[...], whole) + reads_b[...]
    reads = reads - right_exact(reads, ones) * (1.0 / 64.0)
    spread_ = right_exact(reads * reads, ones) * (1.0 / 64.0)
    by_half(
        reads * lax.rsqrt(spread_ + 0.00064) * own_head(scan_norm_gain[...]) * sigmoid(gate_pre), send_scan
    )
    scan_copies = to_mates(lambda core: (send_scan.at[core], feats_scan.at[x, c]), scan_send, scan_recv)

    def keep_scan(core):
        feats_scan[x, c] = send_scan[core]

    start_all(scan_copies, keep_scan)

    outw_cross = remote(outw0, outw0, outw_cross_send, outw_cross_recv, partner)
    outw_cross.wait_recv()
    wait_all(conv_copies, conv_recv)

    def w_scan(q):
        return outw0[q].reshape(512, 128)

    def w_conv(q):
        rows = [outw1[q, j, i].reshape(32, 128) for i in range(2) for j in range(N)]
        return jnp.concatenate(rows, axis=0)

    total_out = one_nt(natural(feats_conv, 0), w_conv(0))
    for q in range(1, NX):
        total_out = total_out + one_nt(natural(feats_conv, q), w_conv(q))
    wait_all(scan_copies, scan_recv)
    for q in range(NX):
        total_out = total_out + one_nt(natural(feats_scan, q), w_scan(q))
    out[...] = total_out.astype(BF16)

    for copies in (tok_copies, outw_waits[:3], [extra_copy, normed_copy, outw_cross]):
        for copy in copies:
            copy.wait_send()
    for copies in (stats_copies, conv_copies, scan_copies):
        sent_all(copies)
    wide.drain()
    thin.drain()
    third.drain()
    lines = line_y.at[pl.ds(0, 7)]
    remote(lines, lines, y_send, y_recv.at[0], partner).wait_send()

    @pl.when(jnp.logical_not(last))
    def _():
        rim_copy.wait_send()

    for k, copy in z_copies:

        @pl.when(z + k < N)
        def _():
            copy.wait_send()


def shards(
    tokens,
    norm_gain,
    query_weight,
    key_weight,
    value_weight,
    decay_weight,
    removal_weight,
    gate_weight,
    key_gain,
    removal_gain,
    removal_bias,
    decay_bias,
    decay_extra,
    scan_norm_gain,
    conv_value_weight,
    conv_gate_weight,
    conv_kernel,
    conv_bias,
    conv_norm_gain,
    out_scan_weight,
    out_conv_weight,
):
    row = lambda v: v.reshape(1, -1)
    anywhere = pl.BlockSpec(memory_space=pl.ANY)
    inside = pl.BlockSpec(memory_space=pltpu.VMEM)
    dma = pltpu.SemaphoreType.DMA
    vmem = pltpu.VMEM
    return pl.pallas_call(
        kernel,
        out_shape=jax.ShapeDtypeStruct((ROWS, 512), BF16),
        in_specs=[anywhere] * 2 + [inside] * 14 + [anywhere] + [inside] * 4,
        out_specs=inside,
        scratch_shapes=[
            vmem((2, 16, FIRST), BF16),
            vmem((2, 16, SECOND), BF16),
            vmem((2, 16, THIRD), BF16),
            vmem((N, N, 2, 16, FIRST), BF16),
            vmem((N, N, 2, 16, SECOND), BF16),
            vmem((N, N, 2, 16, THIRD), BF16),
            vmem((2, ROWS, 128), F32),
            vmem((1, MODEL), F32),
            vmem((NX, ROWS, 512), BF16),
            vmem((2, ROWS, MODEL), BF16),
            vmem((2, ROWS, 512), BF16),
            vmem((NX, 2, N, 2, 16, 128), BF16),
            vmem((NX, N, 2, 2, 16, 128), BF16),
            vmem((N, 80, 128), BF16),
            vmem((N, 80, 128), BF16),
            vmem((32, 128), BF16),
            vmem((ROWS, 128), BF16),
            vmem((ROWS + 32, 128), F32),
            vmem((NX, 2, 16, ROWS), F32),
            vmem((2, 96, 128), BF16),
            vmem((2, 96, 128), BF16),
            vmem((NX, 2, 96, 128), BF16),
            vmem((NX, 2, 96, 128), BF16),
            vmem((ROWS, 128), F32),
            vmem((ROWS, 128), F32),
            dma((3,)),
            dma((3,)),
            dma((3,)),
            dma((2,)),
            dma((2,)),
            dma((4,)),
            dma((16,)),
            dma((16,)),
            dma((16,)),
            dma((4,)),
            dma((16,)),
            dma((16,)),
            dma((16,)),
            dma((4,)),
            dma((16,)),
            dma((16,)),
            dma((16,)),
            dma((3,)),
            dma((3,)),
            dma(()),
            dma(()),
            dma(()),
            dma(()),
            dma((N,)),
            dma((N - 1,)),
            dma((N,)),
            dma(()),
            dma(()),
            dma((8,)),
            dma((8,)),
            dma((8,)),
            dma((8,)),
            dma((8,)),
            dma((8,)),
        ],
        compiler_params=pltpu.CompilerParams(
            collective_id=0, has_side_effects=True, vmem_limit_bytes=56 * 1024 * 1024
        ),
    )(
        tokens,
        row(norm_gain),
        query_weight,
        key_weight,
        value_weight,
        decay_weight,
        removal_weight,
        gate_weight,
        conv_value_weight,
        conv_gate_weight,
        out_scan_weight.T,
        out_conv_weight.T,
        row(key_gain),
        row(removal_gain),
        row(removal_bias),
        row(decay_bias),
        decay_extra,
        row(scan_norm_gain),
        conv_kernel,
        row(conv_bias),
        row(conv_norm_gain),
    )


def solution(mesh):
    torus = Mesh(mesh.devices.reshape(N, N, 2, mesh.shape["tp"]), (*SP, "tp"))
    in_specs = (
        P(SP, "tp"),
        P(),
        P(SP, "tp"),
        P(SP, "tp"),
        P(SP, "tp"),
        P(SP, "tp"),
        P(SP, "tp"),
        P(SP, "tp"),
        P("tp"),
        P("tp"),
        P("tp"),
        P("tp"),
        P(SP, "tp"),
        P("tp"),
        P(SP, "tp"),
        P(SP, "tp"),
        P(None, "tp"),
        P("tp"),
        P("tp"),
        P("tp", SP),
        P("tp", SP),
    )
    return jax.shard_map(
        shards, mesh=torus, in_specs=in_specs, out_specs=P(SP, "tp"), check_vma=False
    )
```

```python
import functools
import math

import jax
import jax.numpy as jnp
from jax import lax
from jax.experimental import pallas as pl
from jax.experimental.pallas import tpu as pltpu
from jax.sharding import Mesh
from jax.sharding import PartitionSpec as P

F32 = jnp.float32
BF16 = jnp.bfloat16
SP = ("sp_0", "sp_1", "sp_2")
MESH = pl.DeviceIdType.MESH
CONV_K = 31
ROWS = 192
BLOCK = 64
BLOCKS = ROWS // BLOCK
MODEL = 2048
NX = 4
PROJ = 1024
N = 8


def split2(a):
    high = a.astype(BF16)
    return high, (a - high.astype(F32)).astype(BF16)


def one(a, b):
    return jnp.dot(a.astype(BF16), b.astype(BF16), preferred_element_type=F32)


def one_nt(a, b):
    return lax.dot_general(
        a.astype(BF16), b.astype(BF16), (((1,), (1,)), ((), ())), preferred_element_type=F32
    )


def three(a, b):
    ah, al = split2(a)
    bh, bl = split2(b)
    return one(ah, bh) + one(al, bh) + one(ah, bl)


def three_nt(a, b):
    ah, al = split2(a)
    bh, bl = split2(b)
    return one_nt(ah, bh) + one_nt(al, bh) + one_nt(ah, bl)


def left_exact(a, b):
    bh, bm = split2(b)
    bl = (b - bh.astype(F32) - bm.astype(F32)).astype(BF16)
    return one(a, bh) + one(a, bm) + one(a, bl)


def right_exact(a, b):
    ah, al = split2(a)
    return one(ah, b) + one(al, b)


def iotas(rows, columns):
    return (
        lax.broadcasted_iota(jnp.int32, (rows, columns), 0),
        lax.broadcasted_iota(jnp.int32, (rows, columns), 1),
    )


def sigmoid(x):
    return 1.0 / (1.0 + jnp.exp(-x))


def head_ones():
    i, j = iotas(128, 128)
    return ((i >> 6) == (j >> 6)).astype(BF16)


PAIRS, INVERSE, GATHERED, STEP, READ, CHAIN = one, one, one, one, one, three
PAIRS_NT = one_nt


def spread(a):
    first = lax.broadcasted_iota(jnp.int32, a.shape, 1) < 64
    return jnp.concatenate([jnp.where(first, a, 0.0), jnp.where(first, 0.0, a)], axis=0)


def masks():
    i, j = iotas(128, 128)
    same_head = (i >> 6) == (j >> 6)
    return i, j, same_head


def prepared(keys, values, decay_pre, removal_pre, key_gain, removal_gain, removal_bias, decay_bias, extra):
    ones = head_ones()
    rate = sigmoid(decay_bias + decay_pre) * math.exp(-0.5) + extra
    removal = sigmoid(removal_bias + removal_pre)
    scaled = keys * key_gain
    unit = scaled * lax.rsqrt(right_exact(scaled * scaled, ones) + 1e-06)
    written = keys * (1.0 + (removal - 1.0) * removal_gain)
    beta = unit * removal
    i, j = iotas(BLOCK, BLOCK)
    lower = (i >= j).astype(BF16)
    blocks = []
    for b in range(BLOCKS):
        rows = slice(b * BLOCK, (b + 1) * BLOCK)
        rate_b = rate[rows]
        falling = -left_exact(lower, rate_b)
        before = falling + rate_b
        middle = falling[BLOCK // 2 : BLOCK // 2 + 1]
        ending = falling[BLOCK - 1 :]
        up = jnp.exp(middle - falling)
        to_end = jnp.exp(ending - falling)
        beta_mid = beta[rows] * up
        keys_mid = written[rows] * up
        blocks.append(
            dict(
                falling=falling,
                middle=middle,
                end_decay=jnp.exp(ending),
                left=spread(-unit[rows] * jnp.exp(before - middle)),
                right=jnp.concatenate([beta_mid, beta_mid, keys_mid, keys_mid], axis=0),
                start_alpha=spread(-unit[rows] * jnp.exp(before)),
                end_beta=spread(beta[rows] * to_end).T,
                end_keys=spread(written[rows] * to_end).T,
                values=spread(values[rows]),
            )
        )
    return blocks


def inverted(blocks):
    i, j, same_head = masks()
    strict = same_head & (i > j)
    eye = (i == j).astype(F32)
    sames = [(i >> s) == (j >> s) for s in (3, 4, 5)] + [same_head]
    for block in blocks:
        pairs = PAIRS_NT(block["left"], block["right"])
        block["links"] = jnp.where(strict, pairs[:, :128], 0.0)
        alpha_keys = jnp.where(strict, pairs[:, 128:], 0.0)
        block["local"] = PAIRS(alpha_keys, block["values"])
        block["power"] = base = jnp.where(sames[0], block["links"], 0.0)
        block["inverse"] = eye + base
    for _ in range(2):
        for block in blocks:
            block["power"] = INVERSE(block["power"], block["power"])
        for block in blocks:
            block["inverse"] = block["inverse"] + INVERSE(block["inverse"], block["power"])
    for s in range(3):
        for block in blocks:
            off = jnp.where(sames[s + 1] & ~sames[s], block["links"], 0.0)
            block["part"] = INVERSE(off, block["inverse"])
        for block in blocks:
            block["inverse"] = block["inverse"] + INVERSE(block["inverse"], block["part"])


def transition(blocks):
    i, j, same_head = masks()
    for block in blocks:
        block["gathered"] = GATHERED(
            block["inverse"], jnp.concatenate([block["start_alpha"], block["local"]], axis=1)
        )
    for block in blocks:
        step = STEP(block["end_beta"], block["gathered"])
        block["step_a"] = step[:, :128] + jnp.where(i == j, block["end_decay"], 0.0)
        block["step_b"] = step[:, 128:] + STEP(block["end_keys"], block["values"])
    both = jnp.concatenate([blocks[0]["step_a"], blocks[0]["step_b"]], axis=1)
    for block in blocks[1:]:
        block["start"] = both
        moved = CHAIN(block["step_a"], both)
        both = jnp.concatenate([moved[:, :128], moved[:, 128:] + block["step_b"]], axis=1)
    return both[:, :128], both[:, 128:]


def read_parts(blocks, recept):
    i, j, same_head = masks()
    inclusive = same_head & (i >= j)
    reads_a, reads_b = [], []
    for b, block in enumerate(blocks):
        rows = slice(b * BLOCK, (b + 1) * BLOCK)
        left = spread(recept[rows] * jnp.exp(block["falling"] - block["middle"]))
        pairs = PAIRS_NT(left, block["right"])
        recept_beta = jnp.where(inclusive, pairs[:, :128], 0.0)
        recept_keys = jnp.where(inclusive, pairs[:, 128:], 0.0)
        reads = READ(recept_beta, block["gathered"])
        read_a = reads[:64, :128] + reads[64:, :128] + recept[rows] * jnp.exp(block["falling"])
        read_b = reads[:, 128:] + READ(recept_keys, block["values"])
        read_b = read_b[:64] + read_b[64:]
        if b:
            seen = READ(read_a, block["start"])
            read_a, read_b = seen[:, :128], seen[:, 128:] + read_b
        reads_a.append(read_a)
        reads_b.append(read_b)
    return jnp.concatenate(reads_a, axis=0), jnp.concatenate(reads_b, axis=0)


def local_scan(recept, keys, values, decay_pre, removal_pre, *rest):
    blocks = prepared(keys, values, decay_pre, removal_pre, *rest)
    inverted(blocks)
    trans = transition(blocks)
    return (*trans, *read_parts(blocks, recept))


def packed_heads(trans_a, trans_b):
    lane = lax.broadcasted_iota(jnp.int32, (64, 128), 1)
    head0 = jnp.where(lane < 64, trans_a[:64], pltpu.roll(trans_b[:64], 64, 1))
    head1 = jnp.where(lane < 64, pltpu.roll(trans_a[64:], 64, 1), trans_b[64:])
    return head0, head1


def coded(both):
    i, j = iotas(64, 128)
    on = i == j
    diagonal = jnp.sum(jnp.where(on, both, 0.0), axis=0, keepdims=True)
    high, rest = split2(diagonal)
    low = (diagonal - high.astype(F32) - rest.astype(F32)).astype(BF16)
    row = lax.broadcasted_iota(jnp.int32, (16, 128), 0)
    below = jnp.where(
        row == 0,
        high.astype(F32),
        jnp.where(row == 1, rest.astype(F32), jnp.where(row == 2, low.astype(F32), 0.0)),
    )
    return jnp.concatenate([jnp.where(on, 0.0, both), below], axis=0).astype(BF16)


def decoded(code):
    code = code.astype(F32)
    i, j = iotas(64, 128)
    diagonal = code[64:65] + code[65:66] + code[66:67]
    return jnp.where(i == j, diagonal, code[:64])


def combine(later, total):
    lane = lax.broadcasted_iota(jnp.int32, later.shape, 1)
    return three(later[:, :64], total) + jnp.where(lane < 64, 0.0, later)


FIRST = 256
SECOND = 256
THIRD = 128


def joined(ref, base, c, first):
    columns = pl.ds(base, first)
    rows = []
    for i in range(N):
        for j in range(N):
            b_ = (1 - c) * i + c * j
            a_ = (1 - c) * j + c * i
            rows.append(ref[b_, a_, :, :, columns].reshape(32, first))
    return jnp.concatenate(rows, axis=0)


def kernel(
    tokens,
    norm_gain,
    w0,
    w1,
    w2,
    w3,
    w4,
    w5,
    w6,
    w7,
    out_scan,
    out_conv,
    key_gain,
    removal_gain,
    removal_bias,
    decay_bias,
    extra,
    scan_norm_gain,
    conv_kernel,
    conv_bias,
    conv_norm_gain,
    out,
    mine1,
    mine2,
    mine3,
    weights,
    later,
    last_w,
    extras,
    norm_gain_v,
    tok,
    normed,
    proj,
    outw0,
    outw1,
    line_y,
    line_z,
    rim,
    conv_in,
    conv_pad,
    stats,
    send_scan,
    send_conv,
    feats_scan,
    feats_conv,
    reads_a,
    reads_b,
    load_sem,
    tok_send,
    tok_recv,
    share_send,
    share_recv,
    wide_sems,
    wide_first,
    wide_plus,
    wide_minus,
    thin_sems,
    thin_first,
    thin_plus,
    thin_minus,
    third_sems,
    third_first,
    third_plus,
    third_minus,
    outw_send,
    outw_recv,
    outw_load,
    outw_cross_send,
    outw_cross_recv,
    y_send,
    y_recv,
    z_send,
    z_recv,
    rim_send,
    rim_recv,
    stats_send,
    stats_recv,
    scan_send,
    scan_recv,
    conv_send,
    conv_recv,
    small_w,
    small_v,
    small_k,
    small_sem,
):
    z, y, c, x = (lax.axis_index(n) for n in (*SP, "tp"))
    upper = c == 1

    def at(z_=None, y_=None, c_=None, x_=None):
        pick = lambda a, b: a if b is None else b
        return (pick(z, z_), pick(y, y_), pick(c, c_), pick(x, x_))

    def remote(src, dst, send, recv, where):
        return pltpu.make_async_remote_copy(
            src_ref=src, dst_ref=dst, send_sem=send, recv_sem=recv, device_id=where, device_id_type=MESH
        )

    partner = at(c_=1 - c)
    a = (1 - c) * y + c * z
    b = (1 - c) * z + c * y

    loads = [
        pltpu.make_async_copy(tokens, tok.at[x], load_sem.at[0]),
        pltpu.make_async_copy(extra, extras.at[c], load_sem.at[1]),
        pltpu.make_async_copy(norm_gain, norm_gain_v, load_sem.at[2]),
    ]
    sources = [w0, w1, w2, w3, w4, w5, w6, w7, out_scan, out_conv]
    vectors = [key_gain, removal_gain, removal_bias, decay_bias, scan_norm_gain, conv_bias, conv_norm_gain]
    weight_loads = [
        pltpu.make_async_copy(ref, small_w.at[k], small_sem.at[k]) for k, ref in enumerate(sources)
    ]
    loads += [
        pltpu.make_async_copy(ref, small_v.at[k], small_sem.at[10 + k]) for k, ref in enumerate(vectors)
    ]
    loads.append(pltpu.make_async_copy(conv_kernel, small_k, small_sem.at[17]))
    for load in weight_loads + loads:
        load.start()
    w0, w1, w2, w3, w4, w5, w6, w7, out_scan, out_conv = (small_w.at[k] for k in range(10))
    key_gain, removal_gain, removal_bias, decay_bias, scan_norm_gain, conv_bias, conv_norm_gain = (
        small_v.at[k] for k in range(7)
    )
    conv_kernel = small_k

    barrier = pltpu.get_barrier_semaphore()
    greeted = [partner]
    for k in range(1, N):
        for core in range(2):
            greeted.append(at(y_=lax.rem(y + k, N), c_=core))
            greeted.append(at(z_=lax.rem(z + k, N), c_=core))
    for k in range(1, NX):
        for core in range(2):
            greeted.append(at(x_=lax.rem(x + k, NX), c_=core))
    chip = z * N + y
    before = lax.rem(chip + N * N - 1, N * N)
    after = lax.rem(chip + 1, N * N)
    greeted.append((before // N, lax.rem(before, N), c, x))
    for device in greeted:
        pl.semaphore_signal(barrier, inc=1, device_id=device, device_id_type=MESH)

    for load in weight_loads:
        load.wait()
    lane16 = lax.broadcasted_iota(jnp.int32, (16, 128), 1) < 64

    def halves(left, right):
        left, right = left.astype(F32), right.astype(F32)
        first = jnp.where(lane16, left, pltpu.roll(right, 64, 1))
        return first.astype(BF16), jnp.where(lane16, pltpu.roll(left, 64, 1), right).astype(BF16)

    for k, (left, right) in enumerate(((w1, w2), (w3, w4))):
        for core, part_ in enumerate(halves(left[...], right[...])):
            mine1[core, :, 128 * k : 128 * (k + 1)] = part_
    for core, part_ in enumerate(halves(w6[...], w7[...])):
        mine2[core, :, 0:128] = part_
    for core, part_ in enumerate(halves(w0[...], w5[...])):
        mine3[core] = part_
    mine2[0, :, 128:256] = out_scan[...]
    mine2[1, :, 128:256] = out_conv[...]

    pl.semaphore_wait(barrier, len(greeted))

    class Gather:
        def __init__(self, own, ref, sems, first_recv, plus_recv, minus_recv):
            self.own, self.ref, self.first_recv = own, ref, first_recv
            self.first_send, self.second_send, self.keep, self.pair_send = (sems.at[k] for k in range(4))
            self.recvs = {1: plus_recv, -1: minus_recv}

        def start(self):
            for k in (0, 1, 7, 2, 6, 3, 5, 4):
                for core in range(2):
                    a_, b_ = (y, z) if core == 0 else (z, y)
                    target = (z, lax.rem(y + k, N), 0, x) if core == 0 else (lax.rem(z + k, N), y, 1, x)
                    src, dst = self.own.at[core], self.ref.at[b_, a_, c]
                    recv = self.first_recv.at[2 * a_ + c]
                    copy = remote(src, dst, self.first_send if k else self.pair_send, recv, target)
                    if k:
                        copy.start()
                    else:

                        @pl.when(c != core)
                        def _():
                            copy.start()

                        @pl.when(c == core)
                        def _():
                            pltpu.make_async_copy(src, dst, self.keep).start()

        def low(self, h):
            return lax.rem(a // 2 + h, 4) * 2

        def piece(self, h, distance):
            return self.ref.at[lax.rem(b + distance + N, N), pl.ds(self.low(h), 2)]

        def copy(self, h, source, sign, reach):
            piece = self.piece(h, -sign * source)
            recv = self.recvs[sign].at[h * 4 + source + reach - 1]
            k = reach if sign > 0 else N - reach
            target = at(z_=lax.rem(z + (1 - c) * k, N), y_=lax.rem(y + c * k, N))
            return remote(piece, piece, self.second_send, recv, target)

        def collect(self, h):
            for k in range(2):
                a_ = self.low(h) + k
                for core in range(2):
                    piece = self.ref.at[b, a_, core]

                    def wait():
                        recv = self.first_recv.at[2 * a_ + core]
                        remote(piece, piece, self.first_send, recv, partner).wait_recv()

                    if h:
                        wait()
                    else:
                        own = jnp.logical_and(a_ == a, c == core)
                        pl.when(jnp.logical_not(own))(wait)
            if h == 0:
                own = self.ref.at[b, a, c]
                pltpu.make_async_copy(own, own, self.keep).wait()
            for reach in (2, 1):
                for sign in (1, -1):
                    self.copy(h, 0, sign, reach).start()

        def has_far(self, h, sign):
            return (h % 2 == 0) == (sign > 0)

        def arrive(self, h, d, sign):
            self.copy(h, 0, sign, d).wait_recv()

        def relay(self, h):
            for sign in (1, -1):
                self.arrive(h, 2, sign)
                if self.has_far(h, sign):
                    self.copy(h, 2, sign, 2).start()
                self.copy(h, 2, sign, 1).start()

        def near(self, h):
            for sign in (1, -1):
                self.arrive(h, 1, sign)

        def far(self, h):
            for sign in (1, -1):
                if self.has_far(h, sign):
                    self.arrive(h, 4, sign)
                self.arrive(h, 3, sign)

        def drain(self):
            fourteen = self.ref.at[0, pl.ds(0, 7)]
            remote(fourteen, fourteen, self.first_send, self.first_recv.at[0], partner).wait_send()
            single = self.ref.at[0, 7, 0]
            remote(single, single, self.pair_send, self.first_recv.at[0], partner).wait_send()
            most = self.ref.at[pl.ds(0, 7)]
            remote(most, most, self.second_send, self.first_recv.at[0], partner).wait_send()

    wide = Gather(mine1, weights, wide_sems, wide_first, wide_plus, wide_minus)
    thin = Gather(mine2, later, thin_sems, thin_first, thin_plus, thin_minus)
    third = Gather(mine3, last_w, third_sems, third_first, third_plus, third_minus)
    wide.start()
    for load in loads:
        load.wait()
    tok_copies = [
        remote(tok.at[x], tok.at[x], tok_send.at[k - 1], tok_recv.at[k - 1], at(x_=lax.rem(x + k, NX)))
        for k in (1, 3, 2)
    ]
    for copy in tok_copies:
        copy.start()
    extra_copy = remote(extras.at[c], extras.at[c], share_send.at[0], share_recv.at[0], partner)
    extra_copy.start()
    normed_copy = remote(normed.at[c], normed.at[c], share_send.at[1], share_recv.at[1], partner)

    order = (0, 1, 3, 2)
    for h in order:
        wide.collect(h)
    thin.start()
    for h in order:
        wide.relay(h)
    third.start()
    for copy in tok_copies:
        copy.wait_recv()
    square = jnp.zeros((ROWS, 1), F32)
    for q in range(NX):
        t = tok[q].astype(F32)
        square = square + jnp.sum(t * t, axis=-1, keepdims=True)
    factor = lax.rsqrt(square * (1.0 / MODEL) + 1e-06)
    for q in range(NX):
        t = tok[q].astype(F32)
        columns = slice(q * 512, (q + 1) * 512)
        normed[c, :, columns] = (t * factor * norm_gain_v[:, columns]).astype(BF16)
    normed_copy.start()
    for h in order:
        thin.collect(h)
    for h in order:
        wide.near(h)
    extra_copy.wait_recv()
    normed_copy.wait_recv()
    for h in order:
        wide.far(h)

    lane = lax.broadcasted_iota(jnp.int32, (ROWS, 128), 1) < 64

    def turned(v):
        return pltpu.roll(v, 64, 1)

    def own_head(v):
        low = lax.broadcasted_iota(jnp.int32, v.shape, 1) < 64
        other = turned(v)
        return jnp.where(upper, jnp.where(low, other, v), jnp.where(low, v, other))

    def project(ref, base, width, target):
        w = joined(ref, base, c, width)
        for half in range(2):
            proj[half, :, target : target + width] = jnp.dot(
                normed[half], w, preferred_element_type=F32
            ).astype(BF16)

    def parts(k):
        columns = slice(128 * k, 128 * (k + 1))
        p0, p1 = proj[0, :, columns].astype(F32), proj[1, :, columns].astype(F32)
        return jnp.where(lane, p0, turned(p1)), jnp.where(lane, turned(p0), p1)

    project(weights, 0, FIRST, 0)
    keys, values = parts(0)
    decay_pre, removal_pre = parts(1)
    e0, e1 = extras[0], extras[1]
    own_extra = jnp.where(
        upper, jnp.where(lane, turned(e0), e1), jnp.where(lane, e0, turned(e1))
    )
    blocks = prepared(
        keys,
        values,
        decay_pre,
        removal_pre,
        own_head(key_gain[...]),
        own_head(removal_gain[...]),
        own_head(removal_bias[...]),
        own_head(decay_bias[...]),
        own_extra,
    )
    inverted(blocks)
    half0, half1 = packed_heads(*transition(blocks))
    line_y[y] = coded(combine(half1, half0))
    for k in (4, 3, 5, 2, 6, 1, 7):
        remote(line_y.at[y], line_y.at[y], y_send, y_recv.at[y], at(y_=lax.rem(y + k, N))).start()
    for h in order:
        thin.relay(h)
    for h in order:
        third.collect(h)
    for h in order:
        thin.near(h)
        thin.far(h)

    def outw_copies(p):
        for k in (1, 3, 2, 0):
            x_ = lax.rem(x + k, NX)
            if p:
                src, dst = later.at[:, pl.ds(2 * x_, 2), :, :, pl.ds(128, 128)], outw1.at[x]
            else:
                src, dst = later.at[pl.ds(2 * x_, 2), :, :, :, pl.ds(128, 128)], outw0.at[x]
            if k:
                yield remote(src, dst, outw_send.at[k - 1], outw_recv.at[k - 1], at(x_=x_))
            else:
                yield pltpu.make_async_copy(src, dst, outw_load)

    for p in range(2):

        @pl.when(c == p)
        def _():
            for copy in outw_copies(p):
                copy.start()

    outw_waits = list(outw_copies(0))

    project(later, 0, 128, 384)
    conv_value, conv_gate = parts(3)
    conv_in[...] = (conv_value * sigmoid(conv_gate)).astype(BF16)
    last = chip == N * N - 1
    start = chip == 0
    rim_copy = remote(
        conv_in.at[pl.ds(ROWS - 32, 32)], rim, rim_send, rim_recv, (after // N, lax.rem(after, N), c, x)
    )

    @pl.when(jnp.logical_not(last))
    def _():
        rim_copy.start()

    lane64 = lax.broadcasted_iota(jnp.int32, (64, 128), 1)
    i, j = iotas(64, 128)
    nothing = (i == j).astype(F32)
    for k in range(N):

        @pl.when(y != k)
        def _():
            remote(line_y.at[k], line_y.at[k], y_send, y_recv.at[k], partner).wait_recv()

    each = [decoded(line_y[k]) for k in range(N)]
    pairs = [combine(each[2 * k + 1], each[2 * k]) for k in range(4)]
    quads = [combine(pairs[1], pairs[0]), combine(pairs[3], pairs[2])]
    line_z[z] = coded(combine(quads[1], quads[0]))
    z_copies = []
    for k in range(N - 1, 0, -1):
        copy = remote(
            line_z.at[z], line_z.at[z], z_send.at[k - 1], z_recv.at[z], at(z_=lax.rem(z + k, N))
        )
        z_copies.append((k, copy))

        @pl.when(z + k < N)
        def _():
            copy.start()

    for h in order:
        third.relay(h)
    inside = jnp.where(y >= 4, quads[0], nothing)
    inside = jnp.where(lax.rem(y, 4) >= 2, combine(jnp.where(y >= 4, pairs[2], pairs[0]), inside), inside)
    previous = decoded(line_y[jnp.maximum(y - 1, 0)])
    inside = jnp.where(lax.rem(y, 2) == 1, combine(previous, inside), inside)

    @pl.when(start)
    def _():
        rim[...] = jnp.zeros_like(rim)

    @pl.when(jnp.logical_not(start))
    def _():
        rim_copy.wait_recv()

    ending = conv_in[pl.ds(ROWS - 32, 32)].astype(F32)
    conv_pad[pl.ds(0, 32)] = turned(jnp.where(lane[:32], ending, rim[...].astype(F32)))
    conv_pad[pl.ds(32, ROWS)] = conv_in[...].astype(F32)
    taps = own_head(conv_kernel[...])
    filtered = own_head(conv_bias[...]) + taps[0:1] * conv_pad[pl.ds(2, ROWS)]
    for k in range(1, CONV_K):
        filtered = filtered + taps[k : k + 1] * conv_pad[pl.ds(2 + k, ROWS)]
    ones = head_ones()
    near = right_exact(filtered, ones) * (1.0 / 64.0)
    around = right_exact((filtered - near) ** 2, ones)
    spot = lax.broadcasted_iota(jnp.int32, (ROWS, 128), 1) & 63
    table = jnp.where(spot == 0, near, jnp.where(spot == 1, around, 0.0)).T
    stats[x, c, 0:8] = table[0:8]
    stats[x, c, 8:16] = table[64:72]
    conv_pad[pl.ds(0, ROWS)] = filtered

    mates = [(k, core) for k in (1, 3, 2, 0) for core in range(2)]

    def to_mates(copy_of, send, recv):
        copies = []
        for k, core in mates:
            src, dst = copy_of(core)
            copy = remote(src, dst, send.at[2 * k + core], recv.at[2 * k + c], at(x_=lax.rem(x + k, NX), c_=core))
            copies.append((k, core, copy))
        return copies

    def start_all(copies, keep):
        for k, core, copy in copies:
            if k:
                copy.start()
            else:

                @pl.when(c != core)
                def _():
                    copy.start()

                if keep is not None:

                    @pl.when(c == core)
                    def _():
                        keep(core)

    def wait_all(copies, recv):
        for k, core, copy in copies:
            src, dst = copy.src_ref, copy.dst_ref
            arriving = remote(dst, dst, recv.at[2 * k + core], recv.at[2 * k + core], partner)
            if k:
                arriving.wait_recv()
            else:

                @pl.when(c != core)
                def _():
                    arriving.wait_recv()

    def sent_all(copies):
        for k, core, copy in copies:
            if k:
                copy.wait_send()
            else:

                @pl.when(c != core)
                def _():
                    copy.wait_send()

    stats_copies = to_mates(lambda core: (stats.at[x, c], stats.at[x, c]), stats_send, stats_recv)
    start_all(stats_copies, None)

    for h in order:
        third.near(h)
        third.far(h)
    project(last_w, 0, 128, 256)
    recept, gate_pre = parts(2)
    reads_a[...], reads_b[...] = read_parts(blocks, recept)

    for copy in outw_waits[:3]:
        copy.wait_recv()
    outw_waits[3].wait()
    for p, ref in enumerate((outw0, outw1)):

        @pl.when(c == p)
        def _():
            remote(ref, ref, outw_cross_send, outw_cross_recv, partner).start()

    wait_all(stats_copies, stats_recv)
    sides = []
    for half in range(2):
        rows = [stats[q, core, 8 * half : 8 * half + 2] for q in range(NX) for core in range(2)]
        center = sum(r[0:1] for r in rows) * (1.0 / 8.0)
        around_row = sum(r[1:2] + 64.0 * (r[0:1] - center) ** 2 for r in rows)
        sides.append((center, lax.rsqrt(around_row * (1.0 / 512.0) + 1e-05)))
    row = lax.broadcasted_iota(jnp.int32, (8, ROWS), 0)
    column = jnp.where(
        row == 0,
        sides[0][0],
        jnp.where(row == 1, sides[0][1], jnp.where(row == 2, sides[1][0], sides[1][1])),
    ).T
    center = jnp.where(lane, column[:, 0:1], column[:, 2:3])
    scale = jnp.where(lane, column[:, 1:2], column[:, 3:4])
    normal = (conv_pad[pl.ds(0, ROWS)] - center) * scale * own_head(conv_norm_gain[...])

    def by_half(v, ref):
        upper_rows, lower_rows = v[:96], v[96:]
        low = lane[:96]
        ref[0] = jnp.where(low, upper_rows, turned(lower_rows)).astype(BF16)
        ref[1] = jnp.where(low, turned(upper_rows), lower_rows).astype(BF16)

    def natural(ref, q):
        f0, f1 = ref[q, 0].astype(F32), ref[q, 1].astype(F32)
        low = lane[:96]
        rows = [jnp.where(low, f0, turned(f1)), jnp.where(low, turned(f0), f1)]
        return jnp.concatenate(rows, axis=0).astype(BF16)

    by_half(normal * sigmoid(normal), send_conv)
    conv_copies = to_mates(lambda core: (send_conv.at[core], feats_conv.at[x, c]), conv_send, conv_recv)

    def keep_conv(core):
        feats_conv[x, c] = send_conv[core]

    start_all(conv_copies, keep_conv)

    for k in range(N - 1):

        @pl.when(k < z)
        def _():
            remote(line_z.at[k], line_z.at[k], z_send.at[0], z_recv.at[k], partner).wait_recv()

    each = [jnp.where(k < z, decoded(line_z[k]), nothing) for k in range(N - 1)]
    pairs = [combine(each[2 * k + 1], each[2 * k]) for k in range(3)]
    state = combine(combine(each[6], pairs[2]), combine(pairs[1], pairs[0]))
    state = jnp.where(lane64 < 64, 0.0, state)
    state0 = jnp.where(lane64 < 64, 0.0, combine(inside, state))
    state1 = combine(half0, state0)
    whole = jnp.concatenate(
        [
            jnp.where(lane64 < 64, turned(state0), 0.0),
            jnp.where(lane64 < 64, 0.0, state1),
        ],
        axis=0,
    )
    reads = three(reads_a[...], whole) + reads_b[...]
    reads = reads - right_exact(reads, ones) * (1.0 / 64.0)
    spread_ = right_exact(reads * reads, ones) * (1.0 / 64.0)
    by_half(
        reads * lax.rsqrt(spread_ + 0.00064) * own_head(scan_norm_gain[...]) * sigmoid(gate_pre), send_scan
    )
    scan_copies = to_mates(lambda core: (send_scan.at[core], feats_scan.at[x, c]), scan_send, scan_recv)

    def keep_scan(core):
        feats_scan[x, c] = send_scan[core]

    start_all(scan_copies, keep_scan)

    outw_cross = remote(outw0, outw0, outw_cross_send, outw_cross_recv, partner)
    outw_cross.wait_recv()
    wait_all(conv_copies, conv_recv)

    def w_scan(q):
        return outw0[q].reshape(512, 128)

    def w_conv(q):
        rows = [outw1[q, j, i].reshape(32, 128) for i in range(2) for j in range(N)]
        return jnp.concatenate(rows, axis=0)

    total_out = one_nt(natural(feats_conv, 0), w_conv(0))
    for q in range(1, NX):
        total_out = total_out + one_nt(natural(feats_conv, q), w_conv(q))
    wait_all(scan_copies, scan_recv)
    for q in range(NX):
        total_out = total_out + one_nt(natural(feats_scan, q), w_scan(q))
    out[...] = total_out.astype(BF16)

    for copies in (tok_copies, outw_waits[:3], [extra_copy, normed_copy, outw_cross]):
        for copy in copies:
            copy.wait_send()
    for copies in (stats_copies, conv_copies, scan_copies):
        sent_all(copies)
    wide.drain()
    thin.drain()
    third.drain()
    lines = line_y.at[pl.ds(0, 7)]
    remote(lines, lines, y_send, y_recv.at[0], partner).wait_send()

    @pl.when(jnp.logical_not(last))
    def _():
        rim_copy.wait_send()

    for k, copy in z_copies:

        @pl.when(z + k < N)
        def _():
            copy.wait_send()


def shards(
    tokens,
    norm_gain,
    query_weight,
    key_weight,
    value_weight,
    decay_weight,
    removal_weight,
    gate_weight,
    key_gain,
    removal_gain,
    removal_bias,
    decay_bias,
    decay_extra,
    scan_norm_gain,
    conv_value_weight,
    conv_gate_weight,
    conv_kernel,
    conv_bias,
    conv_norm_gain,
    out_scan_weight,
    out_conv_weight,
):
    row = lambda v: v.reshape(1, -1)
    anywhere = pl.BlockSpec(memory_space=pl.ANY)
    inside = pl.BlockSpec(memory_space=pltpu.VMEM)
    dma = pltpu.SemaphoreType.DMA
    vmem = pltpu.VMEM
    return pl.pallas_call(
        kernel,
        out_shape=jax.ShapeDtypeStruct((ROWS, 512), BF16),
        in_specs=[anywhere] * 21,
        out_specs=inside,
        scratch_shapes=[
            vmem((2, 16, FIRST), BF16),
            vmem((2, 16, SECOND), BF16),
            vmem((2, 16, THIRD), BF16),
            vmem((N, N, 2, 16, FIRST), BF16),
            vmem((N, N, 2, 16, SECOND), BF16),
            vmem((N, N, 2, 16, THIRD), BF16),
            vmem((2, ROWS, 128), F32),
            vmem((1, MODEL), F32),
            vmem((NX, ROWS, 512), BF16),
            vmem((2, ROWS, MODEL), BF16),
            vmem((2, ROWS, 512), BF16),
            vmem((NX, 2, N, 2, 16, 128), BF16),
            vmem((NX, N, 2, 2, 16, 128), BF16),
            vmem((N, 80, 128), BF16),
            vmem((N, 80, 128), BF16),
            vmem((32, 128), BF16),
            vmem((ROWS, 128), BF16),
            vmem((ROWS + 32, 128), F32),
            vmem((NX, 2, 16, ROWS), F32),
            vmem((2, 96, 128), BF16),
            vmem((2, 96, 128), BF16),
            vmem((NX, 2, 96, 128), BF16),
            vmem((NX, 2, 96, 128), BF16),
            vmem((ROWS, 128), F32),
            vmem((ROWS, 128), F32),
            dma((3,)),
            dma((3,)),
            dma((3,)),
            dma((2,)),
            dma((2,)),
            dma((4,)),
            dma((16,)),
            dma((16,)),
            dma((16,)),
            dma((4,)),
            dma((16,)),
            dma((16,)),
            dma((16,)),
            dma((4,)),
            dma((16,)),
            dma((16,)),
            dma((16,)),
            dma((3,)),
            dma((3,)),
            dma(()),
            dma(()),
            dma(()),
            dma(()),
            dma((N,)),
            dma((N - 1,)),
            dma((N,)),
            dma(()),
            dma(()),
            dma((8,)),
            dma((8,)),
            dma((8,)),
            dma((8,)),
            dma((8,)),
            dma((8,)),
            vmem((10, 16, 128), BF16),
            vmem((7, 1, 128), F32),
            vmem((CONV_K, 128), F32),
            dma((18,)),
        ],
        compiler_params=pltpu.CompilerParams(
            collective_id=0, has_side_effects=True, vmem_limit_bytes=56 * 1024 * 1024
        ),
    )(
        tokens,
        row(norm_gain),
        query_weight,
        key_weight,
        value_weight,
        decay_weight,
        removal_weight,
        gate_weight,
        conv_value_weight,
        conv_gate_weight,
        out_scan_weight.T,
        out_conv_weight.T,
        row(key_gain),
        row(removal_gain),
        row(removal_bias),
        row(decay_bias),
        decay_extra,
        row(scan_norm_gain),
        conv_kernel,
        row(conv_bias),
        row(conv_norm_gain),
    )


def solution(mesh):
    torus = Mesh(mesh.devices.reshape(N, N, 2, mesh.shape["tp"]), (*SP, "tp"))
    in_specs = (
        P(SP, "tp"),
        P(),
        P(SP, "tp"),
        P(SP, "tp"),
        P(SP, "tp"),
        P(SP, "tp"),
        P(SP, "tp"),
        P(SP, "tp"),
        P("tp"),
        P("tp"),
        P("tp"),
        P("tp"),
        P(SP, "tp"),
        P("tp"),
        P(SP, "tp"),
        P(SP, "tp"),
        P(None, "tp"),
        P("tp"),
        P("tp"),
        P("tp", SP),
        P("tp", SP),
    )
    return jax.shard_map(
        shards, mesh=torus, in_specs=in_specs, out_specs=P(SP, "tp"), check_vma=False
    )
```
